512 devices in a mesh: sp: 16 (over z), fs: 4 (over y), tp: 8 (over x, core).
Axes of the slice: x: 4, y: 4, z: 16, core: 2. Of those that a mesh axis runs over, the one named last changes fastest.
Arguments:
- tokens: bfloat16 [4, 4096, 2048], P('fs', 'sp'), may hold values from -6 to 6
- norm_gain: float32 [2048], replicated, may hold values from 0.1 to 1.9
- w_state_in: bfloat16 [2048, 1024], P(('sp', 'fs'), 'tp'), may hold values from -0.125 to 0.125
- w_value: bfloat16 [2048, 1024], P(('sp', 'fs'), 'tp'), may hold values from -0.125 to 0.125
- w_outer: bfloat16 [2048, 1024], P(('sp', 'fs'), 'tp'), may hold values from -0.125 to 0.125
- w_inner: bfloat16 [2048, 1024], P(('sp', 'fs'), 'tp'), may hold values from -0.125 to 0.125
- w_state_out: bfloat16 [2048, 1024], P(('sp', 'fs'), 'tp'), may hold values from -0.125 to 0.125
- w_conv_out: bfloat16 [2048, 1024], P(('sp', 'fs'), 'tp'), may hold values from -0.125 to 0.125
- log_step: float32 [64], P('tp'), may hold values from -4.6 to -3.2
- decay_real: float32 [64, 64], P('tp'), may hold values from -5 to 0
- frequency: float32 [64, 64], P('tp'), may hold values from 1 to 192
- step_rate: float32 [4, 4096], P('fs', 'sp'), may hold values from 0.4 to 2.5
- input_real: float32 [64, 64, 16], P('tp'), may hold values from -1 to 1
- input_imag: float32 [64, 64, 16], P('tp'), may hold values from -1 to 1
- read_real: float32 [64, 16, 64], P('tp'), may hold values from -0.75 to 0.75
- read_imag: float32 [64, 16, 64], P('tp'), may hold values from -0.75 to 0.75
- skip_gain: float32 [64, 16], P('tp'), may hold values from -4 to 4
- conv_taps: float32 [3, 1024], P(None, 'tp'), may hold values from -3.5 to 3.5
- initial_state: float32 [4, 2, 64, 64], P('fs', None, 'tp'), may hold values from -6 to 6
Outputs:
- mixed: bfloat16 [4, 4096, 2048], P('fs', ('sp', 'tp'))
- final_state: float32 [4, 2, 64, 64], P('fs', None, 'tp', 'sp')
The draws below stay inside these ranges and needn't reach their ends.
All inputs are finite; a program needn't handle non-finite values.
Results may differ from the reference program's by a relative error of at most 0.018.
Values may be sent and summed in bfloat16 or wider, within the bound.
No kernel may reach another device: no remote copies, remote signals or barrier semaphores. Data moves between devices by JAX's collectives and lax.ppermute only.
A program may use at most 64 MiB of HBM per device.

```python
import math
import jax
import jax.numpy as jnp
from jax import lax

D = 2048
GROUPS = 64
GROUP = 16
STATE = 64
CW = 1024
KW = 3
SW = 1024
SEQS = 4
LENGTH = 4096
N_TP = 8


def draw_decay_real(key, part):
    base = jax.random.fold_in(key, 7)
    key_pick, key_slow, key_fast = jax.random.split(base, 3)
    share = 0.5
    pick = jax.random.uniform(key_pick, (GROUPS, 1), jnp.float32) < share
    slow = -jnp.exp(jax.random.uniform(key_slow, (GROUPS, STATE), jnp.float32, math.log(5.0 / LENGTH), math.log(60.0 / LENGTH)))
    fast = -jnp.exp(jax.random.uniform(key_fast, (GROUPS, STATE), jnp.float32, math.log(2.0), math.log(5.0)))
    return jnp.where(pick, slow, fast)


def draw_step_rate(key, part):
    base = jax.random.fold_in(key, 13)
    key_slow, key_fine = jax.random.split(base, 2)
    blocks = LENGTH // 256
    slow = jnp.exp(jax.random.uniform(key_slow, (SEQS, blocks), jnp.float32, math.log(0.5), math.log(2.0)))
    fine = jax.random.uniform(key_fine, (SEQS, LENGTH), jnp.float32, 0.8, 1.25)
    return jnp.repeat(slow, 256, axis=1) * fine


def shard_levels(own_key, shape, cuts, smallest, top_value):
    level, own = 1.0, jax.random.fold_in(own_key, 6)
    for axis_at, parts in cuts:
        draws = jnp.exp(jax.random.uniform(jax.random.fold_in(own, axis_at), (parts,), jnp.float32, smallest / len(cuts), top_value / len(cuts)))
        level = level * jnp.repeat(draws, shape[axis_at] // parts).reshape([-1 if axis == axis_at else 1 for axis in range(len(shape))])
    return level


def noise(rng, shape, deviation, reach, pieces=(), kind=jnp.bfloat16):
    drawn = jax.random.normal(rng, shape, jnp.float32) * deviation
    if len(pieces) > 0:
        drawn = shard_levels(rng, shape, pieces, -0.22, 0.18) * drawn
    return jnp.clip(drawn, min=-reach, max=reach).astype(kind)


def setup_inputs(seed: int = 0) -> dict:
    streams_of = jax.random.split(jax.random.key(seed), 20)
    return {
        "tokens": noise(streams_of[0], (SEQS, LENGTH, D), 1.0, 6.0, ((0, 4), (1, 16))),
        "norm_gain": jnp.clip(1.0 + 0.18 * jax.random.normal(streams_of[1], (D,), jnp.float32), 0.1, 1.9),
        "w_state_in": noise(streams_of[2], (D, SW), D ** -0.5, 0.125, ((0, 64), (1, 8))),
        "w_value": noise(streams_of[3], (D, CW), D ** -0.5, 0.125, ((0, 64), (1, 8))),
        "w_outer": noise(streams_of[4], (D, CW), D ** -0.5, 0.125, ((0, 64), (1, 8))),
        "w_inner": noise(streams_of[5], (D, CW), D ** -0.5, 0.125, ((0, 64), (1, 8))),
        "w_state_out": noise(streams_of[6], (D, SW), (SW + CW) ** -0.5, 0.125, ((0, 64), (1, 8))),
        "w_conv_out": noise(streams_of[7], (D, CW), (SW + CW) ** -0.5, 0.125, ((0, 64), (1, 8))),
        "log_step": jnp.clip(-4.6 + 1.3999999 * jax.random.uniform(streams_of[8], (GROUPS,), jnp.float32) ** shard_levels(streams_of[8], (GROUPS,), ((0, 8),), -0.2, 0.2), -4.6, -3.2),
        "decay_real": draw_decay_real(jax.random.fold_in(streams_of[19], 71), 0),
        "frequency": jnp.clip(1.0 + 191.0 * jax.random.uniform(streams_of[10], (GROUPS, STATE), jnp.float32) ** shard_levels(streams_of[10], (GROUPS, STATE), ((0, 8),), -0.2, 0.2), 1.0, 192.0),
        "step_rate": draw_step_rate(jax.random.fold_in(streams_of[19], 71), 0),
        "input_real": noise(streams_of[12], (GROUPS, STATE, GROUP), (2 * GROUP) ** -0.5, 1.0, ((0, 8),), jnp.float32),
        "input_imag": noise(streams_of[13], (GROUPS, STATE, GROUP), (2 * GROUP) ** -0.5, 1.0, ((0, 8),), jnp.float32),
        "read_real": noise(streams_of[14], (GROUPS, GROUP, STATE), STATE ** -0.5, 0.75, ((0, 8),), jnp.float32),
        "read_imag": noise(streams_of[15], (GROUPS, GROUP, STATE), STATE ** -0.5, 0.75, ((0, 8),), jnp.float32),
        "skip_gain": noise(streams_of[16], (GROUPS, GROUP), 1.0, 4.0, ((0, 8),), jnp.float32),
        "conv_taps": noise(streams_of[17], (KW, CW), KW ** -0.5, 3.5, ((1, 8),), jnp.float32),
        "initial_state": noise(streams_of[18], (SEQS, 2, GROUPS, STATE), 1.0, 6.0, ((0, 4), (2, 8)), jnp.float32),
    }


def reference(tokens, norm_gain, w_state_in, w_value, w_outer, w_inner, w_state_out, w_conv_out, log_step, decay_real, frequency, step_rate, input_real, input_imag, read_real, read_imag, skip_gain, conv_taps, initial_state):
    seqs, length, width = tokens.shape
    features = tokens.astype(jnp.float32)
    mean_square = lax.optimization_barrier(jnp.mean(features * features, axis=-1, keepdims=True))
    normed = (features * lax.rsqrt(mean_square + 1e-06) * norm_gain).astype(jnp.bfloat16).reshape(seqs * length, width)

    def project(matrix):
        return jnp.dot(normed, matrix, preferred_element_type=jnp.float32).astype(jnp.bfloat16)
    state_in = project(w_state_in)
    value = project(w_value)
    outer = project(w_outer)
    inner = project(w_inner)
    groups, states = decay_real.shape
    group = skip_gain.shape[1]
    channels = state_in.astype(jnp.float32).reshape(seqs, length, groups, group)
    step = jnp.exp(log_step)[None, None, :] * step_rate[:, :, None]
    modulus = decay_real * decay_real + frequency * frequency

    def advance(carry, inputs):
        hidden_real, hidden_imag = carry
        chan_now, step_now = inputs
        scaled = step_now[..., None]
        grow = jnp.exp(scaled * decay_real)
        angle = scaled * frequency
        bar_real = grow * jnp.cos(angle)
        bar_imag = grow * jnp.sin(angle)
        less_real = bar_real - 1.0
        hold_real = (less_real * decay_real + bar_imag * frequency) / modulus
        hold_imag = (bar_imag * decay_real - less_real * frequency) / modulus
        drive_real = jnp.einsum('sgh,gph->sgp', chan_now, input_real, precision=lax.Precision.HIGHEST)
        drive_imag = jnp.einsum('sgh,gph->sgp', chan_now, input_imag, precision=lax.Precision.HIGHEST)
        push_real = hold_real * drive_real - hold_imag * drive_imag
        push_imag = hold_real * drive_imag + hold_imag * drive_real
        next_real = bar_real * hidden_real - bar_imag * hidden_imag + push_real
        next_imag = bar_real * hidden_imag + bar_imag * hidden_real + push_imag
        response = jnp.einsum('sgp,ghp->sgh', next_real, read_real, precision=lax.Precision.HIGHEST) - jnp.einsum('sgp,ghp->sgh', next_imag, read_imag, precision=lax.Precision.HIGHEST) + skip_gain * chan_now
        return ((next_real, next_imag), response)
    (last_real, last_imag), responses = lax.scan(advance, (initial_state[:, 0], initial_state[:, 1]), (channels.transpose(1, 0, 2, 3), step.transpose(1, 0, 2)))
    state_mix = jax.nn.gelu(responses.transpose(1, 0, 2, 3)).reshape(seqs * length, groups * group).astype(jnp.bfloat16)
    final_state = jnp.stack([last_real, last_imag], axis=1)
    gated = (inner.astype(jnp.float32) * value.astype(jnp.float32)).astype(jnp.bfloat16).reshape(seqs, length, -1)
    taps = conv_taps.shape[0]
    padded = jnp.pad(gated, ((0, 0), (taps - 1, 0), (0, 0))).astype(jnp.float32)
    filtered = jnp.zeros((seqs, length, gated.shape[2]), jnp.float32)
    for tap in range(taps):
        filtered = filtered + conv_taps[tap] * padded[:, tap:tap + length]
    conv_mix = (outer.astype(jnp.float32).reshape(seqs, length, -1) * filtered).astype(jnp.bfloat16).reshape(seqs * length, -1)
    state_block = state_mix.shape[1] // N_TP
    conv_block = conv_mix.shape[1] // N_TP
    total = jnp.zeros((seqs * length, width), jnp.float32)
    for block in range(N_TP):
        part = jnp.dot(state_mix[:, block * state_block:(block + 1) * state_block], w_state_out[:, block * state_block:(block + 1) * state_block].T, preferred_element_type=jnp.float32) + jnp.dot(conv_mix[:, block * conv_block:(block + 1) * conv_block], w_conv_out[:, block * conv_block:(block + 1) * conv_block].T, preferred_element_type=jnp.float32)
        total = total + lax.optimization_barrier(part.astype(jnp.bfloat16)).astype(jnp.float32)
    mixed = total.astype(jnp.bfloat16).reshape(seqs, length, width)
    return (mixed, final_state)
```

```python
import functools

import jax
import jax.numpy as jnp
from jax import lax
from jax.experimental import pallas as pl
from jax.experimental.pallas import tpu as pltpu
from jax.sharding import PartitionSpec as P

F32 = jnp.float32
BF16 = jnp.bfloat16
CHUNKS = 8
HALO = 16


def replicated(x, copies):
    return jnp.broadcast_to(x[None], (copies, *x.shape))


def spread(x, axis):
    copies = lax.axis_size(axis)
    return lax.all_to_all(replicated(x, copies), axis, 0, 0, tiled=True)


def complex_product(left_real, left_imag, right_real, right_imag):
    return (
        left_real * right_real - left_imag * right_imag,
        left_real * right_imag + left_imag * right_real,
    )


def sine_cosine(angle):
    turns = jnp.floor(angle * 0.6366197723675814 + 0.5)
    r = angle - turns * 1.5703125
    r = r - turns * 4.837512969970703e-4
    r = r - turns * 7.549789948768648e-8
    r2 = r * r
    sine = r + r * r2 * (-1.6666654611e-1 + r2 * (8.3321608736e-3 + r2 * -1.9515295891e-4))
    cosine = (
        1.0
        - 0.5 * r2
        + r2 * r2 * (4.166664568298827e-2 + r2 * (-1.388731625493765e-3 + r2 * 2.443315711809948e-5))
    )
    quadrant = turns.astype(jnp.int32)
    odd = (quadrant & 1) == 1
    flip_sine = (quadrant & 2) == 2
    flip_cosine = ((quadrant + 1) & 2) == 2
    base_sine = jnp.where(odd, cosine, sine)
    base_cosine = jnp.where(odd, sine, cosine)
    return (
        jnp.where(flip_sine, -base_sine, base_sine),
        jnp.where(flip_cosine, -base_cosine, base_cosine),
    )


def normed_kernel(x_ref, gain_ref, out_ref):
    x = x_ref[...].astype(F32)
    mean_square = jnp.mean(x * x, axis=-1, keepdims=True)
    out_ref[...] = (x * lax.rsqrt(mean_square + 1e-06) * gain_ref[...]).astype(BF16)


def maps_kernel(rate_ref, scale_ref, decay_ref, freq_ref, bar_ref, hold_ref, cum_ref, total_ref):
    flat = decay_ref.shape[1]
    decay, freq, scale = (decay_ref[...], freq_ref[...], jnp.exp(scale_ref[...]))
    inverse = 1.0 / (decay * decay + freq * freq)
    steps = rate_ref.shape[0] // CHUNKS

    def advance(j, carry):
        cum_real, cum_imag = carry
        rows = pl.ds(pl.multiple_of(j * CHUNKS, CHUNKS), CHUNKS)
        step = rate_ref[rows, :] * scale
        grow = jnp.exp(step * decay)
        sine, cosine = sine_cosine(step * freq)
        bar_real, bar_imag = (grow * cosine, grow * sine)
        less_real = bar_real - 1.0
        bar_ref[0, rows, :] = bar_real
        bar_ref[1, rows, :] = bar_imag
        hold_ref[0, rows, :] = (less_real * decay + bar_imag * freq) * inverse
        hold_ref[1, rows, :] = (bar_imag * decay - less_real * freq) * inverse
        cum_real, cum_imag = complex_product(cum_real, cum_imag, bar_real, bar_imag)
        cum_ref[0, rows, :] = cum_real
        cum_ref[1, rows, :] = cum_imag
        return (cum_real, cum_imag)

    one = jnp.ones((CHUNKS, flat), F32)
    end_real, end_imag = lax.fori_loop(0, steps, advance, (one, jnp.zeros_like(one)))
    real, imag = (end_real[0:1], end_imag[0:1])
    for c in range(1, CHUNKS):
        real, imag = complex_product(real, imag, end_real[c : c + 1], end_imag[c : c + 1])
    total_ref[...] = jnp.concatenate([real, imag], axis=0)


def local_kernel(normed_ref, w_ref, perm_ref, couple_ref, bar_ref, hold_ref, cum_ref, chan_ref, local_ref, end_ref, push_ref):
    fs, sp = w_ref.shape[:2]
    w = jnp.concatenate([w_ref[f, z] for z in range(sp) for f in range(fs)], axis=0)
    state_in = jnp.dot(normed_ref[...], w, preferred_element_type=F32).astype(BF16)
    chan = jnp.dot(perm_ref[...], state_in, preferred_element_type=F32).astype(BF16)
    chan_ref[...] = chan
    flat = bar_ref.shape[2]
    drive = jnp.dot(chan, couple_ref[0], preferred_element_type=F32) + jnp.dot(
        chan, couple_ref[1], preferred_element_type=F32
    )
    push_real, push_imag = complex_product(hold_ref[0], hold_ref[1], drive[:, :flat], drive[:, flat:])
    push_ref[0] = push_real
    push_ref[1] = push_imag
    steps = bar_ref.shape[1] // CHUNKS

    def advance(j, carry):
        rows = pl.ds(pl.multiple_of(j * CHUNKS, CHUNKS), CHUNKS)
        real, imag = complex_product(bar_ref[0, rows, :], bar_ref[1, rows, :], carry[0], carry[1])
        real = real + push_ref[0, rows, :]
        imag = imag + push_ref[1, rows, :]
        local_ref[0, rows, :] = real
        local_ref[1, rows, :] = imag
        return (real, imag)

    zero = jnp.zeros((CHUNKS, flat), F32)
    last_real, last_imag = lax.fori_loop(0, steps, advance, (zero, zero), unroll=4)
    tail = pl.ds((steps - 1) * CHUNKS, CHUNKS)
    end_real, end_imag = (cum_ref[0, tail, :], cum_ref[1, tail, :])
    real, imag = (last_real[0:1], last_imag[0:1])
    for c in range(1, CHUNKS):
        moved_real, moved_imag = complex_product(end_real[c : c + 1], end_imag[c : c + 1], real, imag)
        real = moved_real + last_real[c : c + 1]
        imag = moved_imag + last_imag[c : c + 1]
    end_ref[...] = jnp.concatenate([real, imag], axis=0)


def gelu(v):
    return 0.5 * v * (1.0 + jnp.tanh(0.7978845608 * (v + 0.044715 * v * v * v)))


def halves(x):
    high = x.astype(BF16)
    return high, (x - high.astype(F32)).astype(BF16)


def read_kernel(
    where_ref, maps_ref, ends_ref, initial_ref, local_ref, cum_ref, chan_ref, perm_ref, read_ref, skip_ref, mix_ref, closing_ref
):
    spans = maps_ref.shape[0]
    here = where_ref[0]
    real, imag = (initial_ref[0:1], initial_ref[1:2])
    enter_real, enter_imag = (real, imag)
    for z in range(spans):
        now = here == z
        enter_real = jnp.where(now, real, enter_real)
        enter_imag = jnp.where(now, imag, enter_imag)
        moved_real, moved_imag = complex_product(maps_ref[z, 0:1], maps_ref[z, 1:2], real, imag)
        real = moved_real + ends_ref[z, 0:1]
        imag = moved_imag + ends_ref[z, 1:2]
    closing_ref[...] = jnp.concatenate([real, imag], axis=0)
    rows = local_ref.shape[1]
    flat = local_ref.shape[2]
    steps = rows // CHUNKS
    tail = pl.ds((steps - 1) * CHUNKS, CHUNKS)
    end_real, end_imag = (cum_ref[0, tail, :], cum_ref[1, tail, :])
    last_real, last_imag = (local_ref[0, tail, :], local_ref[1, tail, :])
    in_real, in_imag = ([enter_real], [enter_imag])
    for c in range(CHUNKS - 1):
        moved_real, moved_imag = complex_product(
            end_real[c : c + 1], end_imag[c : c + 1], in_real[-1], in_imag[-1]
        )
        in_real.append(moved_real + last_real[c : c + 1])
        in_imag.append(moved_imag + last_imag[c : c + 1])
    entry_real = jnp.concatenate(in_real, axis=0)[None]
    entry_imag = jnp.concatenate(in_imag, axis=0)[None]
    shape = (steps, CHUNKS, flat)
    moved_real, moved_imag = complex_product(
        cum_ref[0].reshape(shape), cum_ref[1].reshape(shape), entry_real, entry_imag
    )
    hidden_real = local_ref[0] + moved_real.reshape(rows, flat)
    hidden_imag = local_ref[1] + moved_imag.reshape(rows, flat)

    def contract(x, at):
        high, low = halves(x)
        first = jnp.dot(high, read_ref[0, at], preferred_element_type=F32)
        second = jnp.dot(low, read_ref[0, at], preferred_element_type=F32)
        return first + (second + jnp.dot(high, read_ref[1, at], preferred_element_type=F32))

    response = contract(hidden_real, 0) + contract(hidden_imag, 1)
    response = response + skip_ref[...] * chan_ref[...].astype(F32)
    mixed = gelu(response).astype(BF16)
    mix_ref[...] = jnp.dot(perm_ref[...], mixed, preferred_element_type=F32).astype(BF16)


def conv_kernel(normed_ref, halo_ref, w_ref, taps_ref, mix_ref):
    fs, sp = w_ref.shape[:2]
    width = taps_ref.shape[1]
    rows = normed_ref.shape[0]
    w = jnp.concatenate([w_ref[f, z] for z in range(sp) for f in range(fs)], axis=0)
    reach = taps_ref.shape[0] - 1
    here = jnp.dot(normed_ref[...], w, preferred_element_type=F32).astype(BF16).astype(F32)
    before = jnp.dot(halo_ref[...], w[:, : 2 * width], preferred_element_type=F32).astype(BF16).astype(F32)
    gated = (here[:, :width] * here[:, width : 2 * width]).astype(BF16).astype(F32)
    gated_before = (before[:, :width] * before[:, width:]).astype(BF16).astype(F32)
    extended = jnp.concatenate([gated_before, gated], axis=0)
    filtered = taps_ref[reach : reach + 1] * gated
    for tap in range(reach):
        at = HALO - reach + tap
        filtered = filtered + taps_ref[tap : tap + 1] * extended[at : at + rows]
    mix_ref[...] = (here[:, 2 * width :] * filtered).astype(BF16)


def call(kernel, out_shape, flops, *args, scratch=(), smem=0, name=None):
    in_specs = [pl.BlockSpec(memory_space=pltpu.SMEM)] * smem + [
        pl.BlockSpec(memory_space=pltpu.VMEM)
    ] * (len(args) - smem)
    out_specs = jax.tree.map(lambda _: pl.BlockSpec(memory_space=pltpu.VMEM), out_shape)
    return pl.pallas_call(
        kernel,
        out_shape=out_shape,
        in_specs=in_specs,
        out_specs=out_specs,
        scratch_shapes=list(scratch),
        cost_estimate=pl.CostEstimate(flops=flops, bytes_accessed=1 << 20, transcendentals=0),
        name=name,
    )(*args)


def shape(dims, dtype=F32):
    return jax.ShapeDtypeStruct(dims, dtype)


def block_diagonal(blocks):
    groups, rows, columns = blocks.shape
    eye = jnp.eye(groups, dtype=bool)[:, None, :, None]
    return jnp.where(eye, blocks[:, :, None, :], 0.0).reshape(groups * rows, groups * columns)


def body(
    tokens,
    norm_gain,
    w_state_in,
    w_value,
    w_outer,
    w_inner,
    w_state_out,
    w_conv_out,
    log_step,
    decay_real,
    frequency,
    step_rate,
    input_real,
    input_imag,
    read_real,
    read_imag,
    skip_gain,
    conv_taps,
    initial_state,
):
    rows, features = tokens.shape[1:]
    groups, states = decay_real.shape
    group = skip_gain.shape[1]
    flat = groups * states
    width = groups * group
    steps = rows // CHUNKS

    state_shards = spread(w_state_in, "sp")
    conv_shards = spread(jnp.concatenate([w_value, w_inner, w_outer], axis=1), "sp")
    out_shards = spread(jnp.concatenate([w_state_out, w_conv_out], axis=1), "sp")

    count = lax.axis_size("sp")
    edge = lax.ppermute(tokens[0, rows - HALO :], "sp", [(i, i + 1) for i in range(count - 1)])
    gain = norm_gain[None]
    normed = call(normed_kernel, shape((rows, features), BF16), 1 << 22, tokens[0], gain, name="norm")
    halo = call(normed_kernel, shape((HALO, features), BF16), 1 << 18, edge, gain, name="halo")

    rate = step_rate[0].reshape(CHUNKS, steps).T.reshape(rows, 1)
    scale = jnp.repeat(log_step, states)[None]
    bar, hold, cum, total = call(
        maps_kernel,
        (shape((2, rows, flat)), shape((2, rows, flat)), shape((2, rows, flat)), shape((2, flat))),
        1 << 27,
        rate,
        scale,
        decay_real.reshape(1, flat),
        frequency.reshape(1, flat),
        name="maps",
    )
    maps = spread(total, "sp")

    index = jnp.arange(rows)
    source = (index % CHUNKS) * steps + index // CHUNKS
    permute = (source[:, None] == index[None, :]).astype(BF16)
    coupling = jnp.concatenate(
        [
            block_diagonal(jnp.swapaxes(input_real, 1, 2)),
            block_diagonal(jnp.swapaxes(input_imag, 1, 2)),
        ],
        axis=1,
    )
    coupling = jnp.stack(halves(coupling))
    reading = jnp.stack(
        [
            block_diagonal(jnp.swapaxes(read_real, 1, 2)),
            block_diagonal(-jnp.swapaxes(read_imag, 1, 2)),
        ]
    )
    reading = jnp.stack(halves(reading))

    state_weights = spread(state_shards, "fs")
    chan, local, end = call(
        local_kernel,
        (shape((rows, width), BF16), shape((2, rows, flat)), shape((2, flat))),
        1 << 28,
        normed,
        state_weights,
        permute,
        coupling,
        bar,
        hold,
        cum,
        scratch=(pltpu.VMEM((2, rows, flat), F32),),
        name="local",
    )
    ends = spread(end, "sp")
    conv_weights = spread(conv_shards, "fs")
    conv_mix = call(
        conv_kernel,
        shape((rows, width), BF16),
        1 << 29,
        normed,
        halo,
        conv_weights,
        conv_taps,
        name="conv",
    )
    state_mix, closing = call(
        read_kernel,
        (shape((rows, width), BF16), shape((2, flat))),
        1 << 28,
        lax.axis_index("sp").astype(jnp.int32)[None],
        maps,
        ends,
        initial_state[0].reshape(2, flat),
        local,
        cum,
        chan,
        permute.T,
        reading,
        skip_gain.reshape(1, width),
        smem=1,
        name="read",
    )
    out_weights = spread(out_shards, "fs")
    fs, sp = out_weights.shape[:2]
    out_weights = jnp.swapaxes(out_weights, 0, 1).reshape(features, 2 * width)
    mixes = jnp.concatenate([state_mix, conv_mix], axis=1)
    partial = jnp.einsum("rc,dc->rd", mixes, out_weights, preferred_element_type=F32).astype(BF16)
    tp = lax.axis_size("tp")
    parts = lax.all_to_all(partial.reshape(tp, rows // tp, features), "tp", 0, 0, tiled=True)
    mixed = jnp.sum(parts.astype(F32), axis=0).astype(BF16)
    share = states // count
    grid = closing.reshape(2, groups, states)
    own_share = lax.dynamic_slice_in_dim(grid, lax.axis_index("sp") * share, share, 2)
    return (mixed[None], own_share[None])


def solution(mesh):
    return jax.shard_map(
        body,
        mesh=mesh,
        in_specs=(
            P("fs", "sp", None),
            P(),
            P(("sp", "fs"), "tp"),
            P(("sp", "fs"), "tp"),
            P(("sp", "fs"), "tp"),
            P(("sp", "fs"), "tp"),
            P(("sp", "fs"), "tp"),
            P(("sp", "fs"), "tp"),
            P("tp"),
            P("tp", None),
            P("tp", None),
            P("fs", "sp"),
            P("tp", None, None),
            P("tp", None, None),
            P("tp", None, None),
            P("tp", None, None),
            P("tp", None),
            P(None, "tp"),
            P("fs", None, "tp", None),
        ),
        out_specs=(P("fs", ("sp", "tp"), None), P("fs", None, "tp", "sp")),
        check_vma=False,
    )
```

```python
import jax
import jax.numpy as jnp
from jax import lax
from jax.experimental import pallas as pl
from jax.experimental.pallas import tpu as pltpu
from jax.sharding import PartitionSpec as P


F32 = jnp.float32
BF16 = jnp.bfloat16
CHUNKS = 8
HALO = 16
NT = (((1,), (1,)), ((), ()))


def spread(x, axis):
    copies = lax.axis_size(axis)
    many = jnp.broadcast_to(x[None], (copies, *x.shape))
    return lax.all_to_all(many, axis, 0, 0, tiled=True)


def complex_product(left_real, left_imag, right_real, right_imag):
    return (
        left_real * right_real - left_imag * right_imag,
        left_real * right_imag + left_imag * right_real,
    )


def sine_cosine(angle):
    turns = jnp.floor(angle * 0.6366197723675814 + 0.5)
    r = angle - turns * 1.5703125
    r = r - turns * 4.837512969970703e-4
    r = r - turns * 7.549789948768648e-8
    r2 = r * r
    sine = r + r * r2 * (-1.6666654611e-1 + r2 * (8.3321608736e-3 + r2 * -1.9515295891e-4))
    cosine = (
        1.0
        - 0.5 * r2
        + r2 * r2 * (4.166664568298827e-2 + r2 * (-1.388731625493765e-3 + r2 * 2.443315711809948e-5))
    )
    quadrant = turns.astype(jnp.int32)
    odd = (quadrant & 1) == 1
    flip_sine = (quadrant & 2) == 2
    flip_cosine = ((quadrant + 1) & 2) == 2
    base_sine = jnp.where(odd, cosine, sine)
    base_cosine = jnp.where(odd, sine, cosine)
    return (
        jnp.where(flip_sine, -base_sine, base_sine),
        jnp.where(flip_cosine, -base_cosine, base_cosine),
    )


def iota(dims, axis):
    return lax.broadcasted_iota(jnp.int32, dims, axis)


def pieces(x, count):
    found = []
    for _ in range(count):
        part = x.astype(BF16)
        found.append(part)
        x = x - part.astype(F32)
    return found


def picked(x, selector, count=3):
    total = None
    for part in pieces(x, count):
        term = jnp.dot(part, selector, preferred_element_type=F32)
        total = term if total is None else total + term
    return total


def repeat_selector(narrow, wide):
    return (iota((narrow, wide), 1) % narrow == iota((narrow, wide), 0)).astype(BF16)


def flattened(x, groups):
    rows, narrow = x.shape
    wide = groups * narrow
    tiled = picked(x, repeat_selector(narrow, wide))
    own = iota((rows, wide), 1) // narrow == iota((rows, wide), 0) % groups
    tiled = jnp.where(own, tiled, 0.0)
    return [jnp.sum(tiled[at : at + groups], axis=0, keepdims=True) for at in range(0, rows, groups)]


def block_diagonal(x, groups):
    rows, narrow = x.shape
    wide = groups * narrow
    selector = repeat_selector(narrow, wide)
    own = iota((rows, wide), 1) // narrow == iota((rows, wide), 0) // (rows // groups)
    return [
        jnp.where(own, jnp.dot(part, selector, preferred_element_type=F32), 0.0).astype(BF16)
        for part in pieces(x, 2)
    ]


def spread_steps(log_ref, groups, states):
    lane = iota((1, groups * states), 1) // states
    out = jnp.zeros((1, groups * states), F32)
    for g in range(groups):
        out = jnp.where(lane == g, log_ref[g], out)
    return jnp.exp(out)


def chunk_order(rows, flip):
    r, c = (iota((rows, rows), 1 if flip else 0), iota((rows, rows), 0 if flip else 1))
    steps = rows // CHUNKS
    return (c == (r % CHUNKS) * steps + r // CHUNKS).astype(BF16)


def normalized(x, gain):
    x = x.astype(F32)
    mean_square = jnp.mean(x * x, axis=-1, keepdims=True)
    return (x * lax.rsqrt(mean_square + 1e-06) * gain).astype(BF16)


def prep_kernel(
    log_ref, tokens_ref, gain_ref, rate_ref, decay_ref, freq_ref, in_real_ref, in_imag_ref, out_real_ref, out_imag_ref,
    normed_ref, bar_ref, hold_ref, cum_ref, couple_ref, read_ref, column_ref,
):
    groups, states = decay_ref.shape
    flat = groups * states
    rows = tokens_ref.shape[0]
    part = 64

    def norm(i, _):
        at = pl.ds(pl.multiple_of(i * part, part), part)
        normed_ref[at, :] = normalized(tokens_ref[at, :], gain_ref[...])
        return 0

    lax.fori_loop(0, rows // part, norm, 0)
    order = chunk_order(rows, False)
    column = None
    for piece in pieces(jnp.broadcast_to(rate_ref[...], (16, rows)), 3):
        term = lax.dot_general(order, piece, NT, preferred_element_type=F32)
        column = term if column is None else column + term
    column_ref[...] = column
    (decay,) = flattened(decay_ref[...], groups)
    (freq,) = flattened(freq_ref[...], groups)
    scale = spread_steps(log_ref, groups, states)
    inverse = 1.0 / (decay * decay + freq * freq)
    steps = rows // CHUNKS

    def advance(j, carry):
        cum_real, cum_imag = carry
        at = pl.ds(pl.multiple_of(j * CHUNKS, CHUNKS), CHUNKS)
        step = column_ref[at, 0:1] * scale
        grow = jnp.exp(step * decay)
        sine, cosine = sine_cosine(step * freq)
        bar_real, bar_imag = (grow * cosine, grow * sine)
        less_real = bar_real - 1.0
        bar_ref[0, at, :] = bar_real
        bar_ref[1, at, :] = bar_imag
        hold_ref[0, at, :] = (less_real * decay + bar_imag * freq) * inverse
        hold_ref[1, at, :] = (bar_imag * decay - less_real * freq) * inverse
        cum_real, cum_imag = complex_product(cum_real, cum_imag, bar_real, bar_imag)
        cum_ref[0, at, :] = cum_real
        cum_ref[1, at, :] = cum_imag
        return (cum_real, cum_imag)

    one = jnp.ones((CHUNKS, flat), F32)
    lax.fori_loop(0, steps, advance, (one, jnp.zeros_like(one)))
    for at, ref in enumerate((in_real_ref, in_imag_ref)):
        high, low = block_diagonal(ref[...], groups)
        couple_ref[0, :, at * flat : (at + 1) * flat] = high
        couple_ref[1, :, at * flat : (at + 1) * flat] = low
    for at, (ref, sign) in enumerate(((out_real_ref, 1.0), (out_imag_ref, -1.0))):
        high, low = block_diagonal(ref[...] * sign, groups)
        read_ref[0, :, at * flat : (at + 1) * flat] = high
        read_ref[1, :, at * flat : (at + 1) * flat] = low


def gathered_rows(ref):
    fs, sp = ref.shape[:2]
    return jnp.concatenate([ref[f, z] for z in range(sp) for f in range(fs)], axis=0)


def local_kernel(normed_ref, w_ref, couple_ref, bar_ref, hold_ref, cum_ref, rate_ref, chan_ref, local_ref, end_ref, push_ref):
    rows = normed_ref.shape[0]
    w = gathered_rows(w_ref)
    state_in = jnp.dot(normed_ref[...], w, preferred_element_type=F32).astype(BF16)
    chan = jnp.dot(chunk_order(rows, False), state_in, preferred_element_type=F32).astype(BF16)
    chan_ref[...] = chan
    flat = bar_ref.shape[2]
    drive = jnp.dot(chan, couple_ref[0], preferred_element_type=F32) + jnp.dot(
        chan, couple_ref[1], preferred_element_type=F32
    )
    push_real, push_imag = complex_product(hold_ref[0], hold_ref[1], drive[:, :flat], drive[:, flat:])
    push_ref[0] = push_real
    push_ref[1] = push_imag
    steps = rows // CHUNKS

    def advance(j, carry):
        at = pl.ds(pl.multiple_of(j * CHUNKS, CHUNKS), CHUNKS)
        real, imag = complex_product(bar_ref[0, at, :], bar_ref[1, at, :], carry[0], carry[1])
        real = real + push_ref[0, at, :]
        imag = imag + push_ref[1, at, :]
        local_ref[0, at, :] = real
        local_ref[1, at, :] = imag
        return (real, imag)

    zero = jnp.zeros((CHUNKS, flat), F32)
    last_real, last_imag = lax.fori_loop(0, steps, advance, (zero, zero), unroll=4)
    tail = pl.ds((steps - 1) * CHUNKS, CHUNKS)
    end_real, end_imag = (cum_ref[0, tail, :], cum_ref[1, tail, :])
    real, imag = (last_real[0:1], last_imag[0:1])
    for c in range(1, CHUNKS):
        moved_real, moved_imag = complex_product(end_real[c : c + 1], end_imag[c : c + 1], real, imag)
        real = moved_real + last_real[c : c + 1]
        imag = moved_imag + last_imag[c : c + 1]
    end_ref[:, :flat] = jnp.concatenate([real, imag], axis=0)
    whole = jnp.sum(rate_ref[...], axis=1, keepdims=True)
    end_ref[:, flat:] = jnp.broadcast_to(whole, (2, end_ref.shape[1] - flat))


def gelu(v):
    return 0.5 * v * (1.0 + jnp.tanh(0.7978845608 * (v + 0.044715 * v * v * v)))


def read_kernel(
    where_ref, log_ref, ends_ref, decay_ref, freq_ref, initial_ref, local_ref, cum_ref, chan_ref, read_ref, skip_ref,
    mix_ref, closing_ref,
):
    groups, states = decay_ref.shape
    flat = groups * states
    spans = ends_ref.shape[0]
    here = where_ref[0]
    scale = spread_steps(log_ref, groups, states)
    (decay,) = flattened(decay_ref[...], groups)
    (freq,) = flattened(freq_ref[...], groups)
    enter_real, enter_imag = flattened(initial_ref[...], groups)
    real, imag = (enter_real, enter_imag)
    elapsed = jnp.concatenate([ends_ref[z, 0:1, flat:] for z in range(spans)], axis=0)[:, 0:1] * scale
    grow = jnp.exp(elapsed * decay)
    sine, cosine = sine_cosine(elapsed * freq)
    map_real, map_imag = (grow * cosine, grow * sine)
    for z in range(spans):
        now = here == z
        enter_real = jnp.where(now, real, enter_real)
        enter_imag = jnp.where(now, imag, enter_imag)
        moved_real, moved_imag = complex_product(map_real[z : z + 1], map_imag[z : z + 1], real, imag)
        real = moved_real + ends_ref[z, 0:1, :flat]
        imag = moved_imag + ends_ref[z, 1:2, :flat]
    share = states // spans
    lane = iota((flat, share), 0) % states
    wanted = (lane == here * share + iota((flat, share), 1)).astype(BF16)
    own = iota((groups, flat), 1) // states == iota((groups, flat), 0)
    for at, row in enumerate((real, imag)):
        closing_ref[at] = picked(jnp.where(own, jnp.broadcast_to(row, (groups, flat)), 0.0), wanted)
    rows = local_ref.shape[1]
    steps = rows // CHUNKS
    tail = pl.ds((steps - 1) * CHUNKS, CHUNKS)
    end_real, end_imag = (cum_ref[0, tail, :], cum_ref[1, tail, :])
    last_real, last_imag = (local_ref[0, tail, :], local_ref[1, tail, :])
    in_real, in_imag = ([enter_real], [enter_imag])
    for c in range(CHUNKS - 1):
        moved_real, moved_imag = complex_product(
            end_real[c : c + 1], end_imag[c : c + 1], in_real[-1], in_imag[-1]
        )
        in_real.append(moved_real + last_real[c : c + 1])
        in_imag.append(moved_imag + last_imag[c : c + 1])
    entry_real = jnp.concatenate(in_real, axis=0)[None]
    entry_imag = jnp.concatenate(in_imag, axis=0)[None]
    shape = (steps, CHUNKS, flat)
    moved_real, moved_imag = complex_product(
        cum_ref[0].reshape(shape), cum_ref[1].reshape(shape), entry_real, entry_imag
    )
    hidden_real = local_ref[0] + moved_real.reshape(rows, flat)
    hidden_imag = local_ref[1] + moved_imag.reshape(rows, flat)
    response = None
    for at, hidden in enumerate((hidden_real, hidden_imag)):
        high, low = pieces(hidden, 2)
        lanes = pl.ds(at * flat, flat)
        for left, right in ((high, 0), (low, 0), (high, 1)):
            term = lax.dot_general(left, read_ref[right, :, lanes], NT, preferred_element_type=F32)
            response = term if response is None else response + term
    (skip,) = flattened(skip_ref[...], groups)
    mixed = gelu(response + skip * chan_ref[...].astype(F32)).astype(BF16)
    mix_ref[...] = jnp.dot(chunk_order(rows, True), mixed, preferred_element_type=F32).astype(BF16)


def conv_kernel(
    place_ref, normed_ref, halo_ref, gain_ref, own_ref, up_ref, down_ref, left_ref, right_ref, taps_ref,
    mix_ref, weights_ref, w_ref,
):
    width = taps_ref.shape[1]
    rows = normed_ref.shape[0]
    spans, tall, wide = own_ref.shape
    half = left_ref.shape[2]
    split = w_ref.shape[1]
    z, y = (place_ref[0], place_ref[1])

    def placed(dz, turn):
        at_z = (z + dz) & (spans - 1)
        at_y = (y + 2 * dz + turn) & 3
        return pl.ds(pl.multiple_of((at_z * 4 + at_y) * tall, tall), tall)

    def put(at, lanes, piece):
        start, stop = lanes
        if start < split:
            w_ref[at, start : min(stop, split)] = piece[:, : min(stop, split) - start]
        if stop > split:
            begin = max(start, split)
            weights_ref[at, begin - split : stop - split] = piece[:, begin - start :]

    for dz in range(spans):
        put(placed(dz, 0), (0, wide), own_ref[dz])
        put(placed(dz, 1), (0, wide), up_ref[dz])
        put(placed(dz, 3), (0, wide), down_ref[dz])
        put(placed(dz + 1, 2), (0, half), left_ref[dz])
        put(placed(dz - 1, 2), (half, wide), right_ref[dz])
    w = w_ref[...]
    reach = taps_ref.shape[0] - 1
    here = jnp.dot(normed_ref[...], w, preferred_element_type=F32).astype(BF16).astype(F32)
    halo = normalized(halo_ref[...], gain_ref[...])
    before = jnp.dot(halo, w[:, : 2 * width], preferred_element_type=F32).astype(BF16).astype(F32)
    gated = (here[:, :width] * here[:, width : 2 * width]).astype(BF16).astype(F32)
    gated_before = (before[:, :width] * before[:, width:]).astype(BF16).astype(F32)
    extended = jnp.concatenate([gated_before, gated], axis=0)
    filtered = taps_ref[reach : reach + 1] * gated
    for tap in range(reach):
        at = HALO - reach + tap
        filtered = filtered + taps_ref[tap : tap + 1] * extended[at : at + rows]
    mix_ref[...] = (here[:, 2 * width :] * filtered).astype(BF16)


def out_kernel(state_ref, conv_ref, w_ref, out_ref):
    mixes = jnp.concatenate([state_ref[...], conv_ref[...]], axis=1)
    per = 512
    for at in range(0, w_ref.shape[0], per):
        product = lax.dot_general(mixes, w_ref[at : at + per], NT, preferred_element_type=F32)
        out_ref[:, at : at + per] = product.astype(BF16)


def moved(x, dz, dy):
    sp, fs = (lax.axis_size("sp"), lax.axis_size("fs"))
    pairs = [
        (z * fs + y, ((z - dz) % sp) * fs + (y - dy) % fs) for z in range(sp) for y in range(fs)
    ]
    return lax.ppermute(x, ("sp", "fs"), pairs)


def all_shards(x):
    far = [x] + [moved(x, dz, 0) for dz in (4, 8, 12)]
    far = jnp.stack(far)
    near = [far] + [moved(far, dz, dy) for dz, dy in ((1, 2), (2, 0), (-1, 2))]
    near[3] = jnp.roll(near[3], -1, axis=0)
    near = jnp.stack(near, axis=1)
    own = near.reshape(-1, *x.shape)
    half = x.shape[1] // 2 // 128 * 128
    return (
        own,
        moved(own, 0, 1),
        moved(own, 0, -1),
        moved(own[:, :, :half], 1, 0),
        moved(own[:, :, half:], -1, 0),
    )


def call(kernel, out_shape, flops, *args, scratch=(), smem=0):
    in_specs = [pl.BlockSpec(memory_space=pltpu.SMEM)] * smem + [
        pl.BlockSpec(memory_space=pltpu.VMEM)
    ] * (len(args) - smem)
    out_specs = jax.tree.map(lambda _: pl.BlockSpec(memory_space=pltpu.VMEM), out_shape)
    return pl.pallas_call(
        kernel,
        out_shape=out_shape,
        in_specs=in_specs,
        out_specs=out_specs,
        scratch_shapes=list(scratch),
        cost_estimate=pl.CostEstimate(flops=flops, bytes_accessed=1 << 20, transcendentals=0),
        compiler_params=pltpu.CompilerParams(vmem_limit_bytes=20 << 20),
    )(*args)


def shape(dims, dtype=F32):
    return jax.ShapeDtypeStruct(dims, dtype)


def body(
    tokens,
    norm_gain,
    w_state_in,
    w_value,
    w_outer,
    w_inner,
    w_state_out,
    w_conv_out,
    log_step,
    decay_real,
    frequency,
    step_rate,
    input_real,
    input_imag,
    read_real,
    read_imag,
    skip_gain,
    conv_taps,
    initial_state,
):
    rows, features = tokens.shape[1:]
    groups, states = decay_real.shape
    group = skip_gain.shape[1]
    flat = groups * states
    width = groups * group
    count = lax.axis_size("sp")

    state_shards = spread(w_state_in, "sp")
    own, up, down, left, right = all_shards(
        jnp.concatenate([w_value, w_inner, w_outer, w_state_out, w_conv_out], axis=1)
    )
    edge = lax.ppermute(tokens[0, rows - HALO :], "sp", [(i, i + 1) for i in range(count - 1)])
    gain = norm_gain[None]
    normed, bar, hold, cum, coupling, reading, _ = call(
        prep_kernel,
        (
            shape((rows, features), BF16),
            shape((2, rows, flat)),
            shape((2, rows, flat)),
            shape((2, rows, flat)),
            shape((2, width, 2 * flat), BF16),
            shape((2, width, 2 * flat), BF16),
            shape((rows, 16)),
        ),
        1 << 30,
        log_step,
        tokens[0],
        gain,
        step_rate,
        decay_real,
        frequency,
        jnp.swapaxes(input_real, 1, 2).reshape(width, states),
        jnp.swapaxes(input_imag, 1, 2).reshape(width, states),
        read_real.reshape(width, states),
        read_imag.reshape(width, states),
        smem=1,
    )
    state_weights = spread(state_shards, "fs")
    chan, local, end = call(
        local_kernel,
        (shape((rows, width), BF16), shape((2, rows, flat)), shape((2, flat + 128))),
        1 << 29,
        normed,
        state_weights,
        coupling,
        bar,
        hold,
        cum,
        step_rate,
        scratch=(pltpu.VMEM((2, rows, flat), F32),),
    )
    ends = spread(end, "sp")
    place = jnp.stack([lax.axis_index("sp"), lax.axis_index("fs")]).astype(jnp.int32)
    conv_mix, out_weights = call(
        conv_kernel,
        (shape((rows, width), BF16), shape((features, 2 * width), BF16)),
        1 << 29,
        place,
        normed,
        edge,
        gain,
        own,
        up,
        down,
        left,
        right,
        conv_taps,
        scratch=(pltpu.VMEM((features, 3 * width), BF16),),
        smem=1,
    )
    state_mix, closing = call(
        read_kernel,
        (shape((rows, width), BF16), shape((2, groups, states // count))),
        1 << 29,
        lax.axis_index("sp").astype(jnp.int32)[None],
        log_step,
        ends,
        decay_real,
        frequency,
        initial_state[0].reshape(2 * groups, states),
        local,
        cum,
        chan,
        reading,
        skip_gain,
        smem=2,
    )
    partial = call(
        out_kernel, shape((rows, features), BF16), 1 << 29, state_mix, conv_mix, out_weights
    )
    tp = lax.axis_size("tp")
    parts = lax.all_to_all(partial.reshape(tp, rows // tp, features), "tp", 0, 0, tiled=True)
    mixed = jnp.sum(parts.astype(F32), axis=0).astype(BF16)
    return (mixed[None], closing[None])


def solution(mesh):
    return jax.shard_map(
        body,
        mesh=mesh,
        in_specs=(
            P("fs", "sp", None),
            P(),
            P(("sp", "fs"), "tp"),
            P(("sp", "fs"), "tp"),
            P(("sp", "fs"), "tp"),
            P(("sp", "fs"), "tp"),
            P(("sp", "fs"), "tp"),
            P(("sp", "fs"), "tp"),
            P("tp"),
            P("tp", None),
            P("tp", None),
            P("fs", "sp"),
            P("tp", None, None),
            P("tp", None, None),
            P("tp", None, None),
            P("tp", None, None),
            P("tp", None),
            P(None, "tp"),
            P("fs", None, "tp", None),
        ),
        out_specs=(P("fs", ("sp", "tp"), None), P("fs", None, "tp", "sp")),
        check_vma=False,
    )
```

```python
import functools

import jax
import jax.numpy as jnp
from jax import lax
from jax.experimental import pallas as pl
from jax.experimental.pallas import tpu as pltpu
from jax.sharding import PartitionSpec as P


F32 = jnp.float32
BF16 = jnp.bfloat16
CHUNKS = 8
HALO = 16
PACKED = 16
NT = (((1,), (1,)), ((), ()))


def spread(x, axis, groups=None):
    copies = lax.axis_size(axis) if groups is None else len(groups[0])
    many = jnp.broadcast_to(x[None], (copies, *x.shape))
    return lax.all_to_all(many, axis, 0, 0, tiled=True, axis_index_groups=groups)


def complex_product(left_real, left_imag, right_real, right_imag):
    return (
        left_real * right_real - left_imag * right_imag,
        left_real * right_imag + left_imag * right_real,
    )


def sine_cosine(angle):
    turns = jnp.floor(angle * 0.6366197723675814 + 0.5)
    r = angle - turns * 1.5703125
    r = r - turns * 4.837512969970703e-4
    r = r - turns * 7.549789948768648e-8
    r2 = r * r
    sine = r + r * r2 * (-1.6666654611e-1 + r2 * (8.3321608736e-3 + r2 * -1.9515295891e-4))
    cosine = (
        1.0
        - 0.5 * r2
        + r2 * r2 * (4.166664568298827e-2 + r2 * (-1.388731625493765e-3 + r2 * 2.443315711809948e-5))
    )
    quadrant = turns.astype(jnp.int32)
    odd = (quadrant & 1) == 1
    flip_sine = (quadrant & 2) == 2
    flip_cosine = ((quadrant + 1) & 2) == 2
    base_sine = jnp.where(odd, cosine, sine)
    base_cosine = jnp.where(odd, sine, cosine)
    return (
        jnp.where(flip_sine, -base_sine, base_sine),
        jnp.where(flip_cosine, -base_cosine, base_cosine),
    )


def iota(dims, axis):
    return lax.broadcasted_iota(jnp.int32, dims, axis)


def pieces(x, count):
    found = []
    for _ in range(count):
        part = x.astype(BF16)
        found.append(part)
        x = x - part.astype(F32)
    return found


def picked(x, selector, count=3):
    total = None
    for part in pieces(x, count):
        term = jnp.dot(part, selector, preferred_element_type=F32)
        total = term if total is None else total + term
    return total


def repeat_selector(narrow, wide):
    return (iota((narrow, wide), 1) % narrow == iota((narrow, wide), 0)).astype(BF16)


def flattened(x, groups):
    rows, narrow = x.shape
    wide = groups * narrow
    tiled = picked(x, repeat_selector(narrow, wide))
    own = iota((rows, wide), 1) // narrow == iota((rows, wide), 0) % groups
    tiled = jnp.where(own, tiled, 0.0)
    return [jnp.sum(tiled[at : at + groups], axis=0, keepdims=True) for at in range(0, rows, groups)]


def block_diagonal(x, groups):
    rows, narrow = x.shape
    wide = groups * narrow
    selector = repeat_selector(narrow, wide)
    own = iota((rows, wide), 1) // narrow == iota((rows, wide), 0) // (rows // groups)
    return [
        jnp.where(own, jnp.dot(part, selector, preferred_element_type=F32), 0.0).astype(BF16)
        for part in pieces(x, 2)
    ]


def spread_steps(log_ref, groups, states):
    lane = iota((1, groups * states), 1) // states
    out = jnp.zeros((1, groups * states), F32)
    for g in range(groups):
        out = jnp.where(lane == g, log_ref[g], out)
    return jnp.exp(out)


def chunk_order(rows, flip):
    r, c = (iota((rows, rows), 1 if flip else 0), iota((rows, rows), 0 if flip else 1))
    steps = rows // CHUNKS
    return (c == (r % CHUNKS) * steps + r // CHUNKS).astype(BF16)


def normalized(x, gain):
    x = x.astype(F32)
    mean_square = jnp.mean(x * x, axis=-1, keepdims=True)
    return (x * lax.rsqrt(mean_square + 1e-06) * gain).astype(BF16)


def prep_kernel(
    log_ref, tokens_ref, gain_ref, rate_ref, decay_ref, freq_ref, initial_ref, in_real_ref, in_imag_ref,
    out_real_ref, out_imag_ref, skip_ref, taps_ref, normed_ref, bar_ref, pack_ref, column_ref,
):
    groups, states = decay_ref.shape
    flat = groups * states
    rows = tokens_ref.shape[0]
    part = 64

    def norm(i, _):
        at = pl.ds(pl.multiple_of(i * part, part), part)
        normed_ref[at, :] = normalized(tokens_ref[at, :], gain_ref[...])
        return 0

    lax.fori_loop(0, rows // part, norm, 0)
    order = chunk_order(rows, False)
    column = None
    for piece in pieces(jnp.broadcast_to(rate_ref[...], (16, rows)), 3):
        term = lax.dot_general(order, piece, NT, preferred_element_type=F32)
        column = term if column is None else column + term
    column_ref[...] = column
    (decay,) = flattened(decay_ref[...], groups)
    (freq,) = flattened(freq_ref[...], groups)
    scale = spread_steps(log_ref, groups, states)
    for at, ref in enumerate((in_real_ref, in_imag_ref, out_real_ref, out_imag_ref)):
        pack_ref[: ref.shape[0], at * states : (at + 1) * states] = ref[...]
    width = taps_ref.shape[1]
    (skip,) = flattened(skip_ref[...], groups)
    gain_rows = gain_ref.shape[1] // flat
    for at, row in enumerate(
        (
            decay,
            freq,
            scale,
            *flattened(initial_ref[...], groups),
            *(gain_ref[:, i * flat : (i + 1) * flat] for i in range(gain_rows)),
            skip,
            *(taps_ref[i : i + 1] for i in range(taps_ref.shape[0])),
        )
    ):
        pack_ref[width + at : width + at + 1, : row.shape[1]] = row
    steps = rows // CHUNKS

    def advance(j, carry):
        at = pl.ds(pl.multiple_of(j * CHUNKS, CHUNKS), CHUNKS)
        step = column_ref[at, 0:1] * scale
        grow = jnp.exp(step * decay)
        sine, cosine = sine_cosine(step * freq)
        bar_real, bar_imag = (grow * cosine, grow * sine)
        bar_ref[0, at, :] = bar_real
        bar_ref[1, at, :] = bar_imag
        return 0

    lax.fori_loop(0, steps, advance, 0)


def packed(pack_ref, at, wide=None):
    top = pack_ref.shape[0] - PACKED
    return pack_ref[top + at : top + at + 1, : pack_ref.shape[1] if wide is None else wide]


def matrix(pack_ref, at, states):
    return pack_ref[: pack_ref.shape[0] - PACKED, at * states : (at + 1) * states]


def driven(chan, pack_ref, bar_ref, groups, push_ref):
    flat = bar_ref.shape[2]
    drives = []
    for at in range(2):
        high, low = block_diagonal(matrix(pack_ref, at, flat // groups), groups)
        drives.append(
            jnp.dot(chan, high, preferred_element_type=F32) + jnp.dot(chan, low, preferred_element_type=F32)
        )
    decay, freq = (packed(pack_ref, 0), packed(pack_ref, 1))
    inverse = 1.0 / (decay * decay + freq * freq)
    bar_imag = bar_ref[1]
    less_real = bar_ref[0] - 1.0
    push_ref[0], push_ref[1] = complex_product(
        (less_real * decay + bar_imag * freq) * inverse,
        (bar_imag * decay - less_real * freq) * inverse,
        drives[0],
        drives[1],
    )


def scanned(bar_ref, push_ref, start):
    steps = bar_ref.shape[1] // CHUNKS

    def advance(j, carry):
        at = pl.ds(pl.multiple_of(j * CHUNKS, CHUNKS), CHUNKS)
        real, imag = complex_product(bar_ref[0, at, :], bar_ref[1, at, :], carry[0], carry[1])
        real = real + push_ref[0, at, :]
        imag = imag + push_ref[1, at, :]
        push_ref[0, at, :] = real
        push_ref[1, at, :] = imag
        return (real, imag)

    lax.fori_loop(0, steps, advance, start, unroll=4)


def chunk_maps(bar_ref, push_ref):
    steps, flat = (bar_ref.shape[1] // CHUNKS, bar_ref.shape[2])

    def advance(j, carry):
        at = pl.ds(pl.multiple_of(j * CHUNKS, CHUNKS), CHUNKS)
        bar = (bar_ref[0, at, :], bar_ref[1, at, :])
        product = complex_product(*bar, carry[0], carry[1])
        real, imag = complex_product(*bar, carry[2], carry[3])
        return (*product, real + push_ref[0, at, :], imag + push_ref[1, at, :])

    one, zero = (jnp.ones((CHUNKS, flat), F32), jnp.zeros((CHUNKS, flat), F32))
    return lax.fori_loop(0, steps, advance, (one, zero, zero, zero), unroll=4)


def local_kernel(
    groups, normed_ref, w_ref, bar_ref, pack_ref, rate_ref, chan_ref, end_ref, push_ref
):
    rows = normed_ref.shape[0]
    near, fs, far = w_ref.shape[:3]
    w = jnp.concatenate(
        [w_ref[zb, y, za] for za in range(far) for zb in range(near) for y in range(fs)], axis=0
    )
    state_in = jnp.dot(normed_ref[...], w, preferred_element_type=F32).astype(BF16)
    chan = jnp.dot(chunk_order(rows, False), state_in, preferred_element_type=F32).astype(BF16)
    chan_ref[...] = chan
    flat = bar_ref.shape[2]
    driven(chan, pack_ref, bar_ref, groups, push_ref)
    end_real, end_imag, last_real, last_imag = chunk_maps(bar_ref, push_ref)
    real, imag = (last_real[0:1], last_imag[0:1])
    for c in range(1, CHUNKS):
        moved_real, moved_imag = complex_product(end_real[c : c + 1], end_imag[c : c + 1], real, imag)
        real = moved_real + last_real[c : c + 1]
        imag = moved_imag + last_imag[c : c + 1]
    end_ref[:, :flat] = jnp.concatenate([real, imag], axis=0)
    whole = jnp.sum(rate_ref[...], axis=1, keepdims=True)
    end_ref[:, flat:] = jnp.broadcast_to(whole, (2, end_ref.shape[1] - flat))


def gelu(v):
    return 0.5 * v * (1.0 + jnp.tanh(0.7978845608 * (v + 0.044715 * v * v * v)))


def read_kernel(
    groups, ends_ref, bar_ref, chan_ref, pack_ref, mix_ref, closing_ref, push_ref
):
    flat = bar_ref.shape[2]
    states = flat // groups
    spans = ends_ref.shape[0]
    here = lax.axis_index("sp")
    decay, freq, scale, enter_real, enter_imag = (packed(pack_ref, at) for at in range(5))
    real, imag = (enter_real, enter_imag)
    elapsed = jnp.concatenate([ends_ref[z, 0:1, flat:] for z in range(spans)], axis=0)[:, 0:1] * scale
    grow = jnp.exp(elapsed * decay)
    sine, cosine = sine_cosine(elapsed * freq)
    map_real, map_imag = (grow * cosine, grow * sine)
    for z in range(spans):
        now = here == z
        enter_real = jnp.where(now, real, enter_real)
        enter_imag = jnp.where(now, imag, enter_imag)
        moved_real, moved_imag = complex_product(map_real[z : z + 1], map_imag[z : z + 1], real, imag)
        real = moved_real + ends_ref[z, 0:1, :flat]
        imag = moved_imag + ends_ref[z, 1:2, :flat]
    share = states // spans
    lane = iota((flat, share), 0) % states
    wanted = (lane == here * share + iota((flat, share), 1)).astype(BF16)
    own = iota((groups, flat), 1) // states == iota((groups, flat), 0)
    for at, row in enumerate((real, imag)):
        closing_ref[at] = picked(jnp.where(own, jnp.broadcast_to(row, (groups, flat)), 0.0), wanted)
    rows = bar_ref.shape[1]
    chan = chan_ref[...]
    driven(chan, pack_ref, bar_ref, groups, push_ref)
    end_real, end_imag, last_real, last_imag = chunk_maps(bar_ref, push_ref)
    in_real, in_imag = ([enter_real], [enter_imag])
    for c in range(CHUNKS - 1):
        moved_real, moved_imag = complex_product(
            end_real[c : c + 1], end_imag[c : c + 1], in_real[-1], in_imag[-1]
        )
        in_real.append(moved_real + last_real[c : c + 1])
        in_imag.append(moved_imag + last_imag[c : c + 1])
    scanned(bar_ref, push_ref, (jnp.concatenate(in_real, axis=0), jnp.concatenate(in_imag, axis=0)))
    response = None
    for at, sign in enumerate((1.0, -1.0)):
        weights = block_diagonal(matrix(pack_ref, 2 + at, states) * sign, groups)
        high, low = pieces(push_ref[at], 2)
        for left, right in ((high, 0), (low, 0), (high, 1)):
            term = lax.dot_general(left, weights[right], NT, preferred_element_type=F32)
            response = term if response is None else response + term
    skip = packed(pack_ref, 9, mix_ref.shape[1])
    mixed = gelu(response + skip * chan.astype(F32)).astype(BF16)
    mix_ref[...] = jnp.dot(chunk_order(rows, True), mixed, preferred_element_type=F32).astype(BF16)


def conv_kernel(
    normed_ref, halo_ref, own_ref, up_ref, down_ref, left_ref, right_ref, pack_ref, mix_ref, weights_ref, w_ref
):
    width = mix_ref.shape[1]
    rows = normed_ref.shape[0]
    near, far, tall, _ = own_ref.shape
    split = w_ref.shape[1]
    z, y = (lax.axis_index("sp"), lax.axis_index("fs"))

    def put(j, turn, ref, at_j):
        for k in range(far):
            at_z = 4 * k + ((z + j) & 3)
            at_y = (y + 2 * j + turn) & 3
            at = pl.ds(pl.multiple_of((at_z * 4 + at_y) * tall, tall), tall)
            w_ref[at, :] = ref[at_j, k, :, :split]
            weights_ref[at, :] = ref[at_j, k, :, split:]

    for j in range(near):
        put(j, 0, own_ref, j)
        put(j, 1, up_ref, j)
        put(j, 3, down_ref, j)
    for j in range(near // 2):
        put(j + 1, 2, left_ref, j)
        put(j - 1, 2, right_ref, j)
    w = w_ref[...]
    taps = [packed(pack_ref, 10 + at, width) for at in range(3)]
    gain = jnp.concatenate([packed(pack_ref, 5 + at) for at in range(4)], axis=1)
    reach = len(taps) - 1
    here = jnp.dot(normed_ref[...], w, preferred_element_type=F32).astype(BF16).astype(F32)
    halo = normalized(halo_ref[...], gain)
    before = jnp.dot(halo, w[:, : 2 * width], preferred_element_type=F32).astype(BF16).astype(F32)
    gated = (here[:, :width] * here[:, width : 2 * width]).astype(BF16).astype(F32)
    gated_before = (before[:, :width] * before[:, width:]).astype(BF16).astype(F32)
    extended = jnp.concatenate([gated_before, gated], axis=0)
    filtered = taps[reach] * gated
    for tap in range(reach):
        at = HALO - reach + tap
        filtered = filtered + taps[tap] * extended[at : at + rows]
    mix_ref[...] = (here[:, 2 * width :] * filtered).astype(BF16)


def out_kernel(state_ref, conv_ref, w_ref, out_ref):
    mixes = jnp.concatenate([state_ref[...], conv_ref[...]], axis=1)
    per = 512
    for at in range(0, w_ref.shape[0], per):
        product = lax.dot_general(mixes, w_ref[at : at + per], NT, preferred_element_type=F32)
        out_ref[:, at : at + per] = product.astype(BF16)


def moved(x, dz, dy):
    sp, fs = (lax.axis_size("sp"), lax.axis_size("fs"))
    pairs = [
        (z * fs + y, ((z - dz) % sp) * fs + (y - dy) % fs) for z in range(sp) for y in range(fs)
    ]
    return lax.ppermute(x, ("sp", "fs"), pairs)


def all_shards(far):
    near = [far] + [moved(far, dz, dy) for dz, dy in ((1, 2), (2, 0), (-1, 2))]
    own = jnp.stack(near)
    half = own[:2]
    return (own, moved(own, 0, 1), moved(own, 0, -1), moved(half, 1, 0), moved(half, -1, 0))


def call(kernel, out_shape, flops, *args, smem=0, scratch=()):
    vmem = pl.BlockSpec(memory_space=pltpu.VMEM)
    return pl.pallas_call(
        kernel,
        out_shape=out_shape,
        in_specs=[pl.BlockSpec(memory_space=pltpu.SMEM)] * smem + [vmem] * (len(args) - smem),
        out_specs=jax.tree.map(lambda _: vmem, out_shape),
        scratch_shapes=list(scratch),
        cost_estimate=pl.CostEstimate(flops=flops, bytes_accessed=1 << 20, transcendentals=0),
        compiler_params=pltpu.CompilerParams(vmem_limit_bytes=20 << 20),
    )(*args)


def shape(dims, dtype=F32):
    return jax.ShapeDtypeStruct(dims, dtype)


def body(
    tokens,
    norm_gain,
    w_state_in,
    w_value,
    w_outer,
    w_inner,
    w_state_out,
    w_conv_out,
    log_step,
    decay_real,
    frequency,
    step_rate,
    input_real,
    input_imag,
    read_real,
    read_imag,
    skip_gain,
    conv_taps,
    initial_state,
):
    rows, features = tokens.shape[1:]
    groups, states = decay_real.shape
    group = skip_gain.shape[1]
    flat = groups * states
    width = groups * group
    count = lax.axis_size("sp")

    fs = lax.axis_size("fs")
    shards = jnp.concatenate([w_state_in, w_value, w_inner, w_outer, w_state_out, w_conv_out], axis=1)
    apart = [[zb + 4 * za for za in range(count // 4)] for zb in range(4)]
    far = spread(shards, "sp", apart)
    block = 4 * fs
    blocks = [[at + i for i in range(block)] for at in range(0, count * fs, block)]
    state_weights = spread(far[:, :, :width], ("sp", "fs"), blocks)
    state_weights = state_weights.reshape(4, fs, *state_weights.shape[1:])
    own, up, down, left, right = all_shards(far[:, :, width:])
    edge = lax.ppermute(tokens[0, rows - HALO :], "sp", [(i, i + 1) for i in range(count - 1)])
    gain = norm_gain[None]
    into = [jnp.swapaxes(x, 1, 2).reshape(width, states) for x in (input_real, input_imag)]
    normed, bar, pack = call(
        prep_kernel,
        (shape((rows, features), BF16), shape((2, rows, flat)), shape((width + PACKED, flat))),
        1 << 30,
        log_step,
        tokens[0],
        gain,
        step_rate,
        decay_real,
        frequency,
        initial_state[0].reshape(2 * groups, states),
        *into,
        read_real.reshape(width, states),
        read_imag.reshape(width, states),
        skip_gain,
        conv_taps,
        smem=1,
        scratch=(pltpu.VMEM((rows, 16), F32),),
    )
    chan, end = call(
        functools.partial(local_kernel, groups),
        (shape((rows, width), BF16), shape((2, flat + 128))),
        1 << 29,
        normed,
        state_weights,
        bar,
        pack,
        step_rate,
        scratch=(pltpu.VMEM((2, rows, flat), F32),),
    )
    ends = spread(end, "sp")
    conv_mix, out_weights = call(
        conv_kernel,
        (shape((rows, width), BF16), shape((features, 2 * width), BF16)),
        1 << 29,
        normed,
        edge,
        own,
        up,
        down,
        left,
        right,
        pack,
        scratch=(pltpu.VMEM((features, 3 * width), BF16),),
    )
    state_mix, closing = call(
        functools.partial(read_kernel, groups),
        (shape((rows, width), BF16), shape((2, groups, states // count))),
        1 << 29,
        ends,
        bar,
        chan,
        pack,
        scratch=(pltpu.VMEM((2, rows, flat), F32),),
    )
    partial = call(
        out_kernel, shape((rows, features), BF16), 1 << 29, state_mix, conv_mix, out_weights
    )
    tp = lax.axis_size("tp")
    parts = lax.all_to_all(partial.reshape(tp, rows // tp, features), "tp", 0, 0, tiled=True)
    mixed = jnp.sum(parts.astype(F32), axis=0).astype(BF16)
    return (mixed[None], closing[None])


def solution(mesh):
    return jax.shard_map(
        body,
        mesh=mesh,
        in_specs=(
            P("fs", "sp", None),
            P(),
            P(("sp", "fs"), "tp"),
            P(("sp", "fs"), "tp"),
            P(("sp", "fs"), "tp"),
            P(("sp", "fs"), "tp"),
            P(("sp", "fs"), "tp"),
            P(("sp", "fs"), "tp"),
            P("tp"),
            P("tp", None),
            P("tp", None),
            P("fs", "sp"),
            P("tp", None, None),
            P("tp", None, None),
            P("tp", None, None),
            P("tp", None, None),
            P("tp", None),
            P(None, "tp"),
            P("fs", None, "tp", None),
        ),
        out_specs=(P("fs", ("sp", "tp"), None), P("fs", None, "tp", "sp")),
        check_vma=False,
    )
```

```python
import functools

import jax
import jax.numpy as jnp
from jax import lax
from jax.experimental import pallas as pl
from jax.experimental.pallas import tpu as pltpu
from jax.sharding import PartitionSpec as P


F32 = jnp.float32
BF16 = jnp.bfloat16
CHUNKS = 8
HALO = 16
PACKED = 16
NT = (((1,), (1,)), ((), ()))


def spread(x, axis):
    copies = lax.axis_size(axis)
    many = jnp.broadcast_to(x[None], (copies, *x.shape))
    return lax.all_to_all(many, axis, 0, 0, tiled=True)


def complex_product(left_real, left_imag, right_real, right_imag):
    return (
        left_real * right_real - left_imag * right_imag,
        left_real * right_imag + left_imag * right_real,
    )


def sine_cosine(angle):
    turns = jnp.floor(angle * 0.6366197723675814 + 0.5)
    r = angle - turns * 1.5703125
    r = r - turns * 4.837512969970703e-4
    r = r - turns * 7.549789948768648e-8
    r2 = r * r
    sine = r + r * r2 * (-1.6666654611e-1 + r2 * (8.3321608736e-3 + r2 * -1.9515295891e-4))
    cosine = (
        1.0
        - 0.5 * r2
        + r2 * r2 * (4.166664568298827e-2 + r2 * (-1.388731625493765e-3 + r2 * 2.443315711809948e-5))
    )
    quadrant = turns.astype(jnp.int32)
    odd = (quadrant & 1) == 1
    flip_sine = (quadrant & 2) == 2
    flip_cosine = ((quadrant + 1) & 2) == 2
    base_sine = jnp.where(odd, cosine, sine)
    base_cosine = jnp.where(odd, sine, cosine)
    return (
        jnp.where(flip_sine, -base_sine, base_sine),
        jnp.where(flip_cosine, -base_cosine, base_cosine),
    )


def iota(dims, axis):
    return lax.broadcasted_iota(jnp.int32, dims, axis)


def pieces(x, count):
    found = []
    for _ in range(count):
        part = x.astype(BF16)
        found.append(part)
        x = x - part.astype(F32)
    return found


def picked(x, selector, count=3):
    total = None
    for part in pieces(x, count):
        term = jnp.dot(part, selector, preferred_element_type=F32)
        total = term if total is None else total + term
    return total


def repeat_selector(narrow, wide):
    return (iota((narrow, wide), 1) % narrow == iota((narrow, wide), 0)).astype(BF16)


def flattened(x, groups):
    rows, narrow = x.shape
    wide = groups * narrow
    tiled = picked(x, repeat_selector(narrow, wide))
    own = iota((rows, wide), 1) // narrow == iota((rows, wide), 0) % groups
    tiled = jnp.where(own, tiled, 0.0)
    return [jnp.sum(tiled[at : at + groups], axis=0, keepdims=True) for at in range(0, rows, groups)]


def block_diagonal(x, groups):
    rows, narrow = x.shape
    wide = groups * narrow
    selector = repeat_selector(narrow, wide)
    own = iota((rows, wide), 1) // narrow == iota((rows, wide), 0) // (rows // groups)
    return [
        jnp.where(own, jnp.dot(part, selector, preferred_element_type=F32), 0.0).astype(BF16)
        for part in pieces(x, 2)
    ]


def spread_steps(log_ref, groups, states):
    lane = iota((1, groups * states), 1) // states
    out = jnp.zeros((1, groups * states), F32)
    for g in range(groups):
        out = jnp.where(lane == g, log_ref[g], out)
    return jnp.exp(out)


def chunk_order(rows, flip):
    r, c = (iota((rows, rows), 1 if flip else 0), iota((rows, rows), 0 if flip else 1))
    steps = rows // CHUNKS
    return (c == (r % CHUNKS) * steps + r // CHUNKS).astype(BF16)


def normalized(x, gain):
    x = x.astype(F32)
    mean_square = jnp.mean(x * x, axis=-1, keepdims=True)
    return (x * lax.rsqrt(mean_square + 1e-06) * gain).astype(BF16)


def pack_kernel(*refs):
    count = 6
    sources, out_ref, landed, sems = (refs[:count], refs[count], refs[count + 1], refs[count + 2])
    copies = [
        pltpu.make_async_copy(source, landed.at[i], sems.at[i]) for i, source in enumerate(sources)
    ]
    for copy in copies:
        copy.start()
    for copy in copies:
        copy.wait()
    tall = landed.shape[1]
    part = tall // 4
    for z in range(out_ref.shape[0]):
        out_ref[z, :tall] = landed[0]
        q = z % 4
        for i in range(1, count):
            at = tall + (i - 1) * part
            out_ref[z, at : at + part] = landed[i, q * part : (q + 1) * part]


def prep_kernel(
    log_ref, tokens_ref, gain_ref, rate_ref, decay_ref, freq_ref, initial_ref, in_real_ref, in_imag_ref,
    out_real_ref, out_imag_ref, skip_ref, taps_ref, normed_ref, bar_ref, pack_ref, column_ref,
):
    groups, states = decay_ref.shape
    flat = groups * states
    rows = tokens_ref.shape[0]
    part = 64

    def norm(i, _):
        at = pl.ds(pl.multiple_of(i * part, part), part)
        normed_ref[at, :] = normalized(tokens_ref[at, :], gain_ref[...])
        return 0

    lax.fori_loop(0, rows // part, norm, 0)
    order = chunk_order(rows, False)
    column = None
    for piece in pieces(jnp.broadcast_to(rate_ref[...], (16, rows)), 3):
        term = lax.dot_general(order, piece, NT, preferred_element_type=F32)
        column = term if column is None else column + term
    column_ref[...] = column
    (decay,) = flattened(decay_ref[...], groups)
    (freq,) = flattened(freq_ref[...], groups)
    scale = spread_steps(log_ref, groups, states)
    for at, ref in enumerate((in_real_ref, in_imag_ref, out_real_ref, out_imag_ref)):
        pack_ref[: ref.shape[0], at * states : (at + 1) * states] = ref[...]
    width = taps_ref.shape[1]
    (skip,) = flattened(skip_ref[...], groups)
    gain_rows = gain_ref.shape[1] // flat
    for at, row in enumerate(
        (
            decay,
            freq,
            scale,
            *flattened(initial_ref[...], groups),
            *(gain_ref[:, i * flat : (i + 1) * flat] for i in range(gain_rows)),
            skip,
            *(taps_ref[i : i + 1] for i in range(taps_ref.shape[0])),
        )
    ):
        pack_ref[width + at : width + at + 1, : row.shape[1]] = row
    steps = rows // CHUNKS

    def advance(j, carry):
        at = pl.ds(pl.multiple_of(j * CHUNKS, CHUNKS), CHUNKS)
        step = column_ref[at, 0:1] * scale
        grow = jnp.exp(step * decay)
        sine, cosine = sine_cosine(step * freq)
        bar_real, bar_imag = (grow * cosine, grow * sine)
        bar_ref[0, at, :] = bar_real
        bar_ref[1, at, :] = bar_imag
        return 0

    lax.fori_loop(0, steps, advance, 0)


def packed(pack_ref, at, wide=None):
    top = pack_ref.shape[0] - PACKED
    return pack_ref[top + at : top + at + 1, : pack_ref.shape[1] if wide is None else wide]


def matrix(pack_ref, at, states):
    return pack_ref[: pack_ref.shape[0] - PACKED, at * states : (at + 1) * states]


def driven(chan, pack_ref, bar_ref, groups, push_ref):
    flat = bar_ref.shape[2]
    drives = []
    for at in range(2):
        high, low = block_diagonal(matrix(pack_ref, at, flat // groups), groups)
        drives.append(
            jnp.dot(chan, high, preferred_element_type=F32) + jnp.dot(chan, low, preferred_element_type=F32)
        )
    decay, freq = (packed(pack_ref, 0), packed(pack_ref, 1))
    inverse = 1.0 / (decay * decay + freq * freq)
    bar_imag = bar_ref[1]
    less_real = bar_ref[0] - 1.0
    push_ref[0], push_ref[1] = complex_product(
        (less_real * decay + bar_imag * freq) * inverse,
        (bar_imag * decay - less_real * freq) * inverse,
        drives[0],
        drives[1],
    )


def scanned(bar_ref, push_ref, start):
    steps = bar_ref.shape[1] // CHUNKS

    def advance(j, carry):
        at = pl.ds(pl.multiple_of(j * CHUNKS, CHUNKS), CHUNKS)
        real, imag = complex_product(bar_ref[0, at, :], bar_ref[1, at, :], carry[0], carry[1])
        real = real + push_ref[0, at, :]
        imag = imag + push_ref[1, at, :]
        push_ref[0, at, :] = real
        push_ref[1, at, :] = imag
        return (real, imag)

    lax.fori_loop(0, steps, advance, start, unroll=4)


def chunk_maps(bar_ref, push_ref):
    steps, flat = (bar_ref.shape[1] // CHUNKS, bar_ref.shape[2])

    def advance(j, carry):
        at = pl.ds(pl.multiple_of(j * CHUNKS, CHUNKS), CHUNKS)
        bar = (bar_ref[0, at, :], bar_ref[1, at, :])
        product = complex_product(*bar, carry[0], carry[1])
        real, imag = complex_product(*bar, carry[2], carry[3])
        return (*product, real + push_ref[0, at, :], imag + push_ref[1, at, :])

    one, zero = (jnp.ones((CHUNKS, flat), F32), jnp.zeros((CHUNKS, flat), F32))
    return lax.fori_loop(0, steps, advance, (one, zero, zero, zero), unroll=4)


def local_kernel(
    groups, normed_ref, w_ref, bar_ref, pack_ref, rate_ref, chan_ref, end_ref, push_ref
):
    rows = normed_ref.shape[0]
    fs, sp = w_ref.shape[:2]
    w = jnp.concatenate([w_ref[f, z] for z in range(sp) for f in range(fs)], axis=0)
    state_in = jnp.dot(normed_ref[...], w, preferred_element_type=F32).astype(BF16)
    chan = jnp.dot(chunk_order(rows, False), state_in, preferred_element_type=F32).astype(BF16)
    chan_ref[...] = chan
    flat = bar_ref.shape[2]
    driven(chan, pack_ref, bar_ref, groups, push_ref)
    end_real, end_imag, last_real, last_imag = chunk_maps(bar_ref, push_ref)
    real, imag = (last_real[0:1], last_imag[0:1])
    for c in range(1, CHUNKS):
        moved_real, moved_imag = complex_product(end_real[c : c + 1], end_imag[c : c + 1], real, imag)
        real = moved_real + last_real[c : c + 1]
        imag = moved_imag + last_imag[c : c + 1]
    end_ref[:, :flat] = jnp.concatenate([real, imag], axis=0)
    whole = jnp.sum(rate_ref[...], axis=1, keepdims=True)
    end_ref[:, flat:] = jnp.broadcast_to(whole, (2, end_ref.shape[1] - flat))


def gelu(v):
    return 0.5 * v * (1.0 + jnp.tanh(0.7978845608 * (v + 0.044715 * v * v * v)))


def read_kernel(
    groups, ends_ref, bar_ref, chan_ref, pack_ref, mix_ref, closing_ref, push_ref
):
    flat = bar_ref.shape[2]
    states = flat // groups
    spans = ends_ref.shape[0]
    here = lax.axis_index("sp")
    decay, freq, scale, enter_real, enter_imag = (packed(pack_ref, at) for at in range(5))
    real, imag = (enter_real, enter_imag)
    elapsed = jnp.concatenate([ends_ref[z, 0:1, flat:] for z in range(spans)], axis=0)[:, 0:1] * scale
    grow = jnp.exp(elapsed * decay)
    sine, cosine = sine_cosine(elapsed * freq)
    map_real, map_imag = (grow * cosine, grow * sine)
    for z in range(spans):
        now = here == z
        enter_real = jnp.where(now, real, enter_real)
        enter_imag = jnp.where(now, imag, enter_imag)
        moved_real, moved_imag = complex_product(map_real[z : z + 1], map_imag[z : z + 1], real, imag)
        real = moved_real + ends_ref[z, 0:1, :flat]
        imag = moved_imag + ends_ref[z, 1:2, :flat]
    share = states // spans
    lane = iota((flat, share), 0) % states
    wanted = (lane == here * share + iota((flat, share), 1)).astype(BF16)
    own = iota((groups, flat), 1) // states == iota((groups, flat), 0)
    for at, row in enumerate((real, imag)):
        closing_ref[at] = picked(jnp.where(own, jnp.broadcast_to(row, (groups, flat)), 0.0), wanted)
    rows = bar_ref.shape[1]
    chan = chan_ref[...]
    driven(chan, pack_ref, bar_ref, groups, push_ref)
    end_real, end_imag, last_real, last_imag = chunk_maps(bar_ref, push_ref)
    in_real, in_imag = ([enter_real], [enter_imag])
    for c in range(CHUNKS - 1):
        moved_real, moved_imag = complex_product(
            end_real[c : c + 1], end_imag[c : c + 1], in_real[-1], in_imag[-1]
        )
        in_real.append(moved_real + last_real[c : c + 1])
        in_imag.append(moved_imag + last_imag[c : c + 1])
    scanned(bar_ref, push_ref, (jnp.concatenate(in_real, axis=0), jnp.concatenate(in_imag, axis=0)))
    response = None
    for at, sign in enumerate((1.0, -1.0)):
        weights = block_diagonal(matrix(pack_ref, 2 + at, states) * sign, groups)
        high, low = pieces(push_ref[at], 2)
        for left, right in ((high, 0), (low, 0), (high, 1)):
            term = lax.dot_general(left, weights[right], NT, preferred_element_type=F32)
            response = term if response is None else response + term
    skip = packed(pack_ref, 9, mix_ref.shape[1])
    mixed = gelu(response + skip * chan.astype(F32)).astype(BF16)
    mix_ref[...] = jnp.dot(chunk_order(rows, True), mixed, preferred_element_type=F32).astype(BF16)


def conv_kernel(
    normed_ref, halo_ref, own_ref, up_ref, down_ref, left_ref, right_ref, pack_ref, mix_ref, weights_ref, w_ref
):
    width = mix_ref.shape[1]
    rows = normed_ref.shape[0]
    near, far = own_ref.shape[:2]
    part = w_ref.shape[1]
    z, y = (lax.axis_index("sp"), lax.axis_index("fs"))

    def put(j, turn, ref, at_j):
        at_q = (z + j) & 3
        at_y = (y + 2 * j + turn) & 3
        for k in range(far):
            at = (k * 4 + at_y) * 4 + at_q
            for i in range(5):
                piece = ref[at_j, k, i * part : (i + 1) * part]
                if i < 3:
                    w_ref[at, :, i * width : (i + 1) * width] = piece
                else:
                    weights_ref[at, :, (i - 3) * width : (i - 2) * width] = piece

    for j in range(near):
        put(j, 0, own_ref, j)
        put(j, 1, up_ref, j)
        put(j, 3, down_ref, j)
    for j in range(near // 2):
        put(j + 1, 2, left_ref, j)
        put(j - 1, 2, right_ref, j)
    w = w_ref[...].reshape(normed_ref.shape[1], 3 * width)
    taps = [packed(pack_ref, 10 + at, width) for at in range(3)]
    gain = jnp.concatenate([packed(pack_ref, 5 + at) for at in range(4)], axis=1)
    reach = len(taps) - 1
    here = jnp.dot(normed_ref[...], w, preferred_element_type=F32).astype(BF16).astype(F32)
    halo = normalized(halo_ref[...], gain)
    before = jnp.dot(halo, w[:, : 2 * width], preferred_element_type=F32).astype(BF16).astype(F32)
    gated = (here[:, :width] * here[:, width : 2 * width]).astype(BF16).astype(F32)
    gated_before = (before[:, :width] * before[:, width:]).astype(BF16).astype(F32)
    extended = jnp.concatenate([gated_before, gated], axis=0)
    filtered = taps[reach] * gated
    for tap in range(reach):
        at = HALO - reach + tap
        filtered = filtered + taps[tap] * extended[at : at + rows]
    mix_ref[...] = (here[:, 2 * width :] * filtered).astype(BF16)


def out_kernel(state_ref, conv_ref, w_ref, out_ref):
    mixes = jnp.concatenate([state_ref[...], conv_ref[...]], axis=1)
    per = 512
    tall, part, wide = w_ref.shape
    for at in range(0, tall * part, per):
        w = w_ref[at // part : (at + per) // part].reshape(per, wide)
        product = lax.dot_general(mixes, w, NT, preferred_element_type=F32)
        out_ref[:, at : at + per] = product.astype(BF16)


def moved(x, dz, dy):
    sp, fs = (lax.axis_size("sp"), lax.axis_size("fs"))
    pairs = [
        (z * fs + y, ((z - dz) % sp) * fs + (y - dy) % fs) for z in range(sp) for y in range(fs)
    ]
    return lax.ppermute(x, ("sp", "fs"), pairs)


def all_shards(far):
    near = [far] + [moved(far, dz, dy) for dz, dy in ((1, 2), (2, 0), (-1, 2))]
    own = jnp.stack(near)
    half = own[:2]
    return (own, moved(own, 0, 1), moved(own, 0, -1), moved(half, 1, 0), moved(half, -1, 0))


def call(kernel, out_shape, flops, *args, smem=0, anywhere=0, scratch=(), limit=20 << 20):
    vmem = pl.BlockSpec(memory_space=pltpu.VMEM)
    first = [pl.BlockSpec(memory_space=pltpu.SMEM)] * smem + [pl.BlockSpec(memory_space=pl.ANY)] * anywhere
    return pl.pallas_call(
        kernel,
        out_shape=out_shape,
        in_specs=first + [vmem] * (len(args) - len(first)),
        out_specs=jax.tree.map(lambda _: vmem, out_shape),
        scratch_shapes=list(scratch),
        cost_estimate=pl.CostEstimate(flops=flops, bytes_accessed=1 << 20, transcendentals=0),
        compiler_params=pltpu.CompilerParams(vmem_limit_bytes=limit),
    )(*args)


def shape(dims, dtype=F32):
    return jax.ShapeDtypeStruct(dims, dtype)


def body(
    tokens,
    norm_gain,
    w_state_in,
    w_value,
    w_outer,
    w_inner,
    w_state_out,
    w_conv_out,
    log_step,
    decay_real,
    frequency,
    step_rate,
    input_real,
    input_imag,
    read_real,
    read_imag,
    skip_gain,
    conv_taps,
    initial_state,
):
    rows, features = tokens.shape[1:]
    groups, states = decay_real.shape
    group = skip_gain.shape[1]
    flat = groups * states
    width = groups * group
    count = lax.axis_size("sp")

    part = w_state_in.shape[0] // 4
    weights = (w_state_in, w_value, w_inner, w_outer, w_state_out, w_conv_out)
    shards = call(
        pack_kernel,
        shape((count, w_state_in.shape[0] + 5 * part, width), BF16),
        1 << 20,
        *weights,
        anywhere=len(weights),
        scratch=(
            pltpu.VMEM((len(weights), *w_state_in.shape), BF16),
            pltpu.SemaphoreType.DMA((len(weights),)),
        ),
        limit=None,
    )
    far = lax.all_to_all(shards, "sp", 0, 0, tiled=True)
    state_weights = spread(far[:, : 4 * part], "fs")
    own, up, down, left, right = all_shards(far[:, 4 * part :])
    edge = lax.ppermute(tokens[0, rows - HALO :], "sp", [(i, i + 1) for i in range(count - 1)])
    gain = norm_gain[None]
    into = [jnp.swapaxes(x, 1, 2).reshape(width, states) for x in (input_real, input_imag)]
    normed, bar, pack = call(
        prep_kernel,
        (shape((rows, features), BF16), shape((2, rows, flat)), shape((width + PACKED, flat))),
        1 << 30,
        log_step,
        tokens[0],
        gain,
        step_rate,
        decay_real,
        frequency,
        initial_state[0].reshape(2 * groups, states),
        *into,
        read_real.reshape(width, states),
        read_imag.reshape(width, states),
        skip_gain,
        conv_taps,
        smem=1,
        scratch=(pltpu.VMEM((rows, 16), F32),),
    )
    chan, end = call(
        functools.partial(local_kernel, groups),
        (shape((rows, width), BF16), shape((2, flat + 128))),
        1 << 29,
        normed,
        state_weights,
        bar,
        pack,
        step_rate,
        scratch=(pltpu.VMEM((2, rows, flat), F32),),
    )
    ends = spread(end, "sp")
    conv_mix, out_weights = call(
        conv_kernel,
        (shape((rows, width), BF16), shape((features // part, part, 2 * width), BF16)),
        1 << 29,
        normed,
        edge,
        own,
        up,
        down,
        left,
        right,
        pack,
        scratch=(pltpu.VMEM((features // part, part, 3 * width), BF16),),
    )
    state_mix, closing = call(
        functools.partial(read_kernel, groups),
        (shape((rows, width), BF16), shape((2, groups, states // count))),
        1 << 29,
        ends,
        bar,
        chan,
        pack,
        scratch=(pltpu.VMEM((2, rows, flat), F32),),
    )
    partial = call(
        out_kernel, shape((rows, features), BF16), 1 << 29, state_mix, conv_mix, out_weights
    )
    tp = lax.axis_size("tp")
    parts = lax.all_to_all(partial.reshape(tp, rows // tp, features), "tp", 0, 0, tiled=True)
    mixed = jnp.sum(parts.astype(F32), axis=0).astype(BF16)
    return (mixed[None], closing[None])


def solution(mesh):
    return jax.shard_map(
        body,
        mesh=mesh,
        in_specs=(
            P("fs", "sp", None),
            P(),
            P(("sp", "fs"), "tp"),
            P(("sp", "fs"), "tp"),
            P(("sp", "fs"), "tp"),
            P(("sp", "fs"), "tp"),
            P(("sp", "fs"), "tp"),
            P(("sp", "fs"), "tp"),
            P("tp"),
            P("tp", None),
            P("tp", None),
            P("fs", "sp"),
            P("tp", None, None),
            P("tp", None, None),
            P("tp", None, None),
            P("tp", None, None),
            P("tp", None),
            P(None, "tp"),
            P("fs", None, "tp", None),
        ),
        out_specs=(P("fs", ("sp", "tp"), None), P("fs", None, "tp", "sp")),
        check_vma=False,
    )
```

```python
import functools

import jax
import jax.numpy as jnp
from jax import lax
from jax.experimental import pallas as pl
from jax.experimental.pallas import tpu as pltpu
from jax.sharding import PartitionSpec as P


F32 = jnp.float32
BF16 = jnp.bfloat16
CHUNKS = 8
HALO = 16
PACKED = 16
NT = (((1,), (1,)), ((), ()))


def complex_product(left_real, left_imag, right_real, right_imag):
    return (
        left_real * right_real - left_imag * right_imag,
        left_real * right_imag + left_imag * right_real,
    )


def sine_cosine(angle):
    turns = jnp.floor(angle * 0.6366197723675814 + 0.5)
    r = angle - turns * 1.5703125
    r = r - turns * 4.837512969970703e-4
    r = r - turns * 7.549789948768648e-8
    r2 = r * r
    sine = r + r * r2 * (-1.6666654611e-1 + r2 * (8.3321608736e-3 + r2 * -1.9515295891e-4))
    cosine = (
        1.0
        - 0.5 * r2
        + r2 * r2 * (4.166664568298827e-2 + r2 * (-1.388731625493765e-3 + r2 * 2.443315711809948e-5))
    )
    quadrant = turns.astype(jnp.int32)
    odd = (quadrant & 1) == 1
    flip_sine = (quadrant & 2) == 2
    flip_cosine = ((quadrant + 1) & 2) == 2
    base_sine = jnp.where(odd, cosine, sine)
    base_cosine = jnp.where(odd, sine, cosine)
    return (
        jnp.where(flip_sine, -base_sine, base_sine),
        jnp.where(flip_cosine, -base_cosine, base_cosine),
    )


def iota(dims, axis):
    return lax.broadcasted_iota(jnp.int32, dims, axis)


def pieces(x, count):
    found = []
    for _ in range(count):
        part = x.astype(BF16)
        found.append(part)
        x = x - part.astype(F32)
    return found


def picked(x, selector, count=3):
    total = None
    for part in pieces(x, count):
        term = jnp.dot(part, selector, preferred_element_type=F32)
        total = term if total is None else total + term
    return total


def repeat_selector(narrow, wide):
    return (iota((narrow, wide), 1) % narrow == iota((narrow, wide), 0)).astype(BF16)


def flattened(x, groups):
    rows, narrow = x.shape
    wide = groups * narrow
    tiled = picked(x, repeat_selector(narrow, wide))
    own = iota((rows, wide), 1) // narrow == iota((rows, wide), 0) % groups
    tiled = jnp.where(own, tiled, 0.0)
    return [jnp.sum(tiled[at : at + groups], axis=0, keepdims=True) for at in range(0, rows, groups)]


def block_diagonal(x, groups):
    rows, narrow = x.shape
    wide = groups * narrow
    selector = repeat_selector(narrow, wide)
    own = iota((rows, wide), 1) // narrow == iota((rows, wide), 0) // (rows // groups)
    return [
        jnp.where(own, jnp.dot(part, selector, preferred_element_type=F32), 0.0).astype(BF16)
        for part in pieces(x, 2)
    ]


def spread_steps(log_ref, groups, states):
    lane = iota((1, groups * states), 1) // states
    out = jnp.zeros((1, groups * states), F32)
    for g in range(groups):
        out = jnp.where(lane == g, log_ref[g], out)
    return jnp.exp(out)


def chunk_order(rows, flip):
    r, c = (iota((rows, rows), 1 if flip else 0), iota((rows, rows), 0 if flip else 1))
    steps = rows // CHUNKS
    return (c == (r % CHUNKS) * steps + r // CHUNKS).astype(BF16)


def normalized(x, gain):
    x = x.astype(F32)
    mean_square = jnp.mean(x * x, axis=-1, keepdims=True)
    return (x * lax.rsqrt(mean_square + 1e-06) * gain).astype(BF16)


def pack_kernel(*refs):
    count = 6
    sources, out_ref, landed, sems = (refs[:count], refs[count], refs[count + 1], refs[count + 2])
    copies = [
        pltpu.make_async_copy(source, landed.at[i], sems.at[i]) for i, source in enumerate(sources)
    ]
    for copy in copies:
        copy.start()
    for copy in copies:
        copy.wait()
    tall = landed.shape[1]
    part = tall // 4
    for z in range(out_ref.shape[0]):
        out_ref[z, :tall] = landed[0]
        q = z % 4
        for i in range(1, count):
            at = tall + (i - 1) * part
            out_ref[z, at : at + part] = landed[i, q * part : (q + 1) * part]


def prep_kernel(
    log_ref, tokens_ref, gain_ref, rate_ref, decay_ref, freq_ref, initial_ref, in_real_ref, in_imag_ref,
    out_real_ref, out_imag_ref, skip_ref, taps_ref, normed_ref, bar_ref, pack_ref, column_ref,
):
    groups, states = decay_ref.shape
    flat = groups * states
    rows = tokens_ref.shape[0]
    part = 64

    def norm(i, _):
        at = pl.ds(pl.multiple_of(i * part, part), part)
        normed_ref[at, :] = normalized(tokens_ref[at, :], gain_ref[...])
        return 0

    lax.fori_loop(0, rows // part, norm, 0)
    order = chunk_order(rows, False)
    column = None
    for piece in pieces(jnp.broadcast_to(rate_ref[...], (16, rows)), 3):
        term = lax.dot_general(order, piece, NT, preferred_element_type=F32)
        column = term if column is None else column + term
    column_ref[...] = column
    (decay,) = flattened(decay_ref[...], groups)
    (freq,) = flattened(freq_ref[...], groups)
    scale = spread_steps(log_ref, groups, states)
    top = in_real_ref.shape[0] // 2
    for at, ref in enumerate((in_real_ref, in_imag_ref, out_real_ref, out_imag_ref)):
        for i in range(2):
            lanes = slice((2 * at + i) * states, (2 * at + i + 1) * states)
            pack_ref[:top, lanes] = ref[i * top : (i + 1) * top]
    (skip,) = flattened(skip_ref[...], groups)
    gain_rows = gain_ref.shape[1] // flat
    for at, row in enumerate(
        (
            decay,
            freq,
            scale,
            *flattened(initial_ref[...], groups),
            *(gain_ref[:, i * flat : (i + 1) * flat] for i in range(gain_rows)),
            skip,
            *(taps_ref[i : i + 1] for i in range(taps_ref.shape[0])),
        )
    ):
        pack_ref[top + at : top + at + 1, : row.shape[1]] = row
    steps = rows // CHUNKS

    def advance(j, carry):
        at = pl.ds(pl.multiple_of(j * CHUNKS, CHUNKS), CHUNKS)
        step = column_ref[at, 0:1] * scale
        grow = jnp.exp(step * decay)
        sine, cosine = sine_cosine(step * freq)
        bar_real, bar_imag = (grow * cosine, grow * sine)
        bar_ref[0, at, :] = bar_real
        bar_ref[1, at, :] = bar_imag
        return 0

    lax.fori_loop(0, steps, advance, 0)


def packed(pack_ref, at, wide=None):
    top = pack_ref.shape[0] - PACKED
    return pack_ref[top + at : top + at + 1, : pack_ref.shape[1] if wide is None else wide]


def matrix(pack_ref, at, states):
    top = pack_ref.shape[0] - PACKED
    halves = [pack_ref[:top, (2 * at + i) * states : (2 * at + i + 1) * states] for i in range(2)]
    return jnp.concatenate(halves, axis=0)


def driven(chan, pack_ref, bar_ref, groups, push_ref):
    flat = bar_ref.shape[2]
    drives = []
    for at in range(2):
        high, low = block_diagonal(matrix(pack_ref, at, flat // groups), groups)
        drives.append(
            jnp.dot(chan, high, preferred_element_type=F32) + jnp.dot(chan, low, preferred_element_type=F32)
        )
    decay, freq = (packed(pack_ref, 0), packed(pack_ref, 1))
    inverse = 1.0 / (decay * decay + freq * freq)
    bar_imag = bar_ref[1]
    less_real = bar_ref[0] - 1.0
    push_ref[0], push_ref[1] = complex_product(
        (less_real * decay + bar_imag * freq) * inverse,
        (bar_imag * decay - less_real * freq) * inverse,
        drives[0],
        drives[1],
    )


def scanned(bar_ref, push_ref, start):
    steps = bar_ref.shape[1] // CHUNKS

    def advance(j, carry):
        at = pl.ds(pl.multiple_of(j * CHUNKS, CHUNKS), CHUNKS)
        real, imag = complex_product(bar_ref[0, at, :], bar_ref[1, at, :], carry[0], carry[1])
        real = real + push_ref[0, at, :]
        imag = imag + push_ref[1, at, :]
        push_ref[0, at, :] = real
        push_ref[1, at, :] = imag
        return (real, imag)

    lax.fori_loop(0, steps, advance, start, unroll=4)


def chunk_maps(bar_ref, push_ref):
    steps, flat = (bar_ref.shape[1] // CHUNKS, bar_ref.shape[2])

    def advance(j, carry):
        at = pl.ds(pl.multiple_of(j * CHUNKS, CHUNKS), CHUNKS)
        bar = (bar_ref[0, at, :], bar_ref[1, at, :])
        product = complex_product(*bar, carry[0], carry[1])
        real, imag = complex_product(*bar, carry[2], carry[3])
        return (*product, real + push_ref[0, at, :], imag + push_ref[1, at, :])

    one, zero = (jnp.ones((CHUNKS, flat), F32), jnp.zeros((CHUNKS, flat), F32))
    return lax.fori_loop(0, steps, advance, (one, zero, zero, zero), unroll=4)


def local_kernel(
    groups, normed_ref, w_ref, bar_ref, pack_ref, rate_ref, chan_ref, end_ref, push_ref
):
    rows = normed_ref.shape[0]
    fs, sp = w_ref.shape[:2]
    w = jnp.concatenate([w_ref[f, z] for z in range(sp) for f in range(fs)], axis=0)
    state_in = jnp.dot(normed_ref[...], w, preferred_element_type=F32).astype(BF16)
    chan = jnp.dot(chunk_order(rows, False), state_in, preferred_element_type=F32).astype(BF16)
    chan_ref[...] = chan
    flat = bar_ref.shape[2]
    driven(chan, pack_ref, bar_ref, groups, push_ref)
    end_real, end_imag, last_real, last_imag = chunk_maps(bar_ref, push_ref)
    real, imag = (last_real[0:1], last_imag[0:1])
    for c in range(1, CHUNKS):
        moved_real, moved_imag = complex_product(end_real[c : c + 1], end_imag[c : c + 1], real, imag)
        real = moved_real + last_real[c : c + 1]
        imag = moved_imag + last_imag[c : c + 1]
    end = jnp.concatenate([real, imag], axis=0)
    whole = jnp.sum(rate_ref[...], axis=1, keepdims=True)
    whole = jnp.broadcast_to(whole, (2, end_ref.shape[2] - flat))
    for z in range(end_ref.shape[0]):
        end_ref[z, :, :flat] = end
        end_ref[z, :, flat:] = whole


def split_kernel(far_ref, many_ref, rest_ref):
    tall = many_ref.shape[2]
    rest_ref[...] = far_ref[:, tall:]
    for copy in range(many_ref.shape[0]):
        many_ref[copy] = far_ref[:, :tall]


def gelu(v):
    return 0.5 * v * (1.0 + jnp.tanh(0.7978845608 * (v + 0.044715 * v * v * v)))


def read_kernel(
    groups, ends_ref, bar_ref, chan_ref, pack_ref, mix_ref, closing_ref, push_ref
):
    flat = bar_ref.shape[2]
    states = flat // groups
    spans = ends_ref.shape[0]
    here = lax.axis_index("sp")
    decay, freq, scale, enter_real, enter_imag = (packed(pack_ref, at) for at in range(5))
    real, imag = (enter_real, enter_imag)
    elapsed = jnp.concatenate([ends_ref[z, 0:1, flat:] for z in range(spans)], axis=0)[:, 0:1] * scale
    grow = jnp.exp(elapsed * decay)
    sine, cosine = sine_cosine(elapsed * freq)
    map_real, map_imag = (grow * cosine, grow * sine)
    for z in range(spans):
        now = here == z
        enter_real = jnp.where(now, real, enter_real)
        enter_imag = jnp.where(now, imag, enter_imag)
        moved_real, moved_imag = complex_product(map_real[z : z + 1], map_imag[z : z + 1], real, imag)
        real = moved_real + ends_ref[z, 0:1, :flat]
        imag = moved_imag + ends_ref[z, 1:2, :flat]
    share = states // spans
    lane = iota((flat, share), 0) % states
    wanted = (lane == here * share + iota((flat, share), 1)).astype(BF16)
    own = iota((groups, flat), 1) // states == iota((groups, flat), 0)
    for at, row in enumerate((real, imag)):
        closing_ref[at] = picked(jnp.where(own, jnp.broadcast_to(row, (groups, flat)), 0.0), wanted)
    rows = bar_ref.shape[1]
    chan = chan_ref[...]
    driven(chan, pack_ref, bar_ref, groups, push_ref)
    end_real, end_imag, last_real, last_imag = chunk_maps(bar_ref, push_ref)
    in_real, in_imag = ([enter_real], [enter_imag])
    for c in range(CHUNKS - 1):
        moved_real, moved_imag = complex_product(
            end_real[c : c + 1], end_imag[c : c + 1], in_real[-1], in_imag[-1]
        )
        in_real.append(moved_real + last_real[c : c + 1])
        in_imag.append(moved_imag + last_imag[c : c + 1])
    scanned(bar_ref, push_ref, (jnp.concatenate(in_real, axis=0), jnp.concatenate(in_imag, axis=0)))
    response = None
    for at, sign in enumerate((1.0, -1.0)):
        weights = block_diagonal(matrix(pack_ref, 2 + at, states) * sign, groups)
        high, low = pieces(push_ref[at], 2)
        for left, right in ((high, 0), (low, 0), (high, 1)):
            term = lax.dot_general(left, weights[right], NT, preferred_element_type=F32)
            response = term if response is None else response + term
    skip = packed(pack_ref, 9, mix_ref.shape[1])
    mixed = gelu(response + skip * chan.astype(F32)).astype(BF16)
    mix_ref[...] = jnp.dot(chunk_order(rows, True), mixed, preferred_element_type=F32).astype(BF16)


def conv_kernel(
    normed_ref, halo_ref, own_ref, up_ref, down_ref, left_ref, right_ref, pack_ref, mix_ref, weights_ref, w_ref
):
    width = mix_ref.shape[1]
    rows = normed_ref.shape[0]
    near, far = own_ref.shape[:2]
    part = w_ref.shape[1]
    z, y = (lax.axis_index("sp"), lax.axis_index("fs"))

    def put(j, turn, ref, at_j):
        at_q = (z + j) & 3
        at_y = (y + 2 * j + turn) & 3
        for k in range(far):
            at = (k * 4 + at_y) * 4 + at_q
            for i in range(5):
                piece = ref[at_j, k, i * part : (i + 1) * part]
                if i < 3:
                    w_ref[at, :, i * width : (i + 1) * width] = piece
                else:
                    weights_ref[at, :, (i - 3) * width : (i - 2) * width] = piece

    for j in range(near):
        put(j, 0, own_ref, j)
        put(j, 1, up_ref, j)
        put(j, 3, down_ref, j)
    for j in range(near // 2):
        put(j + 1, 2, left_ref, j)
        put(j - 1, 2, right_ref, j)
    w = w_ref[...].reshape(normed_ref.shape[1], 3 * width)
    taps = [packed(pack_ref, 10 + at, width) for at in range(3)]
    gain = jnp.concatenate([packed(pack_ref, 5 + at) for at in range(4)], axis=1)
    reach = len(taps) - 1
    here = jnp.dot(normed_ref[...], w, preferred_element_type=F32).astype(BF16).astype(F32)
    halo = normalized(halo_ref[...], gain)
    before = jnp.dot(halo, w[:, : 2 * width], preferred_element_type=F32).astype(BF16).astype(F32)
    gated = (here[:, :width] * here[:, width : 2 * width]).astype(BF16).astype(F32)
    gated_before = (before[:, :width] * before[:, width:]).astype(BF16).astype(F32)
    extended = jnp.concatenate([gated_before, gated], axis=0)
    filtered = taps[reach] * gated
    for tap in range(reach):
        at = HALO - reach + tap
        filtered = filtered + taps[tap] * extended[at : at + rows]
    mix_ref[...] = (here[:, 2 * width :] * filtered).astype(BF16)


def out_kernel(state_ref, conv_ref, w_ref, out_ref):
    mixes = jnp.concatenate([state_ref[...], conv_ref[...]], axis=1)
    per = 512
    tall, part, wide = w_ref.shape
    for at in range(0, tall * part, per):
        w = w_ref[at // part : (at + per) // part].reshape(per, wide)
        product = lax.dot_general(mixes, w, NT, preferred_element_type=F32)
        out_ref[:, at : at + per] = product.astype(BF16)


def moved(x, dz, dy):
    sp, fs = (lax.axis_size("sp"), lax.axis_size("fs"))
    pairs = [
        (z * fs + y, ((z - dz) % sp) * fs + (y - dy) % fs) for z in range(sp) for y in range(fs)
    ]
    return lax.ppermute(x, ("sp", "fs"), pairs)


def all_shards(far):
    near = [far] + [moved(far, dz, dy) for dz, dy in ((1, 2), (2, 0), (-1, 2))]
    own = jnp.stack(near)
    half = own[:2]
    return (own, moved(own, 0, 1), moved(own, 0, -1), moved(half, 1, 0), moved(half, -1, 0))


def call(kernel, out_shape, flops, *args, smem=0, anywhere=0, scratch=(), limit=20 << 20):
    vmem = pl.BlockSpec(memory_space=pltpu.VMEM)
    first = [pl.BlockSpec(memory_space=pltpu.SMEM)] * smem + [pl.BlockSpec(memory_space=pl.ANY)] * anywhere
    return pl.pallas_call(
        kernel,
        out_shape=out_shape,
        in_specs=first + [vmem] * (len(args) - len(first)),
        out_specs=jax.tree.map(lambda _: vmem, out_shape),
        scratch_shapes=list(scratch),
        cost_estimate=pl.CostEstimate(flops=flops, bytes_accessed=1 << 20, transcendentals=0),
        compiler_params=pltpu.CompilerParams(vmem_limit_bytes=limit),
    )(*args)


def shape(dims, dtype=F32):
    return jax.ShapeDtypeStruct(dims, dtype)


def body(
    tokens,
    norm_gain,
    w_state_in,
    w_value,
    w_outer,
    w_inner,
    w_state_out,
    w_conv_out,
    log_step,
    decay_real,
    frequency,
    step_rate,
    input_real,
    input_imag,
    read_real,
    read_imag,
    skip_gain,
    conv_taps,
    initial_state,
):
    rows, features = tokens.shape[1:]
    groups, states = decay_real.shape
    group = skip_gain.shape[1]
    flat = groups * states
    width = groups * group
    count = lax.axis_size("sp")

    part = w_state_in.shape[0] // 4
    weights = (w_state_in, w_value, w_inner, w_outer, w_state_out, w_conv_out)
    shards = call(
        pack_kernel,
        shape((count, w_state_in.shape[0] + 5 * part, width), BF16),
        1 << 20,
        *weights,
        anywhere=len(weights),
        scratch=(
            pltpu.VMEM((len(weights), *w_state_in.shape), BF16),
            pltpu.SemaphoreType.DMA((len(weights),)),
        ),
        limit=None,
    )
    far = lax.all_to_all(shards, "sp", 0, 0, tiled=True)
    fs = lax.axis_size("fs")
    many, rest = call(
        split_kernel,
        (shape((fs, count, 4 * part, width), BF16), shape((count, 5 * part, width), BF16)),
        1 << 20,
        far,
    )
    state_weights = lax.all_to_all(many, "fs", 0, 0, tiled=True)
    own, up, down, left, right = all_shards(rest)
    edge = lax.ppermute(tokens[0, rows - HALO :], "sp", [(i, i + 1) for i in range(count - 1)])
    gain = norm_gain[None]
    into = [jnp.swapaxes(x, 1, 2).reshape(width, states) for x in (input_real, input_imag)]
    normed, bar, pack = call(
        prep_kernel,
        (shape((rows, features), BF16), shape((2, rows, flat)), shape((width // 2 + PACKED, flat))),
        1 << 30,
        log_step,
        tokens[0],
        gain,
        step_rate,
        decay_real,
        frequency,
        initial_state[0].reshape(2 * groups, states),
        *into,
        read_real.reshape(width, states),
        read_imag.reshape(width, states),
        skip_gain,
        conv_taps,
        smem=1,
        scratch=(pltpu.VMEM((rows, 16), F32),),
    )
    chan, end = call(
        functools.partial(local_kernel, groups),
        (shape((rows, width), BF16), shape((count, 2, flat + 128))),
        1 << 29,
        normed,
        state_weights,
        bar,
        pack,
        step_rate,
        scratch=(pltpu.VMEM((2, rows, flat), F32),),
    )
    ends = lax.all_to_all(end, "sp", 0, 0, tiled=True)
    conv_mix, out_weights = call(
        conv_kernel,
        (shape((rows, width), BF16), shape((features // part, part, 2 * width), BF16)),
        1 << 29,
        normed,
        edge,
        own,
        up,
        down,
        left,
        right,
        pack,
        scratch=(pltpu.VMEM((features // part, part, 3 * width), BF16),),
    )
    state_mix, closing = call(
        functools.partial(read_kernel, groups),
        (shape((rows, width), BF16), shape((2, groups, states // count))),
        1 << 29,
        ends,
        bar,
        chan,
        pack,
        scratch=(pltpu.VMEM((2, rows, flat), F32),),
    )
    partial = call(
        out_kernel, shape((rows, features), BF16), 1 << 29, state_mix, conv_mix, out_weights
    )
    tp = lax.axis_size("tp")
    parts = lax.all_to_all(partial.reshape(tp, rows // tp, features), "tp", 0, 0, tiled=True)
    mixed = jnp.sum(parts.astype(F32), axis=0).astype(BF16)
    return (mixed[None], closing[None])


def solution(mesh):
    return jax.shard_map(
        body,
        mesh=mesh,
        in_specs=(
            P("fs", "sp", None),
            P(),
            P(("sp", "fs"), "tp"),
            P(("sp", "fs"), "tp"),
            P(("sp", "fs"), "tp"),
            P(("sp", "fs"), "tp"),
            P(("sp", "fs"), "tp"),
            P(("sp", "fs"), "tp"),
            P("tp"),
            P("tp", None),
            P("tp", None),
            P("fs", "sp"),
            P("tp", None, None),
            P("tp", None, None),
            P("tp", None, None),
            P("tp", None, None),
            P("tp", None),
            P(None, "tp"),
            P("fs", None, "tp", None),
        ),
        out_specs=(P("fs", ("sp", "tp"), None), P("fs", None, "tp", "sp")),
        check_vma=False,
    )
```

```python
import functools

import jax
import jax.numpy as jnp
from jax import lax
from jax.experimental import pallas as pl
from jax.experimental.pallas import tpu as pltpu
from jax.sharding import PartitionSpec as P


F32 = jnp.float32
BF16 = jnp.bfloat16
CHUNKS = 8
HALO = 16
PACKED = 16
NT = (((1,), (1,)), ((), ()))


def complex_product(left_real, left_imag, right_real, right_imag):
    return (
        left_real * right_real - left_imag * right_imag,
        left_real * right_imag + left_imag * right_real,
    )


def sine_cosine(angle):
    turns = jnp.floor(angle * 0.6366197723675814 + 0.5)
    r = angle - turns * 1.5703125
    r = r - turns * 4.837512969970703e-4
    r = r - turns * 7.549789948768648e-8
    r2 = r * r
    sine = r + r * r2 * (-1.6666654611e-1 + r2 * (8.3321608736e-3 + r2 * -1.9515295891e-4))
    cosine = (
        1.0
        - 0.5 * r2
        + r2 * r2 * (4.166664568298827e-2 + r2 * (-1.388731625493765e-3 + r2 * 2.443315711809948e-5))
    )
    quadrant = turns.astype(jnp.int32)
    odd = (quadrant & 1) == 1
    flip_sine = (quadrant & 2) == 2
    flip_cosine = ((quadrant + 1) & 2) == 2
    base_sine = jnp.where(odd, cosine, sine)
    base_cosine = jnp.where(odd, sine, cosine)
    return (
        jnp.where(flip_sine, -base_sine, base_sine),
        jnp.where(flip_cosine, -base_cosine, base_cosine),
    )


def iota(dims, axis):
    return lax.broadcasted_iota(jnp.int32, dims, axis)


def pieces(x, count):
    found = []
    for _ in range(count):
        part = x.astype(BF16)
        found.append(part)
        x = x - part.astype(F32)
    return found


def picked(x, selector, count=3):
    total = None
    for part in pieces(x, count):
        term = jnp.dot(part, selector, preferred_element_type=F32)
        total = term if total is None else total + term
    return total


def repeat_selector(narrow, wide):
    return (iota((narrow, wide), 1) % narrow == iota((narrow, wide), 0)).astype(BF16)


def flattened(x, groups):
    rows, narrow = x.shape
    wide = groups * narrow
    tiled = picked(x, repeat_selector(narrow, wide))
    own = iota((rows, wide), 1) // narrow == iota((rows, wide), 0) % groups
    tiled = jnp.where(own, tiled, 0.0)
    return [jnp.sum(tiled[at : at + groups], axis=0, keepdims=True) for at in range(0, rows, groups)]


def block_diagonal(x, groups):
    rows, narrow = x.shape
    wide = groups * narrow
    selector = repeat_selector(narrow, wide)
    own = iota((rows, wide), 1) // narrow == iota((rows, wide), 0) // (rows // groups)
    return [
        jnp.where(own, jnp.dot(part, selector, preferred_element_type=F32), 0.0).astype(BF16)
        for part in pieces(x, 2)
    ]


def spread_steps(log_ref, groups, states):
    lane = iota((1, groups * states), 1) // states
    out = jnp.zeros((1, groups * states), F32)
    for g in range(groups):
        out = jnp.where(lane == g, log_ref[g], out)
    return jnp.exp(out)


def chunk_order(rows, flip):
    r, c = (iota((rows, rows), 1 if flip else 0), iota((rows, rows), 0 if flip else 1))
    steps = rows // CHUNKS
    return (c == (r % CHUNKS) * steps + r // CHUNKS).astype(BF16)


def normalized(x, gain):
    x = x.astype(F32)
    mean_square = jnp.mean(x * x, axis=-1, keepdims=True)
    return (x * lax.rsqrt(mean_square + 1e-06) * gain).astype(BF16)


def pack_kernel(*refs):
    count = 6
    sources, out_ref, landed, sems = (refs[:count], refs[count], refs[count + 1], refs[count + 2])
    copies = [
        pltpu.make_async_copy(source, landed.at[i], sems.at[i]) for i, source in enumerate(sources)
    ]
    for copy in copies:
        copy.start()
    for copy in copies:
        copy.wait()
    tall = landed.shape[1]
    part = tall // 4
    for z in range(out_ref.shape[0]):
        out_ref[z, :tall] = landed[0]
        q = z % 4
        for i in range(1, count):
            at = tall + (i - 1) * part
            out_ref[z, at : at + part] = landed[i, q * part : (q + 1) * part]


def prep_kernel(
    log_ref, tokens_ref, gain_ref, rate_ref, decay_ref, freq_ref, initial_ref, in_real_ref, in_imag_ref,
    out_real_ref, out_imag_ref, skip_ref, taps_ref, normed_ref, bar_ref, pack_ref, column_ref,
):
    groups, states = decay_ref.shape
    flat = groups * states
    rows = tokens_ref.shape[0]
    part = 64

    def norm(i, _):
        at = pl.ds(pl.multiple_of(i * part, part), part)
        normed_ref[at, :] = normalized(tokens_ref[at, :], gain_ref[...])
        return 0

    lax.fori_loop(0, rows // part, norm, 0)
    order = chunk_order(rows, False)
    column = None
    for piece in pieces(jnp.broadcast_to(rate_ref[...], (16, rows)), 3):
        term = lax.dot_general(order, piece, NT, preferred_element_type=F32)
        column = term if column is None else column + term
    column_ref[...] = column
    (decay,) = flattened(decay_ref[...], groups)
    (freq,) = flattened(freq_ref[...], groups)
    scale = spread_steps(log_ref, groups, states)
    top = in_real_ref.shape[0] // 2
    for at, ref in enumerate((in_real_ref, in_imag_ref, out_real_ref, out_imag_ref)):
        for i in range(2):
            lanes = slice((2 * at + i) * states, (2 * at + i + 1) * states)
            pack_ref[:top, lanes] = ref[i * top : (i + 1) * top]
    (skip,) = flattened(skip_ref[...], groups)
    gain_rows = gain_ref.shape[1] // flat
    for at, row in enumerate(
        (
            decay,
            freq,
            scale,
            *flattened(initial_ref[...], groups),
            *(gain_ref[:, i * flat : (i + 1) * flat] for i in range(gain_rows)),
            skip,
            *(taps_ref[i : i + 1] for i in range(taps_ref.shape[0])),
        )
    ):
        pack_ref[top + at : top + at + 1, : row.shape[1]] = row
    steps = rows // CHUNKS

    def advance(j, carry):
        at = pl.ds(pl.multiple_of(j * CHUNKS, CHUNKS), CHUNKS)
        step = column_ref[at, 0:1] * scale
        grow = jnp.exp(step * decay)
        sine, cosine = sine_cosine(step * freq)
        bar_real, bar_imag = (grow * cosine, grow * sine)
        bar_ref[0, at, :] = bar_real
        bar_ref[1, at, :] = bar_imag
        return 0

    lax.fori_loop(0, steps, advance, 0)


def packed(pack_ref, at, wide=None):
    top = pack_ref.shape[0] - PACKED
    return pack_ref[top + at : top + at + 1, : pack_ref.shape[1] if wide is None else wide]


def matrix(pack_ref, at, states):
    top = pack_ref.shape[0] - PACKED
    halves = [pack_ref[:top, (2 * at + i) * states : (2 * at + i + 1) * states] for i in range(2)]
    return jnp.concatenate(halves, axis=0)


def driven(chan, pack_ref, bar_ref, groups, push_ref):
    flat = bar_ref.shape[2]
    drives = []
    for at in range(2):
        high, low = block_diagonal(matrix(pack_ref, at, flat // groups), groups)
        drives.append(
            jnp.dot(chan, high, preferred_element_type=F32) + jnp.dot(chan, low, preferred_element_type=F32)
        )
    decay, freq = (packed(pack_ref, 0), packed(pack_ref, 1))
    inverse = 1.0 / (decay * decay + freq * freq)
    bar_imag = bar_ref[1]
    less_real = bar_ref[0] - 1.0
    push_ref[0], push_ref[1] = complex_product(
        (less_real * decay + bar_imag * freq) * inverse,
        (bar_imag * decay - less_real * freq) * inverse,
        drives[0],
        drives[1],
    )


def scanned(bar_ref, push_ref, start):
    steps = bar_ref.shape[1] // CHUNKS

    def advance(j, carry):
        at = pl.ds(pl.multiple_of(j * CHUNKS, CHUNKS), CHUNKS)
        real, imag = complex_product(bar_ref[0, at, :], bar_ref[1, at, :], carry[0], carry[1])
        real = real + push_ref[0, at, :]
        imag = imag + push_ref[1, at, :]
        push_ref[0, at, :] = real
        push_ref[1, at, :] = imag
        return (real, imag)

    lax.fori_loop(0, steps, advance, start, unroll=4)


def chunk_maps(bar_ref, push_ref):
    steps, flat = (bar_ref.shape[1] // CHUNKS, bar_ref.shape[2])

    def advance(j, carry):
        at = pl.ds(pl.multiple_of(j * CHUNKS, CHUNKS), CHUNKS)
        bar = (bar_ref[0, at, :], bar_ref[1, at, :])
        product = complex_product(*bar, carry[0], carry[1])
        real, imag = complex_product(*bar, carry[2], carry[3])
        return (*product, real + push_ref[0, at, :], imag + push_ref[1, at, :])

    one, zero = (jnp.ones((CHUNKS, flat), F32), jnp.zeros((CHUNKS, flat), F32))
    return lax.fori_loop(0, steps, advance, (one, zero, zero, zero), unroll=4)


def local_kernel(
    groups, normed_ref, w_ref, bar_ref, pack_ref, rate_ref, chan_ref, end_ref, push_ref
):
    rows = normed_ref.shape[0]
    fs, sp = w_ref.shape[:2]
    w = jnp.concatenate([w_ref[f, z] for z in range(sp) for f in range(fs)], axis=0)
    state_in = jnp.dot(normed_ref[...], w, preferred_element_type=F32).astype(BF16)
    chan = jnp.dot(chunk_order(rows, False), state_in, preferred_element_type=F32).astype(BF16)
    chan_ref[...] = chan
    flat = bar_ref.shape[2]
    driven(chan, pack_ref, bar_ref, groups, push_ref)
    end_real, end_imag, last_real, last_imag = chunk_maps(bar_ref, push_ref)
    real, imag = (last_real[0:1], last_imag[0:1])
    for c in range(1, CHUNKS):
        moved_real, moved_imag = complex_product(end_real[c : c + 1], end_imag[c : c + 1], real, imag)
        real = moved_real + last_real[c : c + 1]
        imag = moved_imag + last_imag[c : c + 1]
    end = jnp.concatenate([real, imag], axis=0)
    whole = jnp.sum(rate_ref[...], axis=1, keepdims=True)
    whole = jnp.broadcast_to(whole, (2, end_ref.shape[2] - flat))
    for z in range(end_ref.shape[0]):
        end_ref[z, :, :flat] = end
        end_ref[z, :, flat:] = whole


def split_kernel(far_ref, many_ref, rest_ref):
    tall = many_ref.shape[2]
    rest_ref[...] = far_ref[:, tall:]
    for copy in range(many_ref.shape[0]):
        many_ref[copy] = far_ref[:, :tall]


def gelu(v):
    return 0.5 * v * (1.0 + jnp.tanh(0.7978845608 * (v + 0.044715 * v * v * v)))


def read_kernel(
    groups, ends_ref, bar_ref, chan_ref, pack_ref, mix_ref, closing_ref, push_ref
):
    flat = bar_ref.shape[2]
    states = flat // groups
    spans = ends_ref.shape[0]
    here = lax.axis_index("sp")
    decay, freq, scale, enter_real, enter_imag = (packed(pack_ref, at) for at in range(5))
    real, imag = (enter_real, enter_imag)
    elapsed = jnp.concatenate([ends_ref[z, 0:1, flat:] for z in range(spans)], axis=0)[:, 0:1] * scale
    grow = jnp.exp(elapsed * decay)
    sine, cosine = sine_cosine(elapsed * freq)
    map_real, map_imag = (grow * cosine, grow * sine)
    for z in range(spans):
        now = here == z
        enter_real = jnp.where(now, real, enter_real)
        enter_imag = jnp.where(now, imag, enter_imag)
        moved_real, moved_imag = complex_product(map_real[z : z + 1], map_imag[z : z + 1], real, imag)
        real = moved_real + ends_ref[z, 0:1, :flat]
        imag = moved_imag + ends_ref[z, 1:2, :flat]
    share = states // spans
    lane = iota((flat, share), 0) % states
    wanted = (lane == here * share + iota((flat, share), 1)).astype(BF16)
    own = iota((groups, flat), 1) // states == iota((groups, flat), 0)
    for at, row in enumerate((real, imag)):
        closing_ref[at] = picked(jnp.where(own, jnp.broadcast_to(row, (groups, flat)), 0.0), wanted)
    rows = bar_ref.shape[1]
    chan = chan_ref[...]
    driven(chan, pack_ref, bar_ref, groups, push_ref)
    end_real, end_imag, last_real, last_imag = chunk_maps(bar_ref, push_ref)
    in_real, in_imag = ([enter_real], [enter_imag])
    for c in range(CHUNKS - 1):
        moved_real, moved_imag = complex_product(
            end_real[c : c + 1], end_imag[c : c + 1], in_real[-1], in_imag[-1]
        )
        in_real.append(moved_real + last_real[c : c + 1])
        in_imag.append(moved_imag + last_imag[c : c + 1])
    scanned(bar_ref, push_ref, (jnp.concatenate(in_real, axis=0), jnp.concatenate(in_imag, axis=0)))
    response = None
    for at, sign in enumerate((1.0, -1.0)):
        weights = block_diagonal(matrix(pack_ref, 2 + at, states) * sign, groups)
        high, low = pieces(push_ref[at], 2)
        for left, right in ((high, 0), (low, 0), (high, 1)):
            term = lax.dot_general(left, weights[right], NT, preferred_element_type=F32)
            response = term if response is None else response + term
    skip = packed(pack_ref, 9, mix_ref.shape[1])
    mixed = gelu(response + skip * chan.astype(F32)).astype(BF16)
    mix_ref[...] = jnp.dot(chunk_order(rows, True), mixed, preferred_element_type=F32).astype(BF16)


def conv_kernel(
    normed_ref, halo_ref, own_ref, up_ref, down_ref, left_ref, right_ref, pack_ref, mix_ref, weights_ref, w_ref
):
    width = mix_ref.shape[1]
    rows = normed_ref.shape[0]
    near, far = own_ref.shape[:2]
    part = w_ref.shape[1]
    z, y = (lax.axis_index("sp"), lax.axis_index("fs"))

    def put(j, turn, ref, at_j):
        at_q = (z + j) & 3
        at_y = (y + 2 * j + turn) & 3
        for k in range(far):
            at = (k * 4 + at_y) * 4 + at_q
            for i in range(5):
                piece = ref[at_j, k, i * part : (i + 1) * part]
                if i < 3:
                    w_ref[at, :, i * width : (i + 1) * width] = piece
                else:
                    weights_ref[at, :, (i - 3) * width : (i - 2) * width] = piece

    for j in range(near):
        put(j, 0, own_ref, j)
        put(j, 1, up_ref, j)
        put(j, 3, down_ref, j)
    for j in range(near // 2):
        put(j + 1, 2, left_ref, j)
        put(j - 1, 2, right_ref, j)
    w = w_ref[...].reshape(normed_ref.shape[1], 3 * width)
    taps = [packed(pack_ref, 10 + at, width) for at in range(3)]
    gain = jnp.concatenate([packed(pack_ref, 5 + at) for at in range(4)], axis=1)
    reach = len(taps) - 1
    inputs = jnp.concatenate([normalized(halo_ref[...], gain), normed_ref[...]], axis=0)
    here = jnp.dot(inputs, w, preferred_element_type=F32).astype(BF16).astype(F32)
    extended = (here[:, :width] * here[:, width : 2 * width]).astype(BF16).astype(F32)
    filtered = taps[reach] * extended[HALO:]
    for tap in range(reach):
        at = HALO - reach + tap
        filtered = filtered + taps[tap] * extended[at : at + rows]
    mix_ref[...] = (here[HALO:, 2 * width :] * filtered).astype(BF16)


def out_kernel(state_ref, conv_ref, w_ref, mine_ref, theirs_ref):
    chips, rows = mine_ref.shape[:2]
    core = lax.axis_index("tp") & 1

    def rows_of(ref, parity):
        return [ref[pl.ds(pl.multiple_of((2 * x + parity) * rows, rows), rows), :] for x in range(chips)]

    mixes = jnp.concatenate(
        [
            jnp.concatenate([*rows_of(ref, core), *rows_of(ref, 1 - core)], axis=0)
            for ref in (state_ref, conv_ref)
        ],
        axis=1,
    )
    per = 512
    tall, part, wide = w_ref.shape
    for at in range(0, tall * part, per):
        w = w_ref[at // part : (at + per) // part].reshape(per, wide)
        product = lax.dot_general(mixes, w, NT, preferred_element_type=F32).astype(BF16)
        for x in range(chips):
            mine_ref[x, :, at : at + per] = product[x * rows : (x + 1) * rows]
            theirs_ref[x, :, at : at + per] = product[(chips + x) * rows : (chips + x + 1) * rows]


def add_kernel(left_ref, right_ref, sum_ref):
    sum_ref[...] = (left_ref[...].astype(F32) + right_ref[...].astype(F32)).astype(BF16)


def moved(x, dz, dy):
    sp, fs = (lax.axis_size("sp"), lax.axis_size("fs"))
    pairs = [
        (z * fs + y, ((z - dz) % sp) * fs + (y - dy) % fs) for z in range(sp) for y in range(fs)
    ]
    return lax.ppermute(x, ("sp", "fs"), pairs)


def all_shards(far):
    near = [far] + [moved(far, dz, dy) for dz, dy in ((1, 2), (2, 0), (-1, 2))]
    own = jnp.stack(near)
    half = own[:2]
    return (own, moved(own, 0, 1), moved(own, 0, -1), moved(half, 1, 0), moved(half, -1, 0))


def call(kernel, out_shape, flops, *args, smem=0, anywhere=0, scratch=(), limit=20 << 20):
    vmem = pl.BlockSpec(memory_space=pltpu.VMEM)
    first = [pl.BlockSpec(memory_space=pltpu.SMEM)] * smem + [pl.BlockSpec(memory_space=pl.ANY)] * anywhere
    return pl.pallas_call(
        kernel,
        out_shape=out_shape,
        in_specs=first + [vmem] * (len(args) - len(first)),
        out_specs=jax.tree.map(lambda _: vmem, out_shape),
        scratch_shapes=list(scratch),
        cost_estimate=pl.CostEstimate(flops=flops, bytes_accessed=1 << 20, transcendentals=0),
        compiler_params=pltpu.CompilerParams(vmem_limit_bytes=limit),
    )(*args)


def shape(dims, dtype=F32):
    return jax.ShapeDtypeStruct(dims, dtype)


def body(
    tokens,
    norm_gain,
    w_state_in,
    w_value,
    w_outer,
    w_inner,
    w_state_out,
    w_conv_out,
    log_step,
    decay_real,
    frequency,
    step_rate,
    input_real,
    input_imag,
    read_real,
    read_imag,
    skip_gain,
    conv_taps,
    initial_state,
):
    rows, features = tokens.shape[1:]
    groups, states = decay_real.shape
    group = skip_gain.shape[1]
    flat = groups * states
    width = groups * group
    count = lax.axis_size("sp")

    part = w_state_in.shape[0] // 4
    weights = (w_state_in, w_value, w_inner, w_outer, w_state_out, w_conv_out)
    shards = call(
        pack_kernel,
        shape((count, w_state_in.shape[0] + 5 * part, width), BF16),
        1 << 20,
        *weights,
        anywhere=len(weights),
        scratch=(
            pltpu.VMEM((len(weights), *w_state_in.shape), BF16),
            pltpu.SemaphoreType.DMA((len(weights),)),
        ),
        limit=None,
    )
    far = lax.all_to_all(shards, "sp", 0, 0, tiled=True)
    fs = lax.axis_size("fs")
    many, rest = call(
        split_kernel, (shape((fs, count, 4 * part, width), BF16), shape((count, 5 * part, width), BF16)), 1 << 20, far
    )
    state_weights = lax.all_to_all(many, "fs", 0, 0, tiled=True)
    own, up, down, left, right = all_shards(rest)
    edge = lax.ppermute(tokens[0, rows - HALO :], "sp", [(i, i + 1) for i in range(count - 1)])
    gain = norm_gain[None]
    into = [jnp.swapaxes(x, 1, 2).reshape(width, states) for x in (input_real, input_imag)]
    normed, bar, pack = call(
        prep_kernel,
        (shape((rows, features), BF16), shape((2, rows, flat)), shape((width // 2 + PACKED, flat))),
        1 << 30,
        log_step,
        tokens[0],
        gain,
        step_rate,
        decay_real,
        frequency,
        initial_state[0].reshape(2 * groups, states),
        *into,
        read_real.reshape(width, states),
        read_imag.reshape(width, states),
        skip_gain,
        conv_taps,
        smem=1,
        scratch=(pltpu.VMEM((rows, 16), F32),),
    )
    chan, end = call(
        functools.partial(local_kernel, groups),
        (shape((rows, width), BF16), shape((count, 2, flat + 128))),
        1 << 29,
        normed,
        state_weights,
        bar,
        pack,
        step_rate,
        scratch=(pltpu.VMEM((2, rows, flat), F32),),
    )
    ends = lax.all_to_all(end, "sp", 0, 0, tiled=True)
    conv_mix, out_weights = call(
        conv_kernel,
        (shape((rows, width), BF16), shape((features // part, part, 2 * width), BF16)),
        1 << 29,
        normed,
        edge,
        own,
        up,
        down,
        left,
        right,
        pack,
        scratch=(pltpu.VMEM((features // part, part, 3 * width), BF16),),
    )
    state_mix, closing = call(
        functools.partial(read_kernel, groups),
        (shape((rows, width), BF16), shape((2, groups, states // count))),
        1 << 29,
        ends,
        bar,
        chan,
        pack,
        scratch=(pltpu.VMEM((2, rows, flat), F32),),
    )
    tp = lax.axis_size("tp")
    piece = shape((tp // 2, rows // tp, features), BF16)
    mine, theirs = call(out_kernel, (piece, piece), 1 << 29, state_mix, conv_mix, out_weights)
    theirs = lax.ppermute(theirs, "tp", [(i, i ^ 1) for i in range(tp)])
    pair = call(add_kernel, piece, 1 << 20, mine, theirs)
    same_core = [[i for i in range(core, tp, 2)] for core in range(2)]
    parts = lax.all_to_all(pair, "tp", 0, 0, tiled=True, axis_index_groups=same_core)
    mixed = jnp.sum(parts.astype(F32), axis=0).astype(BF16)
    return (mixed[None], closing[None])


def solution(mesh):
    return jax.shard_map(
        body,
        mesh=mesh,
        in_specs=(
            P("fs", "sp", None),
            P(),
            P(("sp", "fs"), "tp"),
            P(("sp", "fs"), "tp"),
            P(("sp", "fs"), "tp"),
            P(("sp", "fs"), "tp"),
            P(("sp", "fs"), "tp"),
            P(("sp", "fs"), "tp"),
            P("tp"),
            P("tp", None),
            P("tp", None),
            P("fs", "sp"),
            P("tp", None, None),
            P("tp", None, None),
            P("tp", None, None),
            P("tp", None, None),
            P("tp", None),
            P(None, "tp"),
            P("fs", None, "tp", None),
        ),
        out_specs=(P("fs", ("sp", "tp"), None), P("fs", None, "tp", "sp")),
        check_vma=False,
    )
```

```python
import functools

import jax
import jax.numpy as jnp
from jax import lax
from jax.experimental import pallas as pl
from jax.experimental.pallas import tpu as pltpu
from jax.sharding import PartitionSpec as P


F32 = jnp.float32
BF16 = jnp.bfloat16
CHUNKS = 8
HALO = 16
PACKED = 16
NT = (((1,), (1,)), ((), ()))


def complex_product(left_real, left_imag, right_real, right_imag):
    return (
        left_real * right_real - left_imag * right_imag,
        left_real * right_imag + left_imag * right_real,
    )


def sine_cosine(angle):
    turns = jnp.floor(angle * 0.6366197723675814 + 0.5)
    r = angle - turns * 1.5703125
    r = r - turns * 4.837512969970703e-4
    r = r - turns * 7.549789948768648e-8
    r2 = r * r
    sine = r + r * r2 * (-1.6666654611e-1 + r2 * (8.3321608736e-3 + r2 * -1.9515295891e-4))
    cosine = (
        1.0
        - 0.5 * r2
        + r2 * r2 * (4.166664568298827e-2 + r2 * (-1.388731625493765e-3 + r2 * 2.443315711809948e-5))
    )
    quadrant = turns.astype(jnp.int32)
    odd = (quadrant & 1) == 1
    flip_sine = (quadrant & 2) == 2
    flip_cosine = ((quadrant + 1) & 2) == 2
    base_sine = jnp.where(odd, cosine, sine)
    base_cosine = jnp.where(odd, sine, cosine)
    return (
        jnp.where(flip_sine, -base_sine, base_sine),
        jnp.where(flip_cosine, -base_cosine, base_cosine),
    )


def iota(dims, axis):
    return lax.broadcasted_iota(jnp.int32, dims, axis)


def pieces(x, count):
    found = []
    for _ in range(count):
        part = x.astype(BF16)
        found.append(part)
        x = x - part.astype(F32)
    return found


def picked(x, selector, count=3):
    total = None
    for part in pieces(x, count):
        term = jnp.dot(part, selector, preferred_element_type=F32)
        total = term if total is None else total + term
    return total


def repeat_selector(narrow, wide):
    return (iota((narrow, wide), 1) % narrow == iota((narrow, wide), 0)).astype(BF16)


def flattened(x, groups):
    rows, narrow = x.shape
    wide = groups * narrow
    tiled = picked(x, repeat_selector(narrow, wide))
    own = iota((rows, wide), 1) // narrow == iota((rows, wide), 0) % groups
    tiled = jnp.where(own, tiled, 0.0)
    return [jnp.sum(tiled[at : at + groups], axis=0, keepdims=True) for at in range(0, rows, groups)]


def block_diagonal(x, groups):
    rows, narrow = x.shape
    wide = groups * narrow
    selector = repeat_selector(narrow, wide)
    own = iota((rows, wide), 1) // narrow == iota((rows, wide), 0) // (rows // groups)
    return [
        jnp.where(own, jnp.dot(part, selector, preferred_element_type=F32), 0.0).astype(BF16)
        for part in pieces(x, 2)
    ]


def spread_steps(log_ref, groups, states):
    lane = iota((1, groups * states), 1) // states
    out = jnp.zeros((1, groups * states), F32)
    for g in range(groups):
        out = jnp.where(lane == g, log_ref[g], out)
    return jnp.exp(out)


def chunk_order(rows, flip):
    r, c = (iota((rows, rows), 1 if flip else 0), iota((rows, rows), 0 if flip else 1))
    steps = rows // CHUNKS
    return (c == (r % CHUNKS) * steps + r // CHUNKS).astype(BF16)


def normalized(x, gain):
    x = x.astype(F32)
    mean_square = jnp.mean(x * x, axis=-1, keepdims=True)
    return (x * lax.rsqrt(mean_square + 1e-06) * gain).astype(BF16)


def pack_kernel(*refs):
    count = 6
    sources, out_ref, landed, sems = (refs[:count], refs[count], refs[count + 1], refs[count + 2])
    copies = [
        pltpu.make_async_copy(source, landed.at[i], sems.at[i]) for i, source in enumerate(sources)
    ]
    for copy in copies:
        copy.start()
    for copy in copies:
        copy.wait()
    tall = landed.shape[1]
    part = tall // 4
    for z in range(out_ref.shape[0]):
        out_ref[z, :tall] = landed[0]
        q = z % 4
        for i in range(1, count):
            at = tall + (i - 1) * part
            out_ref[z, at : at + part] = landed[i, q * part : (q + 1) * part]


def prep_kernel(
    log_ref, tokens_ref, gain_ref, rate_ref, decay_ref, freq_ref, initial_ref, in_real_ref, in_imag_ref,
    out_real_ref, out_imag_ref, skip_ref, taps_ref, normed_ref, bar_ref, pack_ref, column_ref,
):
    groups, states = decay_ref.shape
    flat = groups * states
    rows = tokens_ref.shape[0]
    part = 64

    def norm(i, _):
        at = pl.ds(pl.multiple_of(i * part, part), part)
        normed_ref[at, :] = normalized(tokens_ref[at, :], gain_ref[...])
        return 0

    lax.fori_loop(0, rows // part, norm, 0)
    order = chunk_order(rows, False)
    column = None
    for piece in pieces(jnp.broadcast_to(rate_ref[...], (16, rows)), 3):
        term = lax.dot_general(order, piece, NT, preferred_element_type=F32)
        column = term if column is None else column + term
    column_ref[...] = column
    (decay,) = flattened(decay_ref[...], groups)
    (freq,) = flattened(freq_ref[...], groups)
    scale = spread_steps(log_ref, groups, states)
    top = in_real_ref.shape[0] // 2
    for at, ref in enumerate((in_real_ref, in_imag_ref, out_real_ref, out_imag_ref)):
        for i in range(2):
            lanes = slice((2 * at + i) * states, (2 * at + i + 1) * states)
            pack_ref[:top, lanes] = ref[i * top : (i + 1) * top]
    (skip,) = flattened(skip_ref[...], groups)
    gain_rows = gain_ref.shape[1] // flat
    for at, row in enumerate(
        (
            decay,
            freq,
            scale,
            *flattened(initial_ref[...], groups),
            *(gain_ref[:, i * flat : (i + 1) * flat] for i in range(gain_rows)),
            skip,
            *(taps_ref[i : i + 1] for i in range(taps_ref.shape[0])),
        )
    ):
        pack_ref[top + at : top + at + 1, : row.shape[1]] = row
    steps = rows // CHUNKS

    def advance(j, carry):
        at = pl.ds(pl.multiple_of(j * CHUNKS, CHUNKS), CHUNKS)
        step = column_ref[at, 0:1] * scale
        grow = jnp.exp(step * decay)
        sine, cosine = sine_cosine(step * freq)
        bar_real, bar_imag = (grow * cosine, grow * sine)
        bar_ref[0, at, :] = bar_real
        bar_ref[1, at, :] = bar_imag
        return 0

    lax.fori_loop(0, steps, advance, 0)


def packed(pack_ref, at, wide=None):
    top = pack_ref.shape[0] - PACKED
    return pack_ref[top + at : top + at + 1, : pack_ref.shape[1] if wide is None else wide]


def matrix(pack_ref, at, states):
    top = pack_ref.shape[0] - PACKED
    halves = [pack_ref[:top, (2 * at + i) * states : (2 * at + i + 1) * states] for i in range(2)]
    return jnp.concatenate(halves, axis=0)


def driven(chan, pack_ref, bar_ref, groups, push_ref):
    flat = bar_ref.shape[2]
    drives = []
    for at in range(2):
        high, low = block_diagonal(matrix(pack_ref, at, flat // groups), groups)
        drives.append(
            jnp.dot(chan, high, preferred_element_type=F32) + jnp.dot(chan, low, preferred_element_type=F32)
        )
    decay, freq = (packed(pack_ref, 0), packed(pack_ref, 1))
    inverse = 1.0 / (decay * decay + freq * freq)
    bar_imag = bar_ref[1]
    less_real = bar_ref[0] - 1.0
    push_ref[0], push_ref[1] = complex_product(
        (less_real * decay + bar_imag * freq) * inverse,
        (bar_imag * decay - less_real * freq) * inverse,
        drives[0],
        drives[1],
    )


def scanned(bar_ref, push_ref, start):
    steps = bar_ref.shape[1] // CHUNKS

    def advance(j, carry):
        at = pl.ds(pl.multiple_of(j * CHUNKS, CHUNKS), CHUNKS)
        real, imag = complex_product(bar_ref[0, at, :], bar_ref[1, at, :], carry[0], carry[1])
        real = real + push_ref[0, at, :]
        imag = imag + push_ref[1, at, :]
        push_ref[0, at, :] = real
        push_ref[1, at, :] = imag
        return (real, imag)

    lax.fori_loop(0, steps, advance, start, unroll=4)


def chunk_maps(bar_ref, push_ref):
    steps, flat = (bar_ref.shape[1] // CHUNKS, bar_ref.shape[2])

    def advance(j, carry):
        at = pl.ds(pl.multiple_of(j * CHUNKS, CHUNKS), CHUNKS)
        bar = (bar_ref[0, at, :], bar_ref[1, at, :])
        product = complex_product(*bar, carry[0], carry[1])
        real, imag = complex_product(*bar, carry[2], carry[3])
        return (*product, real + push_ref[0, at, :], imag + push_ref[1, at, :])

    one, zero = (jnp.ones((CHUNKS, flat), F32), jnp.zeros((CHUNKS, flat), F32))
    return lax.fori_loop(0, steps, advance, (one, zero, zero, zero), unroll=4)


def local_kernel(
    groups, normed_ref, w_ref, bar_ref, pack_ref, rate_ref, chan_ref, end_ref, push_ref
):
    rows = normed_ref.shape[0]
    fs, sp = w_ref.shape[:2]
    w = jnp.concatenate([w_ref[f, z] for z in range(sp) for f in range(fs)], axis=0)
    state_in = jnp.dot(normed_ref[...], w, preferred_element_type=F32).astype(BF16)
    chan = jnp.dot(chunk_order(rows, False), state_in, preferred_element_type=F32).astype(BF16)
    chan_ref[...] = chan
    flat = bar_ref.shape[2]
    driven(chan, pack_ref, bar_ref, groups, push_ref)
    end_real, end_imag, last_real, last_imag = chunk_maps(bar_ref, push_ref)
    real, imag = (last_real[0:1], last_imag[0:1])
    for c in range(1, CHUNKS):
        moved_real, moved_imag = complex_product(end_real[c : c + 1], end_imag[c : c + 1], real, imag)
        real = moved_real + last_real[c : c + 1]
        imag = moved_imag + last_imag[c : c + 1]
    end = jnp.concatenate([real, imag], axis=0)
    whole = jnp.sum(rate_ref[...], axis=1, keepdims=True)
    whole = jnp.broadcast_to(whole, (2, end_ref.shape[2] - flat))
    for z in range(end_ref.shape[0]):
        end_ref[z, :, :flat] = end
        end_ref[z, :, flat:] = whole


def split_kernel(far_ref, many_ref, rest_ref):
    tall = many_ref.shape[2]
    rest_ref[...] = far_ref[:, tall:]
    for copy in range(many_ref.shape[0]):
        many_ref[copy] = far_ref[:, :tall]


def gelu(v):
    return 0.5 * v * (1.0 + jnp.tanh(0.7978845608 * (v + 0.044715 * v * v * v)))


def read_kernel(
    groups, ends_ref, bar_ref, chan_ref, pack_ref, mix_ref, closing_ref, push_ref
):
    flat = bar_ref.shape[2]
    states = flat // groups
    spans = ends_ref.shape[0]
    here = lax.axis_index("sp")
    decay, freq, scale, enter_real, enter_imag = (packed(pack_ref, at) for at in range(5))
    real, imag = (enter_real, enter_imag)
    elapsed = jnp.concatenate([ends_ref[z, 0:1, flat:] for z in range(spans)], axis=0)[:, 0:1] * scale
    grow = jnp.exp(elapsed * decay)
    sine, cosine = sine_cosine(elapsed * freq)
    map_real, map_imag = (grow * cosine, grow * sine)
    for z in range(spans):
        now = here == z
        enter_real = jnp.where(now, real, enter_real)
        enter_imag = jnp.where(now, imag, enter_imag)
        moved_real, moved_imag = complex_product(map_real[z : z + 1], map_imag[z : z + 1], real, imag)
        real = moved_real + ends_ref[z, 0:1, :flat]
        imag = moved_imag + ends_ref[z, 1:2, :flat]
    share = states // spans
    lane = iota((flat, share), 0) % states
    wanted = (lane == here * share + iota((flat, share), 1)).astype(BF16)
    own = iota((groups, flat), 1) // states == iota((groups, flat), 0)
    for at, row in enumerate((real, imag)):
        closing_ref[at] = picked(jnp.where(own, jnp.broadcast_to(row, (groups, flat)), 0.0), wanted)
    rows = bar_ref.shape[1]
    chan = chan_ref[...]
    driven(chan, pack_ref, bar_ref, groups, push_ref)
    end_real, end_imag, last_real, last_imag = chunk_maps(bar_ref, push_ref)
    in_real, in_imag = ([enter_real], [enter_imag])
    for c in range(CHUNKS - 1):
        moved_real, moved_imag = complex_product(
            end_real[c : c + 1], end_imag[c : c + 1], in_real[-1], in_imag[-1]
        )
        in_real.append(moved_real + last_real[c : c + 1])
        in_imag.append(moved_imag + last_imag[c : c + 1])
    scanned(bar_ref, push_ref, (jnp.concatenate(in_real, axis=0), jnp.concatenate(in_imag, axis=0)))
    response = None
    for at, sign in enumerate((1.0, -1.0)):
        weights = block_diagonal(matrix(pack_ref, 2 + at, states) * sign, groups)
        high, low = pieces(push_ref[at], 2)
        for left, right in ((high, 0), (low, 0), (high, 1)):
            term = lax.dot_general(left, weights[right], NT, preferred_element_type=F32)
            response = term if response is None else response + term
    skip = packed(pack_ref, 9, mix_ref.shape[1])
    mixed = gelu(response + skip * chan.astype(F32)).astype(BF16)
    mix_ref[...] = jnp.dot(chunk_order(rows, True), mixed, preferred_element_type=F32).astype(BF16)


def conv_kernel(
    state_ref, normed_ref, halo_ref, own_ref, up_ref, down_ref, left_ref, right_ref, pack_ref,
    mine_ref, theirs_ref, mix_ref, weights_ref, w_ref,
):
    width = mix_ref.shape[1]
    rows = normed_ref.shape[0]
    near, far = own_ref.shape[:2]
    part = w_ref.shape[1]
    z, y = (lax.axis_index("sp"), lax.axis_index("fs"))

    def put(j, turn, ref, at_j):
        at_q = (z + j) & 3
        at_y = (y + 2 * j + turn) & 3
        for k in range(far):
            at = (k * 4 + at_y) * 4 + at_q
            for i in range(5):
                piece = ref[at_j, k, i * part : (i + 1) * part]
                if i < 3:
                    w_ref[at, :, i * width : (i + 1) * width] = piece
                else:
                    weights_ref[at, :, (i - 3) * width : (i - 2) * width] = piece

    for j in range(near):
        put(j, 0, own_ref, j)
        put(j, 1, up_ref, j)
        put(j, 3, down_ref, j)
    for j in range(near // 2):
        put(j + 1, 2, left_ref, j)
        put(j - 1, 2, right_ref, j)
    w = w_ref[...].reshape(normed_ref.shape[1], 3 * width)
    taps = [packed(pack_ref, 10 + at, width) for at in range(3)]
    gain = jnp.concatenate([packed(pack_ref, 5 + at) for at in range(4)], axis=1)
    reach = len(taps) - 1
    inputs = jnp.concatenate([normalized(halo_ref[...], gain), normed_ref[...]], axis=0)
    here = jnp.dot(inputs, w, preferred_element_type=F32).astype(BF16).astype(F32)
    extended = (here[:, :width] * here[:, width : 2 * width]).astype(BF16).astype(F32)
    filtered = taps[reach] * extended[HALO:]
    for tap in range(reach):
        at = HALO - reach + tap
        filtered = filtered + taps[tap] * extended[at : at + rows]
    mix_ref[...] = (here[HALO:, 2 * width :] * filtered).astype(BF16)
    output(state_ref, mix_ref, weights_ref, mine_ref, theirs_ref)


def output(state_ref, conv_ref, w_ref, mine_ref, theirs_ref):
    chips, rows = mine_ref.shape[:2]
    core = lax.axis_index("tp") & 1

    def rows_of(ref, parity):
        return [ref[pl.ds(pl.multiple_of((2 * x + parity) * rows, rows), rows), :] for x in range(chips)]

    mixes = jnp.concatenate(
        [
            jnp.concatenate([*rows_of(ref, core), *rows_of(ref, 1 - core)], axis=0)
            for ref in (state_ref, conv_ref)
        ],
        axis=1,
    )
    per = 512
    tall, part, wide = w_ref.shape
    for at in range(0, tall * part, per):
        w = w_ref[at // part : (at + per) // part].reshape(per, wide)
        product = lax.dot_general(mixes, w, NT, preferred_element_type=F32).astype(BF16)
        for x in range(chips):
            mine_ref[x, :, at : at + per] = product[x * rows : (x + 1) * rows]
            theirs_ref[x, :, at : at + per] = product[(chips + x) * rows : (chips + x + 1) * rows]


def add_kernel(left_ref, right_ref, *out_refs):
    chips = len(out_refs)
    chip = lax.axis_index("tp") >> 1
    for k, ref in enumerate(out_refs):
        to = (chip + k) & (chips - 1)
        ref[...] = (left_ref[to].astype(F32) + right_ref[to].astype(F32)).astype(BF16)


def moved(x, dz, dy):
    sp, fs = (lax.axis_size("sp"), lax.axis_size("fs"))
    pairs = [
        (z * fs + y, ((z - dz) % sp) * fs + (y - dy) % fs) for z in range(sp) for y in range(fs)
    ]
    return lax.ppermute(x, ("sp", "fs"), pairs)


def all_shards(far):
    near = [far] + [moved(far, dz, dy) for dz, dy in ((1, 2), (2, 0), (-1, 2))]
    own = jnp.stack(near)
    half = own[:2]
    return (own, moved(own, 0, 1), moved(own, 0, -1), moved(half, 1, 0), moved(half, -1, 0))


def call(kernel, out_shape, flops, *args, smem=0, anywhere=0, scratch=(), limit=20 << 20):
    vmem = pl.BlockSpec(memory_space=pltpu.VMEM)
    first = [pl.BlockSpec(memory_space=pltpu.SMEM)] * smem + [pl.BlockSpec(memory_space=pl.ANY)] * anywhere
    return pl.pallas_call(
        kernel,
        out_shape=out_shape,
        in_specs=first + [vmem] * (len(args) - len(first)),
        out_specs=jax.tree.map(lambda _: vmem, out_shape),
        scratch_shapes=list(scratch),
        cost_estimate=pl.CostEstimate(flops=flops, bytes_accessed=1 << 20, transcendentals=0),
        compiler_params=pltpu.CompilerParams(vmem_limit_bytes=limit),
    )(*args)


def shape(dims, dtype=F32):
    return jax.ShapeDtypeStruct(dims, dtype)


def body(
    tokens,
    norm_gain,
    w_state_in,
    w_value,
    w_outer,
    w_inner,
    w_state_out,
    w_conv_out,
    log_step,
    decay_real,
    frequency,
    step_rate,
    input_real,
    input_imag,
    read_real,
    read_imag,
    skip_gain,
    conv_taps,
    initial_state,
):
    rows, features = tokens.shape[1:]
    groups, states = decay_real.shape
    group = skip_gain.shape[1]
    flat = groups * states
    width = groups * group
    count = lax.axis_size("sp")

    part = w_state_in.shape[0] // 4
    weights = (w_state_in, w_value, w_inner, w_outer, w_state_out, w_conv_out)
    shards = call(
        pack_kernel,
        shape((count, w_state_in.shape[0] + 5 * part, width), BF16),
        1 << 20,
        *weights,
        anywhere=len(weights),
        scratch=(
            pltpu.VMEM((len(weights), *w_state_in.shape), BF16),
            pltpu.SemaphoreType.DMA((len(weights),)),
        ),
        limit=None,
    )
    far = lax.all_to_all(shards, "sp", 0, 0, tiled=True)
    fs = lax.axis_size("fs")
    many, rest = call(
        split_kernel,
        (shape((fs, count, 4 * part, width), BF16), shape((count, 5 * part, width), BF16)),
        1 << 20,
        far,
    )
    state_weights = lax.all_to_all(many, "fs", 0, 0, tiled=True)
    own, up, down, left, right = all_shards(rest)
    edge = lax.ppermute(tokens[0, rows - HALO :], "sp", [(i, i + 1) for i in range(count - 1)])
    gain = norm_gain[None]
    into = [jnp.swapaxes(x, 1, 2).reshape(width, states) for x in (input_real, input_imag)]
    normed, bar, pack = call(
        prep_kernel,
        (shape((rows, features), BF16), shape((2, rows, flat)), shape((width // 2 + PACKED, flat))),
        1 << 30,
        log_step,
        tokens[0],
        gain,
        step_rate,
        decay_real,
        frequency,
        initial_state[0].reshape(2 * groups, states),
        *into,
        read_real.reshape(width, states),
        read_imag.reshape(width, states),
        skip_gain,
        conv_taps,
        smem=1,
        scratch=(pltpu.VMEM((rows, 16), F32),),
    )
    chan, end = call(
        functools.partial(local_kernel, groups),
        (shape((rows, width), BF16), shape((count, 2, flat + 128))),
        1 << 29,
        normed,
        state_weights,
        bar,
        pack,
        step_rate,
        scratch=(pltpu.VMEM((2, rows, flat), F32),),
    )
    ends = lax.all_to_all(end, "sp", 0, 0, tiled=True)
    state_mix, closing = call(
        functools.partial(read_kernel, groups),
        (shape((rows, width), BF16), shape((2, groups, states // count))),
        1 << 29,
        ends,
        bar,
        chan,
        pack,
        scratch=(pltpu.VMEM((2, rows, flat), F32),),
    )
    tp = lax.axis_size("tp")
    chips = tp // 2
    piece = shape((chips, rows // tp, features), BF16)
    mine, theirs = call(
        conv_kernel,
        (piece, piece),
        1 << 29,
        state_mix,
        normed,
        edge,
        own,
        up,
        down,
        left,
        right,
        pack,
        scratch=(
            pltpu.VMEM((rows, width), BF16),
            pltpu.VMEM((features // part, part, 2 * width), BF16),
            pltpu.VMEM((features // part, part, 3 * width), BF16),
        ),
    )
    theirs = lax.ppermute(theirs, "tp", [(i, i ^ 1) for i in range(tp)])
    sent = call(add_kernel, (shape((rows // tp, features), BF16),) * chips, 1 << 20, mine, theirs)
    total = sent[0].astype(F32)
    for k in range(1, chips):
        pairs = [(i, (i + 2 * k) % tp) for i in range(tp)]
        total = total + lax.ppermute(sent[k], "tp", pairs).astype(F32)
    mixed = total.astype(BF16)
    return (mixed[None], closing[None])


def solution(mesh):
    return jax.shard_map(
        body,
        mesh=mesh,
        in_specs=(
            P("fs", "sp", None),
            P(),
            P(("sp", "fs"), "tp"),
            P(("sp", "fs"), "tp"),
            P(("sp", "fs"), "tp"),
            P(("sp", "fs"), "tp"),
            P(("sp", "fs"), "tp"),
            P(("sp", "fs"), "tp"),
            P("tp"),
            P("tp", None),
            P("tp", None),
            P("fs", "sp"),
            P("tp", None, None),
            P("tp", None, None),
            P("tp", None, None),
            P("tp", None, None),
            P("tp", None),
            P(None, "tp"),
            P("fs", None, "tp", None),
        ),
        out_specs=(P("fs", ("sp", "tp"), None), P("fs", None, "tp", "sp")),
        check_vma=False,
    )
```

```python
import functools

import jax
import jax.numpy as jnp
from jax import lax
from jax.experimental import pallas as pl
from jax.experimental.pallas import tpu as pltpu
from jax.sharding import PartitionSpec as P


F32 = jnp.float32
BF16 = jnp.bfloat16
CHUNKS = 8
HALO = 16
PACKED = 16
CLASS = ((0, 0), (2, 1), (-2, -1), (0, 2))
NEAR = ((1, 0), (-1, 0), (0, 1), (0, -1))
NT = (((1,), (1,)), ((), ()))


def complex_product(left_real, left_imag, right_real, right_imag):
    return (
        left_real * right_real - left_imag * right_imag,
        left_real * right_imag + left_imag * right_real,
    )


def sine_cosine(angle):
    turns = jnp.floor(angle * 0.6366197723675814 + 0.5)
    r = angle - turns * 1.5703125
    r = r - turns * 4.837512969970703e-4
    r = r - turns * 7.549789948768648e-8
    r2 = r * r
    sine = r + r * r2 * (-1.6666654611e-1 + r2 * (8.3321608736e-3 + r2 * -1.9515295891e-4))
    cosine = (
        1.0
        - 0.5 * r2
        + r2 * r2 * (4.166664568298827e-2 + r2 * (-1.388731625493765e-3 + r2 * 2.443315711809948e-5))
    )
    quadrant = turns.astype(jnp.int32)
    odd = (quadrant & 1) == 1
    flip_sine = (quadrant & 2) == 2
    flip_cosine = ((quadrant + 1) & 2) == 2
    base_sine = jnp.where(odd, cosine, sine)
    base_cosine = jnp.where(odd, sine, cosine)
    return (
        jnp.where(flip_sine, -base_sine, base_sine),
        jnp.where(flip_cosine, -base_cosine, base_cosine),
    )


def iota(dims, axis):
    return lax.broadcasted_iota(jnp.int32, dims, axis)


def pieces(x, count):
    found = []
    for _ in range(count):
        part = x.astype(BF16)
        found.append(part)
        x = x - part.astype(F32)
    return found


def picked(x, selector, count=3):
    total = None
    for part in pieces(x, count):
        term = jnp.dot(part, selector, preferred_element_type=F32)
        total = term if total is None else total + term
    return total


def repeat_selector(narrow, wide):
    return (iota((narrow, wide), 1) % narrow == iota((narrow, wide), 0)).astype(BF16)


def flattened(x, groups):
    rows, narrow = x.shape
    wide = groups * narrow
    tiled = picked(x, repeat_selector(narrow, wide))
    own = iota((rows, wide), 1) // narrow == iota((rows, wide), 0) % groups
    tiled = jnp.where(own, tiled, 0.0)
    return [jnp.sum(tiled[at : at + groups], axis=0, keepdims=True) for at in range(0, rows, groups)]


def block_diagonal(x, groups):
    rows, narrow = x.shape
    wide = groups * narrow
    selector = repeat_selector(narrow, wide)
    own = iota((rows, wide), 1) // narrow == iota((rows, wide), 0) // (rows // groups)
    return [
        jnp.where(own, jnp.dot(part, selector, preferred_element_type=F32), 0.0).astype(BF16)
        for part in pieces(x, 2)
    ]


def spread_steps(log_ref, groups, states):
    lane = iota((1, groups * states), 1) // states
    out = jnp.zeros((1, groups * states), F32)
    for g in range(groups):
        out = jnp.where(lane == g, log_ref[g], out)
    return jnp.exp(out)


def chunk_order(rows, flip):
    r, c = (iota((rows, rows), 1 if flip else 0), iota((rows, rows), 0 if flip else 1))
    steps = rows // CHUNKS
    return (c == (r % CHUNKS) * steps + r // CHUNKS).astype(BF16)


def normalized(x, gain):
    x = x.astype(F32)
    mean_square = jnp.mean(x * x, axis=-1, keepdims=True)
    return (x * lax.rsqrt(mean_square + 1e-06) * gain).astype(BF16)


def pack_kernel(*refs):
    count = 6
    sources, out_ref, landed, sems = (refs[:count], refs[count], refs[count + 1], refs[count + 2])
    copies = [
        pltpu.make_async_copy(source, landed.at[i], sems.at[i]) for i, source in enumerate(sources)
    ]
    for copy in copies:
        copy.start()
    for copy in copies:
        copy.wait()
    tall = landed.shape[1]
    part = tall // 4
    for z in range(out_ref.shape[0]):
        out_ref[z, :tall] = landed[0]
        q = z % 4
        for i in range(1, count):
            at = tall + (i - 1) * part
            out_ref[z, at : at + part] = landed[i, q * part : (q + 1) * part]


def prep_kernel(
    log_ref, tokens_ref, gain_ref, rate_ref, decay_ref, freq_ref, initial_ref, in_real_ref, in_imag_ref,
    out_real_ref, out_imag_ref, skip_ref, taps_ref, normed_ref, bar_ref, pack_ref, column_ref,
):
    groups, states = decay_ref.shape
    flat = groups * states
    rows = tokens_ref.shape[0]
    part = 64

    def norm(i, _):
        at = pl.ds(pl.multiple_of(i * part, part), part)
        normed_ref[at, :] = normalized(tokens_ref[at, :], gain_ref[...])
        return 0

    lax.fori_loop(0, rows // part, norm, 0)
    order = chunk_order(rows, False)
    column = None
    for piece in pieces(jnp.broadcast_to(rate_ref[...], (16, rows)), 3):
        term = lax.dot_general(order, piece, NT, preferred_element_type=F32)
        column = term if column is None else column + term
    column_ref[...] = column
    (decay,) = flattened(decay_ref[...], groups)
    (freq,) = flattened(freq_ref[...], groups)
    scale = spread_steps(log_ref, groups, states)
    top = in_real_ref.shape[0] // 2
    for at, ref in enumerate((in_real_ref, in_imag_ref, out_real_ref, out_imag_ref)):
        for i in range(2):
            lanes = slice((2 * at + i) * states, (2 * at + i + 1) * states)
            pack_ref[:top, lanes] = ref[i * top : (i + 1) * top]
    (skip,) = flattened(skip_ref[...], groups)
    gain_rows = gain_ref.shape[1] // flat
    for at, row in enumerate(
        (
            decay,
            freq,
            scale,
            *flattened(initial_ref[...], groups),
            *(gain_ref[:, i * flat : (i + 1) * flat] for i in range(gain_rows)),
            skip,
            *(taps_ref[i : i + 1] for i in range(taps_ref.shape[0])),
        )
    ):
        pack_ref[top + at : top + at + 1, : row.shape[1]] = row
    steps = rows // CHUNKS

    def advance(j, carry):
        at = pl.ds(pl.multiple_of(j * CHUNKS, CHUNKS), CHUNKS)
        step = column_ref[at, 0:1] * scale
        grow = jnp.exp(step * decay)
        sine, cosine = sine_cosine(step * freq)
        bar_real, bar_imag = (grow * cosine, grow * sine)
        bar_ref[0, at, :] = bar_real
        bar_ref[1, at, :] = bar_imag
        return 0

    lax.fori_loop(0, steps, advance, 0)


def packed(pack_ref, at, wide=None):
    top = pack_ref.shape[0] - PACKED
    return pack_ref[top + at : top + at + 1, : pack_ref.shape[1] if wide is None else wide]


def matrix(pack_ref, at, states):
    top = pack_ref.shape[0] - PACKED
    halves = [pack_ref[:top, (2 * at + i) * states : (2 * at + i + 1) * states] for i in range(2)]
    return jnp.concatenate(halves, axis=0)


def driven(chan, pack_ref, bar_ref, groups, push_ref):
    flat = bar_ref.shape[2]
    twice = jnp.concatenate([chan, chan], axis=1)
    drives = []
    for at in range(2):
        both = jnp.concatenate(block_diagonal(matrix(pack_ref, at, flat // groups), groups), axis=0)
        drives.append(jnp.dot(twice, both, preferred_element_type=F32))
    decay, freq = (packed(pack_ref, 0), packed(pack_ref, 1))
    inverse = 1.0 / (decay * decay + freq * freq)
    bar_imag = bar_ref[1]
    less_real = bar_ref[0] - 1.0
    push_ref[0], push_ref[1] = complex_product(
        (less_real * decay + bar_imag * freq) * inverse,
        (bar_imag * decay - less_real * freq) * inverse,
        drives[0],
        drives[1],
    )


def scanned(bar_ref, push_ref, start):
    steps = bar_ref.shape[1] // CHUNKS

    def advance(j, carry):
        at = pl.ds(pl.multiple_of(j * CHUNKS, CHUNKS), CHUNKS)
        real, imag = complex_product(bar_ref[0, at, :], bar_ref[1, at, :], carry[0], carry[1])
        real = real + push_ref[0, at, :]
        imag = imag + push_ref[1, at, :]
        push_ref[0, at, :] = real
        push_ref[1, at, :] = imag
        return (real, imag)

    lax.fori_loop(0, steps, advance, start, unroll=4)


def chunk_maps(bar_ref, push_ref):
    steps, flat = (bar_ref.shape[1] // CHUNKS, bar_ref.shape[2])

    def advance(j, carry):
        at = pl.ds(pl.multiple_of(j * CHUNKS, CHUNKS), CHUNKS)
        bar = (bar_ref[0, at, :], bar_ref[1, at, :])
        product = complex_product(*bar, carry[0], carry[1])
        real, imag = complex_product(*bar, carry[2], carry[3])
        return (*product, real + push_ref[0, at, :], imag + push_ref[1, at, :])

    one, zero = (jnp.ones((CHUNKS, flat), F32), jnp.zeros((CHUNKS, flat), F32))
    return lax.fori_loop(0, steps, advance, (one, zero, zero, zero), unroll=4)


def local_kernel(
    groups, normed_ref, w_ref, bar_ref, pack_ref, rate_ref, chan_ref, end_ref, push_ref
):
    rows = normed_ref.shape[0]
    fs, sp = w_ref.shape[:2]
    w = jnp.concatenate([w_ref[f, z] for z in range(sp) for f in range(fs)], axis=0)
    state_in = jnp.dot(normed_ref[...], w, preferred_element_type=F32).astype(BF16)
    chan = jnp.dot(chunk_order(rows, False), state_in, preferred_element_type=F32).astype(BF16)
    chan_ref[...] = chan
    flat = bar_ref.shape[2]
    driven(chan, pack_ref, bar_ref, groups, push_ref)
    end_real, end_imag, last_real, last_imag = chunk_maps(bar_ref, push_ref)
    real, imag = (last_real[0:1], last_imag[0:1])
    for c in range(1, CHUNKS):
        moved_real, moved_imag = complex_product(end_real[c : c + 1], end_imag[c : c + 1], real, imag)
        real = moved_real + last_real[c : c + 1]
        imag = moved_imag + last_imag[c : c + 1]
    end = jnp.concatenate([real, imag], axis=0)
    whole = jnp.sum(rate_ref[...], axis=1, keepdims=True)
    whole = jnp.broadcast_to(whole, (2, end_ref.shape[2] - flat))
    for z in range(end_ref.shape[0]):
        end_ref[z, :, :flat] = end
        end_ref[z, :, flat:] = whole


def split_kernel(far_ref, many_ref, rest_ref):
    tall = many_ref.shape[2]
    rest_ref[...] = far_ref[:, tall:]
    for copy in range(many_ref.shape[0]):
        many_ref[copy] = far_ref[:, :tall]


def gelu(v):
    return 0.5 * v * (1.0 + jnp.tanh(0.7978845608 * (v + 0.044715 * v * v * v)))


def read_kernel(
    groups, ends_ref, bar_ref, chan_ref, pack_ref, mix_ref, closing_ref, push_ref
):
    flat = bar_ref.shape[2]
    states = flat // groups
    spans = ends_ref.shape[0]
    here = lax.axis_index("sp")
    decay, freq, scale, enter_real, enter_imag = (packed(pack_ref, at) for at in range(5))
    real, imag = (enter_real, enter_imag)
    elapsed = jnp.concatenate([ends_ref[z, 0:1, flat:] for z in range(spans)], axis=0)[:, 0:1] * scale
    grow = jnp.exp(elapsed * decay)
    sine, cosine = sine_cosine(elapsed * freq)
    map_real, map_imag = (grow * cosine, grow * sine)
    for z in range(spans):
        now = here == z
        enter_real = jnp.where(now, real, enter_real)
        enter_imag = jnp.where(now, imag, enter_imag)
        moved_real, moved_imag = complex_product(map_real[z : z + 1], map_imag[z : z + 1], real, imag)
        real = moved_real + ends_ref[z, 0:1, :flat]
        imag = moved_imag + ends_ref[z, 1:2, :flat]
    share = states // spans
    lane = iota((flat, share), 0) % states
    wanted = (lane == here * share + iota((flat, share), 1)).astype(BF16)
    own = iota((groups, flat), 1) // states == iota((groups, flat), 0)
    for at, row in enumerate((real, imag)):
        closing_ref[at] = picked(jnp.where(own, jnp.broadcast_to(row, (groups, flat)), 0.0), wanted)
    rows = bar_ref.shape[1]
    chan = chan_ref[...]
    driven(chan, pack_ref, bar_ref, groups, push_ref)
    end_real, end_imag, last_real, last_imag = chunk_maps(bar_ref, push_ref)
    in_real, in_imag = ([enter_real], [enter_imag])
    for c in range(CHUNKS - 1):
        moved_real, moved_imag = complex_product(
            end_real[c : c + 1], end_imag[c : c + 1], in_real[-1], in_imag[-1]
        )
        in_real.append(moved_real + last_real[c : c + 1])
        in_imag.append(moved_imag + last_imag[c : c + 1])
    scanned(bar_ref, push_ref, (jnp.concatenate(in_real, axis=0), jnp.concatenate(in_imag, axis=0)))
    response = None
    for at, sign in enumerate((1.0, -1.0)):
        weights = block_diagonal(matrix(pack_ref, 2 + at, states) * sign, groups)
        high, low = pieces(push_ref[at], 2)
        for left, right in ((high, 0), (low, 0), (high, 1)):
            term = lax.dot_general(left, weights[right], NT, preferred_element_type=F32)
            response = term if response is None else response + term
    skip = packed(pack_ref, 9, mix_ref.shape[1])
    mixed = gelu(response + skip * chan.astype(F32)).astype(BF16)
    mix_ref[...] = jnp.dot(chunk_order(rows, True), mixed, preferred_element_type=F32).astype(BF16)


def conv_kernel(
    state_ref, normed_ref, halo_ref, own_ref, up_ref, down_ref, left_ref, right_ref, pack_ref,
    mine_ref, theirs_ref, mix_ref, weights_ref, w_ref,
):
    width = mix_ref.shape[1]
    rows = normed_ref.shape[0]
    far = own_ref.shape[1]
    part = w_ref.shape[1]
    z, y = (lax.axis_index("sp"), lax.axis_index("fs"))

    def put(dz, dy, ref):
        for j in range(ref.shape[0]):
            at_q = (z + dz + CLASS[j][0]) & 3
            at_y = (y + dy + CLASS[j][1]) & 3
            for k in range(far):
                at = (k * 4 + at_y) * 4 + at_q
                for i in range(5):
                    piece = ref[j, k, i * part : (i + 1) * part]
                    if i < 3:
                        w_ref[at, :, i * width : (i + 1) * width] = piece
                    else:
                        weights_ref[at, :, (i - 3) * width : (i - 2) * width] = piece

    for (dz, dy), ref in zip(NEAR, (up_ref, down_ref, left_ref, right_ref)):
        put(dz, dy, ref)
    put(0, 0, own_ref)
    w = w_ref[...].reshape(normed_ref.shape[1], 3 * width)
    taps = [packed(pack_ref, 10 + at, width) for at in range(3)]
    gain = jnp.concatenate([packed(pack_ref, 5 + at) for at in range(4)], axis=1)
    reach = len(taps) - 1
    inputs = jnp.concatenate([normalized(halo_ref[...], gain), normed_ref[...]], axis=0)
    here = jnp.dot(inputs, w, preferred_element_type=F32).astype(BF16).astype(F32)
    extended = (here[:, :width] * here[:, width : 2 * width]).astype(BF16).astype(F32)
    filtered = taps[reach] * extended[HALO:]
    for tap in range(reach):
        at = HALO - reach + tap
        filtered = filtered + taps[tap] * extended[at : at + rows]
    mix_ref[...] = (here[HALO:, 2 * width :] * filtered).astype(BF16)
    output(state_ref, mix_ref, weights_ref, mine_ref, theirs_ref)


def output(state_ref, conv_ref, w_ref, mine_ref, theirs_ref):
    chips, rows = mine_ref.shape[:2]
    core = lax.axis_index("tp") & 1

    def rows_of(ref, parity):
        return [ref[pl.ds(pl.multiple_of((2 * x + parity) * rows, rows), rows), :] for x in range(chips)]

    mixes = jnp.concatenate(
        [
            jnp.concatenate([*rows_of(ref, core), *rows_of(ref, 1 - core)], axis=0)
            for ref in (state_ref, conv_ref)
        ],
        axis=1,
    )
    per = 512
    tall, part, wide = w_ref.shape
    for at in range(0, tall * part, per):
        w = w_ref[at // part : (at + per) // part].reshape(per, wide)
        product = lax.dot_general(mixes, w, NT, preferred_element_type=F32).astype(BF16)
        for x in range(chips):
            mine_ref[x, :, at : at + per] = product[x * rows : (x + 1) * rows]
            theirs_ref[x, :, at : at + per] = product[(chips + x) * rows : (chips + x + 1) * rows]


def add_kernel(left_ref, right_ref, sum_ref):
    sum_ref[...] = (left_ref[...].astype(F32) + right_ref[...].astype(F32)).astype(BF16)


def moved(x, dz, dy):
    sp, fs = (lax.axis_size("sp"), lax.axis_size("fs"))
    pairs = [
        (z * fs + y, ((z - dz) % sp) * fs + (y - dy) % fs) for z in range(sp) for y in range(fs)
    ]
    return lax.ppermute(x, ("sp", "fs"), pairs)


def all_shards(far):
    own = jnp.stack([far] + [moved(far, dz, dy) for dz, dy in CLASS[1:]])
    half = own[:2]
    return (own, *(moved(own if dz else half, dz, dy) for dz, dy in NEAR))


def call(kernel, out_shape, flops, *args, smem=0, anywhere=0, scratch=(), limit=20 << 20):
    vmem = pl.BlockSpec(memory_space=pltpu.VMEM)
    first = [pl.BlockSpec(memory_space=pltpu.SMEM)] * smem + [pl.BlockSpec(memory_space=pl.ANY)] * anywhere
    return pl.pallas_call(
        kernel,
        out_shape=out_shape,
        in_specs=first + [vmem] * (len(args) - len(first)),
        out_specs=jax.tree.map(lambda _: vmem, out_shape),
        scratch_shapes=list(scratch),
        cost_estimate=pl.CostEstimate(flops=flops, bytes_accessed=1 << 20, transcendentals=0),
        compiler_params=pltpu.CompilerParams(vmem_limit_bytes=limit),
    )(*args)


def shape(dims, dtype=F32):
    return jax.ShapeDtypeStruct(dims, dtype)


def body(
    tokens,
    norm_gain,
    w_state_in,
    w_value,
    w_outer,
    w_inner,
    w_state_out,
    w_conv_out,
    log_step,
    decay_real,
    frequency,
    step_rate,
    input_real,
    input_imag,
    read_real,
    read_imag,
    skip_gain,
    conv_taps,
    initial_state,
):
    rows, features = tokens.shape[1:]
    groups, states = decay_real.shape
    group = skip_gain.shape[1]
    flat = groups * states
    width = groups * group
    count = lax.axis_size("sp")

    part = w_state_in.shape[0] // 4
    weights = (w_state_in, w_value, w_inner, w_outer, w_state_out, w_conv_out)
    shards = call(
        pack_kernel,
        shape((count, w_state_in.shape[0] + 5 * part, width), BF16),
        1 << 20,
        *weights,
        anywhere=len(weights),
        scratch=(
            pltpu.VMEM((len(weights), *w_state_in.shape), BF16),
            pltpu.SemaphoreType.DMA((len(weights),)),
        ),
        limit=None,
    )
    far = lax.all_to_all(shards, "sp", 0, 0, tiled=True)
    fs = lax.axis_size("fs")
    many, rest = call(
        split_kernel,
        (shape((fs, count, 4 * part, width), BF16), shape((count, 5 * part, width), BF16)),
        1 << 20,
        far,
    )
    state_weights = lax.all_to_all(many, "fs", 0, 0, tiled=True)
    own, up, down, left, right = all_shards(rest)
    edge = lax.ppermute(tokens[0, rows - HALO :], "sp", [(i, i + 1) for i in range(count - 1)])
    gain = norm_gain[None]
    into = [jnp.swapaxes(x, 1, 2).reshape(width, states) for x in (input_real, input_imag)]
    normed, bar, pack = call(
        prep_kernel,
        (shape((rows, features), BF16), shape((2, rows, flat)), shape((width // 2 + PACKED, flat))),
        1 << 30,
        log_step,
        tokens[0],
        gain,
        step_rate,
        decay_real,
        frequency,
        initial_state[0].reshape(2 * groups, states),
        *into,
        read_real.reshape(width, states),
        read_imag.reshape(width, states),
        skip_gain,
        conv_taps,
        smem=1,
        scratch=(pltpu.VMEM((rows, 16), F32),),
    )
    chan, end = call(
        functools.partial(local_kernel, groups),
        (shape((rows, width), BF16), shape((count, 2, flat + 128))),
        1 << 29,
        normed,
        state_weights,
        bar,
        pack,
        step_rate,
        scratch=(pltpu.VMEM((2, rows, flat), F32),),
    )
    ends = lax.all_to_all(end, "sp", 0, 0, tiled=True)
    state_mix, closing = call(
        functools.partial(read_kernel, groups),
        (shape((rows, width), BF16), shape((2, groups, states // count))),
        1 << 29,
        ends,
        bar,
        chan,
        pack,
        scratch=(pltpu.VMEM((2, rows, flat), F32),),
    )
    tp = lax.axis_size("tp")
    chips = tp // 2
    piece = shape((chips, rows // tp, features), BF16)
    mine, theirs = call(
        conv_kernel,
        (piece, piece),
        1 << 29,
        state_mix,
        normed,
        edge,
        own,
        up,
        down,
        left,
        right,
        pack,
        scratch=(
            pltpu.VMEM((rows, width), BF16),
            pltpu.VMEM((features // part, part, 2 * width), BF16),
            pltpu.VMEM((features // part, part, 3 * width), BF16),
        ),
    )
    theirs = lax.ppermute(theirs, "tp", [(i, i ^ 1) for i in range(tp)])
    pair = call(add_kernel, piece, 1 << 20, mine, theirs)
    same_core = [[i for i in range(core, tp, 2)] for core in range(2)]
    parts = lax.all_to_all(pair, "tp", 0, 0, tiled=True, axis_index_groups=same_core)
    mixed = jnp.sum(parts.astype(F32), axis=0).astype(BF16)
    return (mixed[None], closing[None])


def solution(mesh):
    return jax.shard_map(
        body,
        mesh=mesh,
        in_specs=(
            P("fs", "sp", None),
            P(),
            P(("sp", "fs"), "tp"),
            P(("sp", "fs"), "tp"),
            P(("sp", "fs"), "tp"),
            P(("sp", "fs"), "tp"),
            P(("sp", "fs"), "tp"),
            P(("sp", "fs"), "tp"),
            P("tp"),
            P("tp", None),
            P("tp", None),
            P("fs", "sp"),
            P("tp", None, None),
            P("tp", None, None),
            P("tp", None, None),
            P("tp", None, None),
            P("tp", None),
            P(None, "tp"),
            P("fs", None, "tp", None),
        ),
        out_specs=(P("fs", ("sp", "tp"), None), P("fs", None, "tp", "sp")),
        check_vma=False,
    )
```

```python
import functools

import jax
import jax.numpy as jnp
from jax import lax
from jax.experimental import pallas as pl
from jax.experimental.pallas import tpu as pltpu
from jax.sharding import PartitionSpec as P


F32 = jnp.float32
BF16 = jnp.bfloat16
CHUNKS = 8
HALO = 16
PACKED = 16
PRODUCTS = 2 * CHUNKS
MATRIX = 64
CLASS = ((0, 0), (2, 1), (-2, -1), (0, 2))
NEAR = ((1, 0), (-1, 0), (0, 1), (0, -1))
NT = (((1,), (1,)), ((), ()))


def complex_product(left_real, left_imag, right_real, right_imag):
    return (
        left_real * right_real - left_imag * right_imag,
        left_real * right_imag + left_imag * right_real,
    )


def sine_cosine(angle):
    turns = jnp.floor(angle * 0.6366197723675814 + 0.5)
    r = angle - turns * 1.5703125
    r = r - turns * 4.837512969970703e-4
    r = r - turns * 7.549789948768648e-8
    r2 = r * r
    sine = r + r * r2 * (-1.6666654611e-1 + r2 * (8.3321608736e-3 + r2 * -1.9515295891e-4))
    cosine = (
        1.0
        - 0.5 * r2
        + r2 * r2 * (4.166664568298827e-2 + r2 * (-1.388731625493765e-3 + r2 * 2.443315711809948e-5))
    )
    quadrant = turns.astype(jnp.int32)
    odd = (quadrant & 1) == 1
    flip_sine = (quadrant & 2) == 2
    flip_cosine = ((quadrant + 1) & 2) == 2
    base_sine = jnp.where(odd, cosine, sine)
    base_cosine = jnp.where(odd, sine, cosine)
    return (
        jnp.where(flip_sine, -base_sine, base_sine),
        jnp.where(flip_cosine, -base_cosine, base_cosine),
    )


def iota(dims, axis):
    return lax.broadcasted_iota(jnp.int32, dims, axis)


def pieces(x, count):
    found = []
    for _ in range(count):
        part = x.astype(BF16)
        found.append(part)
        x = x - part.astype(F32)
    return found


def picked(x, selector, count=3):
    total = None
    for part in pieces(x, count):
        term = jnp.dot(part, selector, preferred_element_type=F32)
        total = term if total is None else total + term
    return total


def repeat_selector(narrow, wide):
    return (iota((narrow, wide), 1) % narrow == iota((narrow, wide), 0)).astype(BF16)


def flattened(x, groups):
    rows, narrow = x.shape
    wide = groups * narrow
    tiled = picked(x, repeat_selector(narrow, wide))
    own = iota((rows, wide), 1) // narrow == iota((rows, wide), 0) % groups
    tiled = jnp.where(own, tiled, 0.0)
    return [jnp.sum(tiled[at : at + groups], axis=0, keepdims=True) for at in range(0, rows, groups)]


def block_diagonal(x, groups):
    rows, narrow = x.shape
    wide = groups * narrow
    selector = repeat_selector(narrow, wide)
    own = iota((rows, wide), 1) // narrow == iota((rows, wide), 0) // (rows // groups)
    return [
        jnp.where(own, jnp.dot(part, selector, preferred_element_type=F32), 0.0).astype(BF16)
        for part in pieces(x, 2)
    ]


def spread_steps(log_ref, groups, states):
    lane = iota((1, groups * states), 1) // states
    out = jnp.zeros((1, groups * states), F32)
    for g in range(groups):
        out = jnp.where(lane == g, log_ref[g], out)
    return jnp.exp(out)


def chunk_order(rows, flip):
    r, c = (iota((rows, rows), 1 if flip else 0), iota((rows, rows), 0 if flip else 1))
    steps = rows // CHUNKS
    return (c == (r % CHUNKS) * steps + r // CHUNKS).astype(BF16)


def normalized(x, gain):
    x = x.astype(F32)
    mean_square = jnp.mean(x * x, axis=-1, keepdims=True)
    return (x * lax.rsqrt(mean_square + 1e-06) * gain).astype(BF16)


def pack_kernel(*refs):
    count = 6
    sources, out_ref, landed, sems = (refs[:count], refs[count], refs[count + 1], refs[count + 2])
    copies = [
        pltpu.make_async_copy(source, landed.at[i], sems.at[i]) for i, source in enumerate(sources)
    ]
    for copy in copies:
        copy.start()
    for copy in copies:
        copy.wait()
    tall = landed.shape[1]
    part = tall // 4
    for z in range(out_ref.shape[0]):
        out_ref[z, :tall] = landed[0]
        q = z % 4
        for i in range(1, count):
            at = tall + (i - 1) * part
            out_ref[z, at : at + part] = landed[i, q * part : (q + 1) * part]


def prep_kernel(
    log_ref, tokens_ref, gain_ref, rate_ref, decay_ref, freq_ref, initial_ref, in_real_ref, in_imag_ref,
    out_real_ref, out_imag_ref, skip_ref, taps_ref, normed_ref, bar_ref, pack_ref, column_ref,
):
    groups, states = decay_ref.shape
    flat = groups * states
    rows = tokens_ref.shape[0]
    part = 64

    def norm(i, _):
        at = pl.ds(pl.multiple_of(i * part, part), part)
        normed_ref[at, :] = normalized(tokens_ref[at, :], gain_ref[...])
        return 0

    lax.fori_loop(0, rows // part, norm, 0)
    order = chunk_order(rows, False)
    column = None
    for piece in pieces(jnp.broadcast_to(rate_ref[...], (16, rows)), 3):
        term = lax.dot_general(order, piece, NT, preferred_element_type=F32)
        column = term if column is None else column + term
    column_ref[...] = column
    (decay,) = flattened(decay_ref[...], groups)
    (freq,) = flattened(freq_ref[...], groups)
    scale = spread_steps(log_ref, groups, states)
    top = MATRIX
    for at, ref in enumerate((in_real_ref, in_imag_ref, out_real_ref, out_imag_ref)):
        for i in range(2):
            lanes = slice((2 * at + i) * states, (2 * at + i + 1) * states)
            pack_ref[:top, lanes] = ref[i * top : (i + 1) * top]
    (skip,) = flattened(skip_ref[...], groups)
    gain_rows = gain_ref.shape[1] // flat
    for at, row in enumerate(
        (
            decay,
            freq,
            scale,
            *flattened(initial_ref[...], groups),
            *(gain_ref[:, i * flat : (i + 1) * flat] for i in range(gain_rows)),
            skip,
            *(taps_ref[i : i + 1] for i in range(taps_ref.shape[0])),
        )
    ):
        pack_ref[top + at : top + at + 1, : row.shape[1]] = row
    steps = rows // CHUNKS

    def advance(j, carry):
        at = pl.ds(pl.multiple_of(j * CHUNKS, CHUNKS), CHUNKS)
        step = column_ref[at, 0:1] * scale
        grow = jnp.exp(step * decay)
        sine, cosine = sine_cosine(step * freq)
        bar_real, bar_imag = (grow * cosine, grow * sine)
        bar_ref[0, at, :] = bar_real
        bar_ref[1, at, :] = bar_imag
        return complex_product(carry[0], carry[1], bar_real, bar_imag)

    one = jnp.ones((CHUNKS, flat), F32)
    product_real, product_imag = lax.fori_loop(0, steps, advance, (one, jnp.zeros_like(one)))
    at = MATRIX + PACKED
    pack_ref[at : at + CHUNKS] = product_real
    pack_ref[at + CHUNKS : at + 2 * CHUNKS] = product_imag


def packed(pack_ref, at, wide=None):
    top = MATRIX
    return pack_ref[top + at : top + at + 1, : pack_ref.shape[1] if wide is None else wide]


def products(pack_ref):
    at = MATRIX + PACKED
    return (pack_ref[at : at + CHUNKS], pack_ref[at + CHUNKS : at + 2 * CHUNKS])


def chan_blocks(pack_ref, rows):
    at, wide = (MATRIX + PACKED + PRODUCTS, pack_ref.shape[1])
    tall = pack_ref.shape[0] - at
    width = wide * tall // rows
    return [
        (slice(i * tall, (i + 1) * tall), slice(at, at + tall), slice(i * width, (i + 1) * width))
        for i in range(rows // tall)
    ]


def matrix(pack_ref, at, states):
    top = MATRIX
    halves = [pack_ref[:top, (2 * at + i) * states : (2 * at + i + 1) * states] for i in range(2)]
    return jnp.concatenate(halves, axis=0)


def driven(chan, pack_ref, bar_ref, groups, push_ref):
    flat = bar_ref.shape[2]
    twice = jnp.concatenate([chan, chan], axis=1)
    drives = []
    for at in range(2):
        both = jnp.concatenate(block_diagonal(matrix(pack_ref, at, flat // groups), groups), axis=0)
        drives.append(jnp.dot(twice, both, preferred_element_type=F32))
    decay, freq = (packed(pack_ref, 0), packed(pack_ref, 1))
    inverse = 1.0 / (decay * decay + freq * freq)
    bar_imag = bar_ref[1]
    less_real = bar_ref[0] - 1.0
    push_ref[0], push_ref[1] = complex_product(
        (less_real * decay + bar_imag * freq) * inverse,
        (bar_imag * decay - less_real * freq) * inverse,
        drives[0],
        drives[1],
    )


def scanned(bar_ref, push_ref, start):
    steps = bar_ref.shape[1] // CHUNKS

    def advance(j, carry):
        at = pl.ds(pl.multiple_of(j * CHUNKS, CHUNKS), CHUNKS)
        real, imag = complex_product(bar_ref[0, at, :], bar_ref[1, at, :], carry[0], carry[1])
        real = real + push_ref[0, at, :]
        imag = imag + push_ref[1, at, :]
        push_ref[0, at, :] = real
        push_ref[1, at, :] = imag
        return (real, imag)

    lax.fori_loop(0, steps, advance, start, unroll=4)


def chunk_ends(bar_ref, push_ref):
    steps, flat = (bar_ref.shape[1] // CHUNKS, bar_ref.shape[2])

    def advance(j, carry):
        at = pl.ds(pl.multiple_of(j * CHUNKS, CHUNKS), CHUNKS)
        real, imag = complex_product(bar_ref[0, at, :], bar_ref[1, at, :], carry[0], carry[1])
        return (real + push_ref[0, at, :], imag + push_ref[1, at, :])

    zero = jnp.zeros((CHUNKS, flat), F32)
    return lax.fori_loop(0, steps, advance, (zero, zero), unroll=4)


def local_kernel(
    groups, normed_ref, w_ref, bar_ref, pack_ref, rate_ref, kept_ref, end_ref, push_ref
):
    rows = normed_ref.shape[0]
    fs, sp = w_ref.shape[:2]
    w = jnp.concatenate([w_ref[f, z] for z in range(sp) for f in range(fs)], axis=0)
    state_in = jnp.dot(normed_ref[...], w, preferred_element_type=F32).astype(BF16)
    chan = jnp.dot(chunk_order(rows, False), state_in, preferred_element_type=F32).astype(BF16)
    top = MATRIX + PACKED + PRODUCTS
    kept_ref[:top] = pack_ref[:top]
    for rows_at, to, lanes in chan_blocks(kept_ref, rows):
        kept_ref[to, lanes] = chan[rows_at].astype(F32)
    flat = bar_ref.shape[2]
    driven(chan, pack_ref, bar_ref, groups, push_ref)
    end_real, end_imag = products(pack_ref)
    last_real, last_imag = chunk_ends(bar_ref, push_ref)
    real, imag = (last_real[0:1], last_imag[0:1])
    for c in range(1, CHUNKS):
        moved_real, moved_imag = complex_product(end_real[c : c + 1], end_imag[c : c + 1], real, imag)
        real = moved_real + last_real[c : c + 1]
        imag = moved_imag + last_imag[c : c + 1]
    end = jnp.concatenate([real, imag], axis=0)
    whole = jnp.sum(rate_ref[...], axis=1, keepdims=True)
    whole = jnp.broadcast_to(whole, (2, end_ref.shape[2] - flat))
    for z in range(end_ref.shape[0]):
        end_ref[z, :, :flat] = end
        end_ref[z, :, flat:] = whole


def split_kernel(far_ref, many_ref, rest_ref):
    tall = many_ref.shape[2]
    rest_ref[...] = far_ref[:, tall:]
    for copy in range(many_ref.shape[0]):
        many_ref[copy] = far_ref[:, :tall]


def gelu(v):
    return 0.5 * v * (1.0 + jnp.tanh(0.7978845608 * (v + 0.044715 * v * v * v)))


def read_kernel(
    groups, ends_ref, bar_ref, pack_ref, mix_ref, closing_ref, push_ref
):
    flat = bar_ref.shape[2]
    states = flat // groups
    spans = ends_ref.shape[0]
    here = lax.axis_index("sp")
    decay, freq, scale, enter_real, enter_imag = (packed(pack_ref, at) for at in range(5))
    real, imag = (enter_real, enter_imag)
    elapsed = jnp.concatenate([ends_ref[z, 0:1, flat:] for z in range(spans)], axis=0)[:, 0:1] * scale
    grow = jnp.exp(elapsed * decay)
    sine, cosine = sine_cosine(elapsed * freq)
    map_real, map_imag = (grow * cosine, grow * sine)
    for z in range(spans):
        now = here == z
        enter_real = jnp.where(now, real, enter_real)
        enter_imag = jnp.where(now, imag, enter_imag)
        moved_real, moved_imag = complex_product(map_real[z : z + 1], map_imag[z : z + 1], real, imag)
        real = moved_real + ends_ref[z, 0:1, :flat]
        imag = moved_imag + ends_ref[z, 1:2, :flat]
    share = states // spans
    lane = iota((flat, share), 0) % states
    wanted = (lane == here * share + iota((flat, share), 1)).astype(BF16)
    own = iota((groups, flat), 1) // states == iota((groups, flat), 0)
    for at, row in enumerate((real, imag)):
        closing_ref[at] = picked(jnp.where(own, jnp.broadcast_to(row, (groups, flat)), 0.0), wanted)
    rows = bar_ref.shape[1]
    wide = [pack_ref[at, lanes] for _, at, lanes in chan_blocks(pack_ref, rows)]
    chan = jnp.concatenate(wide, axis=0).astype(BF16)
    driven(chan, pack_ref, bar_ref, groups, push_ref)
    end_real, end_imag = products(pack_ref)
    last_real, last_imag = chunk_ends(bar_ref, push_ref)
    in_real, in_imag = ([enter_real], [enter_imag])
    for c in range(CHUNKS - 1):
        moved_real, moved_imag = complex_product(
            end_real[c : c + 1], end_imag[c : c + 1], in_real[-1], in_imag[-1]
        )
        in_real.append(moved_real + last_real[c : c + 1])
        in_imag.append(moved_imag + last_imag[c : c + 1])
    scanned(bar_ref, push_ref, (jnp.concatenate(in_real, axis=0), jnp.concatenate(in_imag, axis=0)))
    response = None
    for at, sign in enumerate((1.0, -1.0)):
        weights = block_diagonal(matrix(pack_ref, 2 + at, states) * sign, groups)
        high, low = pieces(push_ref[at], 2)
        for left, right in ((high, 0), (low, 0), (high, 1)):
            term = lax.dot_general(left, weights[right], NT, preferred_element_type=F32)
            response = term if response is None else response + term
    skip = packed(pack_ref, 9, mix_ref.shape[1])
    mixed = gelu(response + skip * chan.astype(F32)).astype(BF16)
    mix_ref[...] = jnp.dot(chunk_order(rows, True), mixed, preferred_element_type=F32).astype(BF16)


def conv_kernel(
    state_ref, normed_ref, halo_ref, own_ref, up_ref, down_ref, left_ref, right_ref, pack_ref,
    mine_ref, theirs_ref, mix_ref, weights_ref, w_ref,
):
    width = mix_ref.shape[1]
    rows = normed_ref.shape[0]
    far = own_ref.shape[1]
    part = w_ref.shape[1]
    z, y = (lax.axis_index("sp"), lax.axis_index("fs"))

    def put(dz, dy, ref):
        for j in range(ref.shape[0]):
            at_q = (z + dz + CLASS[j][0]) & 3
            at_y = (y + dy + CLASS[j][1]) & 3
            for k in range(far):
                at = (k * 4 + at_y) * 4 + at_q
                for i in range(5):
                    piece = ref[j, k, i * part : (i + 1) * part]
                    if i < 3:
                        w_ref[at, :, i * width : (i + 1) * width] = piece
                    else:
                        weights_ref[at, :, (i - 3) * width : (i - 2) * width] = piece

    for (dz, dy), ref in zip(NEAR, (up_ref, down_ref, left_ref, right_ref)):
        put(dz, dy, ref)
    put(0, 0, own_ref)
    w = w_ref[...].reshape(normed_ref.shape[1], 3 * width)
    taps = [packed(pack_ref, 10 + at, width) for at in range(3)]
    gain = jnp.concatenate([packed(pack_ref, 5 + at) for at in range(4)], axis=1)
    reach = len(taps) - 1
    inputs = jnp.concatenate([normalized(halo_ref[...], gain), normed_ref[...]], axis=0)
    here = jnp.dot(inputs, w, preferred_element_type=F32).astype(BF16).astype(F32)
    extended = (here[:, :width] * here[:, width : 2 * width]).astype(BF16).astype(F32)
    filtered = taps[reach] * extended[HALO:]
    for tap in range(reach):
        at = HALO - reach + tap
        filtered = filtered + taps[tap] * extended[at : at + rows]
    mix_ref[...] = (here[HALO:, 2 * width :] * filtered).astype(BF16)
    output(state_ref, mix_ref, weights_ref, mine_ref, theirs_ref)


def output(state_ref, conv_ref, w_ref, mine_ref, theirs_ref):
    chips, rows = mine_ref.shape[:2]
    core = lax.axis_index("tp") & 1

    def rows_of(ref, parity):
        return [ref[pl.ds(pl.multiple_of((2 * x + parity) * rows, rows), rows), :] for x in range(chips)]

    mixes = jnp.concatenate(
        [
            jnp.concatenate([*rows_of(ref, core), *rows_of(ref, 1 - core)], axis=0)
            for ref in (state_ref, conv_ref)
        ],
        axis=1,
    )
    per = 512
    tall, part, wide = w_ref.shape
    for at in range(0, tall * part, per):
        w = w_ref[at // part : (at + per) // part].reshape(per, wide)
        product = lax.dot_general(mixes, w, NT, preferred_element_type=F32).astype(BF16)
        for x in range(chips):
            mine_ref[x, :, at : at + per] = product[x * rows : (x + 1) * rows]
            theirs_ref[x, :, at : at + per] = product[(chips + x) * rows : (chips + x + 1) * rows]


def add_kernel(left_ref, right_ref, sum_ref):
    sum_ref[...] = (left_ref[...].astype(F32) + right_ref[...].astype(F32)).astype(BF16)


def moved(x, dz, dy):
    sp, fs = (lax.axis_size("sp"), lax.axis_size("fs"))
    pairs = [
        (z * fs + y, ((z - dz) % sp) * fs + (y - dy) % fs) for z in range(sp) for y in range(fs)
    ]
    return lax.ppermute(x, ("sp", "fs"), pairs)


def all_shards(far):
    own = jnp.stack([far] + [moved(far, dz, dy) for dz, dy in CLASS[1:]])
    half = own[:2]
    return (own, *(moved(own if dz else half, dz, dy) for dz, dy in NEAR))


def call(kernel, out_shape, flops, *args, smem=0, anywhere=0, aliases=None, scratch=(), limit=20 << 20):
    vmem = pl.BlockSpec(memory_space=pltpu.VMEM)
    first = [pl.BlockSpec(memory_space=pltpu.SMEM)] * smem + [pl.BlockSpec(memory_space=pl.ANY)] * anywhere
    return pl.pallas_call(
        kernel,
        out_shape=out_shape,
        in_specs=first + [vmem] * (len(args) - len(first)),
        out_specs=jax.tree.map(lambda _: vmem, out_shape),
        scratch_shapes=list(scratch),
        input_output_aliases=aliases or {},
        cost_estimate=pl.CostEstimate(flops=flops, bytes_accessed=1 << 20, transcendentals=0),
        compiler_params=pltpu.CompilerParams(vmem_limit_bytes=limit),
    )(*args)


def shape(dims, dtype=F32):
    return jax.ShapeDtypeStruct(dims, dtype)


def body(
    tokens,
    norm_gain,
    w_state_in,
    w_value,
    w_outer,
    w_inner,
    w_state_out,
    w_conv_out,
    log_step,
    decay_real,
    frequency,
    step_rate,
    input_real,
    input_imag,
    read_real,
    read_imag,
    skip_gain,
    conv_taps,
    initial_state,
):
    rows, features = tokens.shape[1:]
    groups, states = decay_real.shape
    group = skip_gain.shape[1]
    flat = groups * states
    width = groups * group
    count = lax.axis_size("sp")

    part = w_state_in.shape[0] // 4
    weights = (w_state_in, w_value, w_inner, w_outer, w_state_out, w_conv_out)
    shards = call(
        pack_kernel,
        shape((count, w_state_in.shape[0] + 5 * part, width), BF16),
        1 << 20,
        *weights,
        anywhere=len(weights),
        scratch=(
            pltpu.VMEM((len(weights), *w_state_in.shape), BF16),
            pltpu.SemaphoreType.DMA((len(weights),)),
        ),
        limit=None,
    )
    far = lax.all_to_all(shards, "sp", 0, 0, tiled=True)
    fs = lax.axis_size("fs")
    many, rest = call(
        split_kernel,
        (shape((fs, count, 4 * part, width), BF16), shape((count, 5 * part, width), BF16)),
        1 << 20,
        far,
    )
    state_weights = lax.all_to_all(many, "fs", 0, 0, tiled=True)
    own, up, down, left, right = all_shards(rest)
    edge = lax.ppermute(tokens[0, rows - HALO :], "sp", [(i, i + 1) for i in range(count - 1)])
    gain = norm_gain[None]
    into = [jnp.swapaxes(x, 1, 2).reshape(width, states) for x in (input_real, input_imag)]
    normed, bar, pack = call(
        prep_kernel,
        (shape((rows, features), BF16), shape((2, rows, flat)), shape((MATRIX + PACKED + PRODUCTS + rows * width // flat, flat))),
        1 << 30,
        log_step,
        tokens[0],
        gain,
        step_rate,
        decay_real,
        frequency,
        initial_state[0].reshape(2 * groups, states),
        *into,
        read_real.reshape(width, states),
        read_imag.reshape(width, states),
        skip_gain,
        conv_taps,
        smem=1,
        scratch=(pltpu.VMEM((rows, 16), F32),),
    )
    pack, end = call(
        functools.partial(local_kernel, groups),
        (shape(pack.shape), shape((count, 2, flat + 128))),
        1 << 29,
        normed,
        state_weights,
        bar,
        pack,
        step_rate,
        aliases={3: 0},
        scratch=(pltpu.VMEM((2, rows, flat), F32),),
    )
    ends = lax.all_to_all(end, "sp", 0, 0, tiled=True)
    state_mix, closing = call(
        functools.partial(read_kernel, groups),
        (shape((rows, width), BF16), shape((2, groups, states // count))),
        1 << 29,
        ends,
        bar,
        pack,
        scratch=(pltpu.VMEM((2, rows, flat), F32),),
    )
    tp = lax.axis_size("tp")
    chips = tp // 2
    piece = shape((chips, rows // tp, features), BF16)
    mine, theirs = call(
        conv_kernel,
        (piece, piece),
        1 << 29,
        state_mix,
        normed,
        edge,
        own,
        up,
        down,
        left,
        right,
        pack,
        scratch=(
            pltpu.VMEM((rows, width), BF16),
            pltpu.VMEM((features // part, part, 2 * width), BF16),
            pltpu.VMEM((features // part, part, 3 * width), BF16),
        ),
    )
    theirs = lax.ppermute(theirs, "tp", [(i, i ^ 1) for i in range(tp)])
    pair = call(add_kernel, piece, 1 << 20, mine, theirs)
    same_core = [[i for i in range(core, tp, 2)] for core in range(2)]
    parts = lax.all_to_all(pair, "tp", 0, 0, tiled=True, axis_index_groups=same_core)
    mixed = jnp.sum(parts.astype(F32), axis=0).astype(BF16)
    return (mixed[None], closing[None])


def solution(mesh):
    return jax.shard_map(
        body,
        mesh=mesh,
        in_specs=(
            P("fs", "sp", None),
            P(),
            P(("sp", "fs"), "tp"),
            P(("sp", "fs"), "tp"),
            P(("sp", "fs"), "tp"),
            P(("sp", "fs"), "tp"),
            P(("sp", "fs"), "tp"),
            P(("sp", "fs"), "tp"),
            P("tp"),
            P("tp", None),
            P("tp", None),
            P("fs", "sp"),
            P("tp", None, None),
            P("tp", None, None),
            P("tp", None, None),
            P("tp", None, None),
            P("tp", None),
            P(None, "tp"),
            P("fs", None, "tp", None),
        ),
        out_specs=(P("fs", ("sp", "tp"), None), P("fs", None, "tp", "sp")),
        check_vma=False,
    )
```

```python
import functools

import jax
import jax.numpy as jnp
from jax import lax
from jax.experimental import pallas as pl
from jax.experimental.pallas import tpu as pltpu
from jax.sharding import PartitionSpec as P


F32 = jnp.float32
BF16 = jnp.bfloat16
CHUNKS = 8
HALO = 16
PACKED = 16
PRODUCTS = 2 * CHUNKS
MATRIX = 64
CLASSES = (((0, 0), (2, 1), (-2, -1), (0, 2)), ((0, 0), (1, 2), (2, 0), (-1, 2)))
NEARS = (((1, 0), (-1, 0), (0, 1), (0, -1)), ((0, 1), (0, -1), (1, 0), (-1, 0)))
NT = (((1,), (1,)), ((), ()))


def complex_product(left_real, left_imag, right_real, right_imag):
    return (
        left_real * right_real - left_imag * right_imag,
        left_real * right_imag + left_imag * right_real,
    )


def sine_cosine(angle):
    turns = jnp.floor(angle * 0.6366197723675814 + 0.5)
    r = angle - turns * 1.5703125
    r = r - turns * 4.837512969970703e-4
    r = r - turns * 7.549789948768648e-8
    r2 = r * r
    sine = r + r * r2 * (-1.6666654611e-1 + r2 * (8.3321608736e-3 + r2 * -1.9515295891e-4))
    cosine = (
        1.0
        - 0.5 * r2
        + r2 * r2 * (4.166664568298827e-2 + r2 * (-1.388731625493765e-3 + r2 * 2.443315711809948e-5))
    )
    quadrant = turns.astype(jnp.int32)
    odd = (quadrant & 1) == 1
    flip_sine = (quadrant & 2) == 2
    flip_cosine = ((quadrant + 1) & 2) == 2
    base_sine = jnp.where(odd, cosine, sine)
    base_cosine = jnp.where(odd, sine, cosine)
    return (
        jnp.where(flip_sine, -base_sine, base_sine),
        jnp.where(flip_cosine, -base_cosine, base_cosine),
    )


def iota(dims, axis):
    return lax.broadcasted_iota(jnp.int32, dims, axis)


def pieces(x, count):
    found = []
    for _ in range(count):
        part = x.astype(BF16)
        found.append(part)
        x = x - part.astype(F32)
    return found


def picked(x, selector, count=3):
    total = None
    for part in pieces(x, count):
        term = jnp.dot(part, selector, preferred_element_type=F32)
        total = term if total is None else total + term
    return total


def repeat_selector(narrow, wide):
    return (iota((narrow, wide), 1) % narrow == iota((narrow, wide), 0)).astype(BF16)


def flattened(x, groups):
    rows, narrow = x.shape
    wide = groups * narrow
    tiled = picked(x, repeat_selector(narrow, wide))
    own = iota((rows, wide), 1) // narrow == iota((rows, wide), 0) % groups
    tiled = jnp.where(own, tiled, 0.0)
    return [jnp.sum(tiled[at : at + groups], axis=0, keepdims=True) for at in range(0, rows, groups)]


def block_diagonal(x, groups):
    rows, narrow = x.shape
    wide = groups * narrow
    selector = repeat_selector(narrow, wide)
    own = iota((rows, wide), 1) // narrow == iota((rows, wide), 0) // (rows // groups)
    return [
        jnp.where(own, jnp.dot(part, selector, preferred_element_type=F32), 0.0).astype(BF16)
        for part in pieces(x, 2)
    ]


def spread_steps(log_ref, groups, states):
    lane = iota((1, groups * states), 1) // states
    out = jnp.zeros((1, groups * states), F32)
    for g in range(groups):
        out = jnp.where(lane == g, log_ref[g], out)
    return jnp.exp(out)


def chunk_order(rows, flip):
    r, c = (iota((rows, rows), 1 if flip else 0), iota((rows, rows), 0 if flip else 1))
    steps = rows // CHUNKS
    return (c == (r % CHUNKS) * steps + r // CHUNKS).astype(BF16)


def normalized(x, gain):
    x = x.astype(F32)
    mean_square = jnp.mean(x * x, axis=-1, keepdims=True)
    return (x * lax.rsqrt(mean_square + 1e-06) * gain).astype(BF16)


def pack_kernel(*refs):
    count = 6
    sources, out_ref, landed, sems = (refs[:count], refs[count], refs[count + 1], refs[count + 2])
    copies = [
        pltpu.make_async_copy(source, landed.at[i], sems.at[i]) for i, source in enumerate(sources)
    ]
    for copy in copies:
        copy.start()
    for copy in copies:
        copy.wait()
    tall = landed.shape[1]
    part = tall // 4
    for z in range(out_ref.shape[0]):
        out_ref[z, :tall] = landed[0]
        q = z % 4
        for i in range(1, count):
            at = tall + (i - 1) * part
            out_ref[z, at : at + part] = landed[i, q * part : (q + 1) * part]


def prep_kernel(
    log_ref, tokens_ref, gain_ref, rate_ref, decay_ref, freq_ref, initial_ref, in_real_ref, in_imag_ref,
    out_real_ref, out_imag_ref, skip_ref, taps_ref, normed_ref, bar_ref, pack_ref, column_ref,
):
    groups, states = decay_ref.shape
    flat = groups * states
    rows = tokens_ref.shape[0]
    part = 64

    def norm(i, _):
        at = pl.ds(pl.multiple_of(i * part, part), part)
        normed_ref[at, :] = normalized(tokens_ref[at, :], gain_ref[...])
        return 0

    lax.fori_loop(0, rows // part, norm, 0)
    order = chunk_order(rows, False)
    column = None
    for piece in pieces(jnp.broadcast_to(rate_ref[...], (16, rows)), 3):
        term = lax.dot_general(order, piece, NT, preferred_element_type=F32)
        column = term if column is None else column + term
    column_ref[...] = column
    (decay,) = flattened(decay_ref[...], groups)
    (freq,) = flattened(freq_ref[...], groups)
    scale = spread_steps(log_ref, groups, states)
    top = MATRIX
    for at, ref in enumerate((in_real_ref, in_imag_ref, out_real_ref, out_imag_ref)):
        for i in range(2):
            lanes = slice((2 * at + i) * states, (2 * at + i + 1) * states)
            pack_ref[:top, lanes] = ref[i * top : (i + 1) * top]
    (skip,) = flattened(skip_ref[...], groups)
    gain_rows = gain_ref.shape[1] // flat
    for at, row in enumerate(
        (
            decay,
            freq,
            scale,
            *flattened(initial_ref[...], groups),
            *(gain_ref[:, i * flat : (i + 1) * flat] for i in range(gain_rows)),
            skip,
            *(taps_ref[i : i + 1] for i in range(taps_ref.shape[0])),
        )
    ):
        pack_ref[top + at : top + at + 1, : row.shape[1]] = row
    steps = rows // CHUNKS

    def advance(j, carry):
        at = pl.ds(pl.multiple_of(j * CHUNKS, CHUNKS), CHUNKS)
        step = column_ref[at, 0:1] * scale
        grow = jnp.exp(step * decay)
        sine, cosine = sine_cosine(step * freq)
        bar_real, bar_imag = (grow * cosine, grow * sine)
        bar_ref[0, at, :] = bar_real
        bar_ref[1, at, :] = bar_imag
        return complex_product(carry[0], carry[1], bar_real, bar_imag)

    one = jnp.ones((CHUNKS, flat), F32)
    product_real, product_imag = lax.fori_loop(0, steps, advance, (one, jnp.zeros_like(one)))
    at = MATRIX + PACKED
    pack_ref[at : at + CHUNKS] = product_real
    pack_ref[at + CHUNKS : at + 2 * CHUNKS] = product_imag


def packed(pack_ref, at, wide=None):
    top = MATRIX
    return pack_ref[top + at : top + at + 1, : pack_ref.shape[1] if wide is None else wide]


def products(pack_ref):
    at = MATRIX + PACKED
    return (pack_ref[at : at + CHUNKS], pack_ref[at + CHUNKS : at + 2 * CHUNKS])


def chan_blocks(pack_ref, rows):
    at, wide = (MATRIX + PACKED + PRODUCTS, pack_ref.shape[1])
    tall = pack_ref.shape[0] - at
    width = wide * tall // rows
    return [
        (slice(i * tall, (i + 1) * tall), slice(at, at + tall), slice(i * width, (i + 1) * width))
        for i in range(rows // tall)
    ]


def matrix(pack_ref, at, states):
    top = MATRIX
    halves = [pack_ref[:top, (2 * at + i) * states : (2 * at + i + 1) * states] for i in range(2)]
    return jnp.concatenate(halves, axis=0)


def driven(chan, pack_ref, bar_ref, groups, push_ref):
    flat = bar_ref.shape[2]
    twice = jnp.concatenate([chan, chan], axis=1)
    drives = []
    for at in range(2):
        both = jnp.concatenate(block_diagonal(matrix(pack_ref, at, flat // groups), groups), axis=0)
        drives.append(jnp.dot(twice, both, preferred_element_type=F32))
    decay, freq = (packed(pack_ref, 0), packed(pack_ref, 1))
    inverse = 1.0 / (decay * decay + freq * freq)
    bar_imag = bar_ref[1]
    less_real = bar_ref[0] - 1.0
    push_ref[0], push_ref[1] = complex_product(
        (less_real * decay + bar_imag * freq) * inverse,
        (bar_imag * decay - less_real * freq) * inverse,
        drives[0],
        drives[1],
    )


def scanned(bar_ref, push_ref, start):
    steps = bar_ref.shape[1] // CHUNKS

    def advance(j, carry):
        at = pl.ds(pl.multiple_of(j * CHUNKS, CHUNKS), CHUNKS)
        real, imag = complex_product(bar_ref[0, at, :], bar_ref[1, at, :], carry[0], carry[1])
        real = real + push_ref[0, at, :]
        imag = imag + push_ref[1, at, :]
        push_ref[0, at, :] = real
        push_ref[1, at, :] = imag
        return (real, imag)

    lax.fori_loop(0, steps, advance, start, unroll=4)


def chunk_ends(bar_ref, push_ref):
    steps, flat = (bar_ref.shape[1] // CHUNKS, bar_ref.shape[2])

    def advance(j, carry):
        at = pl.ds(pl.multiple_of(j * CHUNKS, CHUNKS), CHUNKS)
        real, imag = complex_product(bar_ref[0, at, :], bar_ref[1, at, :], carry[0], carry[1])
        return (real + push_ref[0, at, :], imag + push_ref[1, at, :])

    zero = jnp.zeros((CHUNKS, flat), F32)
    return lax.fori_loop(0, steps, advance, (zero, zero), unroll=4)


def local_kernel(
    groups, normed_ref, w_ref, bar_ref, pack_ref, rate_ref, kept_ref, end_ref, push_ref
):
    rows = normed_ref.shape[0]
    fs, sp = w_ref.shape[:2]
    w = jnp.concatenate([w_ref[f, z] for z in range(sp) for f in range(fs)], axis=0)
    state_in = jnp.dot(normed_ref[...], w, preferred_element_type=F32).astype(BF16)
    chan = jnp.dot(chunk_order(rows, False), state_in, preferred_element_type=F32).astype(BF16)
    top = MATRIX + PACKED + PRODUCTS
    kept_ref[:top] = pack_ref[:top]
    for rows_at, to, lanes in chan_blocks(kept_ref, rows):
        kept_ref[to, lanes] = chan[rows_at].astype(F32)
    flat = bar_ref.shape[2]
    driven(chan, pack_ref, bar_ref, groups, push_ref)
    end_real, end_imag = products(pack_ref)
    last_real, last_imag = chunk_ends(bar_ref, push_ref)
    real, imag = (last_real[0:1], last_imag[0:1])
    for c in range(1, CHUNKS):
        moved_real, moved_imag = complex_product(end_real[c : c + 1], end_imag[c : c + 1], real, imag)
        real = moved_real + last_real[c : c + 1]
        imag = moved_imag + last_imag[c : c + 1]
    end = jnp.concatenate([real, imag], axis=0)
    whole = jnp.sum(rate_ref[...], axis=1, keepdims=True)
    whole = jnp.broadcast_to(whole, (2, end_ref.shape[2] - flat))
    for z in range(end_ref.shape[0]):
        end_ref[z, :, :flat] = end
        end_ref[z, :, flat:] = whole


def split_kernel(far_ref, many_ref, rest_ref):
    tall = many_ref.shape[2]
    rest_ref[...] = far_ref[:, tall:]
    for copy in range(many_ref.shape[0]):
        many_ref[copy] = far_ref[:, :tall]


def gelu(v):
    return 0.5 * v * (1.0 + jnp.tanh(0.7978845608 * (v + 0.044715 * v * v * v)))


def read_kernel(
    groups, ends_ref, bar_ref, pack_ref, mix_ref, closing_ref, push_ref
):
    flat = bar_ref.shape[2]
    states = flat // groups
    spans = ends_ref.shape[0]
    here = lax.axis_index("sp")
    decay, freq, scale, enter_real, enter_imag = (packed(pack_ref, at) for at in range(5))
    real, imag = (enter_real, enter_imag)
    elapsed = jnp.concatenate([ends_ref[z, 0:1, flat:] for z in range(spans)], axis=0)[:, 0:1] * scale
    grow = jnp.exp(elapsed * decay)
    sine, cosine = sine_cosine(elapsed * freq)
    map_real, map_imag = (grow * cosine, grow * sine)
    for z in range(spans):
        now = here == z
        enter_real = jnp.where(now, real, enter_real)
        enter_imag = jnp.where(now, imag, enter_imag)
        moved_real, moved_imag = complex_product(map_real[z : z + 1], map_imag[z : z + 1], real, imag)
        real = moved_real + ends_ref[z, 0:1, :flat]
        imag = moved_imag + ends_ref[z, 1:2, :flat]
    share = states // spans
    lane = iota((flat, share), 0) % states
    wanted = (lane == here * share + iota((flat, share), 1)).astype(BF16)
    own = iota((groups, flat), 1) // states == iota((groups, flat), 0)
    for at, row in enumerate((real, imag)):
        closing_ref[at] = picked(jnp.where(own, jnp.broadcast_to(row, (groups, flat)), 0.0), wanted)
    rows = bar_ref.shape[1]
    wide = [pack_ref[at, lanes] for _, at, lanes in chan_blocks(pack_ref, rows)]
    chan = jnp.concatenate(wide, axis=0).astype(BF16)
    driven(chan, pack_ref, bar_ref, groups, push_ref)
    end_real, end_imag = products(pack_ref)
    last_real, last_imag = chunk_ends(bar_ref, push_ref)
    in_real, in_imag = ([enter_real], [enter_imag])
    for c in range(CHUNKS - 1):
        moved_real, moved_imag = complex_product(
            end_real[c : c + 1], end_imag[c : c + 1], in_real[-1], in_imag[-1]
        )
        in_real.append(moved_real + last_real[c : c + 1])
        in_imag.append(moved_imag + last_imag[c : c + 1])
    scanned(bar_ref, push_ref, (jnp.concatenate(in_real, axis=0), jnp.concatenate(in_imag, axis=0)))
    response = None
    for at, sign in enumerate((1.0, -1.0)):
        weights = block_diagonal(matrix(pack_ref, 2 + at, states) * sign, groups)
        high, low = pieces(push_ref[at], 2)
        for left, right in ((high, 0), (low, 0), (high, 1)):
            term = lax.dot_general(left, weights[right], NT, preferred_element_type=F32)
            response = term if response is None else response + term
    skip = packed(pack_ref, 9, mix_ref.shape[1])
    mixed = gelu(response + skip * chan.astype(F32)).astype(BF16)
    mix_ref[...] = jnp.dot(chunk_order(rows, True), mixed, preferred_element_type=F32).astype(BF16)


def conv_kernel(
    state_ref, normed_ref, halo_ref, own_ref, up_ref, down_ref, left_ref, right_ref, pack_ref,
    mine_ref, theirs_ref, mix_ref, weights_ref, w_ref,
):
    width = mix_ref.shape[1]
    rows = normed_ref.shape[0]
    far = own_ref.shape[1]
    part = w_ref.shape[1]
    z, y = (lax.axis_index("sp"), lax.axis_index("fs"))

    core = lax.axis_index("tp") & 1

    def by_core(choices):
        return tuple(core * (b - a) + a for a, b in zip(*choices))

    def put(near, ref):
        for j in range(ref.shape[0]):
            far_z, far_y = by_core([offsets[j] for offsets in CLASSES])
            at_q = (z + near[0] + far_z) & 3
            at_y = (y + near[1] + far_y) & 3
            for k in range(far):
                at = (k * 4 + at_y) * 4 + at_q
                for i in range(5):
                    piece = ref[j, k, i * part : (i + 1) * part]
                    if i < 3:
                        w_ref[at, :, i * width : (i + 1) * width] = piece
                    else:
                        weights_ref[at, :, (i - 3) * width : (i - 2) * width] = piece

    for at, ref in enumerate((up_ref, down_ref, left_ref, right_ref)):
        put(by_core([offsets[at] for offsets in NEARS]), ref)
    put((0, 0), own_ref)
    w = w_ref[...].reshape(normed_ref.shape[1], 3 * width)
    taps = [packed(pack_ref, 10 + at, width) for at in range(3)]
    gain = jnp.concatenate([packed(pack_ref, 5 + at) for at in range(4)], axis=1)
    reach = len(taps) - 1
    inputs = jnp.concatenate([normalized(halo_ref[...], gain), normed_ref[...]], axis=0)
    here = jnp.dot(inputs, w, preferred_element_type=F32).astype(BF16).astype(F32)
    extended = (here[:, :width] * here[:, width : 2 * width]).astype(BF16).astype(F32)
    filtered = taps[reach] * extended[HALO:]
    for tap in range(reach):
        at = HALO - reach + tap
        filtered = filtered + taps[tap] * extended[at : at + rows]
    mix_ref[...] = (here[HALO:, 2 * width :] * filtered).astype(BF16)
    output(state_ref, mix_ref, weights_ref, mine_ref, theirs_ref)


def output(state_ref, conv_ref, w_ref, mine_ref, theirs_ref):
    chips, rows = mine_ref.shape[:2]
    core = lax.axis_index("tp") & 1

    def rows_of(ref, parity):
        return [ref[pl.ds(pl.multiple_of((2 * x + parity) * rows, rows), rows), :] for x in range(chips)]

    mixes = jnp.concatenate(
        [
            jnp.concatenate([*rows_of(ref, core), *rows_of(ref, 1 - core)], axis=0)
            for ref in (state_ref, conv_ref)
        ],
        axis=1,
    )
    per = 512
    tall, part, wide = w_ref.shape
    for at in range(0, tall * part, per):
        w = w_ref[at // part : (at + per) // part].reshape(per, wide)
        product = lax.dot_general(mixes, w, NT, preferred_element_type=F32).astype(BF16)
        for x in range(chips):
            mine_ref[x, :, at : at + per] = product[x * rows : (x + 1) * rows]
            theirs_ref[x, :, at : at + per] = product[(chips + x) * rows : (chips + x + 1) * rows]


def add_kernel(left_ref, right_ref, sum_ref):
    sum_ref[...] = (left_ref[...].astype(F32) + right_ref[...].astype(F32)).astype(BF16)


def moved(x, offsets):
    sp, fs, tp = (lax.axis_size(axis) for axis in ("sp", "fs", "tp"))
    pairs = []
    for z in range(sp):
        for y in range(fs):
            for t in range(tp):
                dz, dy = offsets[t % 2]
                source = ((z + dz) % sp * fs + (y + dy) % fs) * tp + t
                pairs.append((source, (z * fs + y) * tp + t))
    return lax.ppermute(x, ("sp", "fs", "tp"), pairs)


def all_shards(far):
    own = jnp.stack([far] + [moved(far, offsets) for offsets in list(zip(*CLASSES))[1:]])
    half = own[:2]
    return (own, *(moved(own if at < 2 else half, offsets) for at, offsets in enumerate(zip(*NEARS))))


def call(kernel, out_shape, flops, *args, smem=0, anywhere=0, aliases=None, scratch=(), limit=20 << 20):
    vmem = pl.BlockSpec(memory_space=pltpu.VMEM)
    first = [pl.BlockSpec(memory_space=pltpu.SMEM)] * smem + [pl.BlockSpec(memory_space=pl.ANY)] * anywhere
    return pl.pallas_call(
        kernel,
        out_shape=out_shape,
        in_specs=first + [vmem] * (len(args) - len(first)),
        out_specs=jax.tree.map(lambda _: vmem, out_shape),
        scratch_shapes=list(scratch),
        input_output_aliases=aliases or {},
        cost_estimate=pl.CostEstimate(flops=flops, bytes_accessed=1 << 20, transcendentals=0),
        compiler_params=pltpu.CompilerParams(vmem_limit_bytes=limit),
    )(*args)


def shape(dims, dtype=F32):
    return jax.ShapeDtypeStruct(dims, dtype)


def body(
    tokens,
    norm_gain,
    w_state_in,
    w_value,
    w_outer,
    w_inner,
    w_state_out,
    w_conv_out,
    log_step,
    decay_real,
    frequency,
    step_rate,
    input_real,
    input_imag,
    read_real,
    read_imag,
    skip_gain,
    conv_taps,
    initial_state,
):
    rows, features = tokens.shape[1:]
    groups, states = decay_real.shape
    group = skip_gain.shape[1]
    flat = groups * states
    width = groups * group
    count = lax.axis_size("sp")

    part = w_state_in.shape[0] // 4
    weights = (w_state_in, w_value, w_inner, w_outer, w_state_out, w_conv_out)
    shards = call(
        pack_kernel,
        shape((count, w_state_in.shape[0] + 5 * part, width), BF16),
        1 << 20,
        *weights,
        anywhere=len(weights),
        scratch=(
            pltpu.VMEM((len(weights), *w_state_in.shape), BF16),
            pltpu.SemaphoreType.DMA((len(weights),)),
        ),
        limit=None,
    )
    far = lax.all_to_all(shards, "sp", 0, 0, tiled=True)
    fs = lax.axis_size("fs")
    many, rest = call(
        split_kernel,
        (shape((fs, count, 4 * part, width), BF16), shape((count, 5 * part, width), BF16)),
        1 << 20,
        far,
    )
    state_weights = lax.all_to_all(many, "fs", 0, 0, tiled=True)
    own, up, down, left, right = all_shards(rest)
    edge = lax.ppermute(tokens[0, rows - HALO :], "sp", [(i, i + 1) for i in range(count - 1)])
    gain = norm_gain[None]
    into = [jnp.swapaxes(x, 1, 2).reshape(width, states) for x in (input_real, input_imag)]
    normed, bar, pack = call(
        prep_kernel,
        (shape((rows, features), BF16), shape((2, rows, flat)), shape((MATRIX + PACKED + PRODUCTS + rows * width // flat, flat))),
        1 << 30,
        log_step,
        tokens[0],
        gain,
        step_rate,
        decay_real,
        frequency,
        initial_state[0].reshape(2 * groups, states),
        *into,
        read_real.reshape(width, states),
        read_imag.reshape(width, states),
        skip_gain,
        conv_taps,
        smem=1,
        scratch=(pltpu.VMEM((rows, 16), F32),),
    )
    pack, end = call(
        functools.partial(local_kernel, groups),
        (shape(pack.shape), shape((count, 2, flat + 128))),
        1 << 29,
        normed,
        state_weights,
        bar,
        pack,
        step_rate,
        aliases={3: 0},
        scratch=(pltpu.VMEM((2, rows, flat), F32),),
    )
    ends = lax.all_to_all(end, "sp", 0, 0, tiled=True)
    state_mix, closing = call(
        functools.partial(read_kernel, groups),
        (shape((rows, width), BF16), shape((2, groups, states // count))),
        1 << 29,
        ends,
        bar,
        pack,
        scratch=(pltpu.VMEM((2, rows, flat), F32),),
    )
    tp = lax.axis_size("tp")
    chips = tp // 2
    piece = shape((chips, rows // tp, features), BF16)
    mine, theirs = call(
        conv_kernel,
        (piece, piece),
        1 << 29,
        state_mix,
        normed,
        edge,
        own,
        up,
        down,
        left,
        right,
        pack,
        scratch=(
            pltpu.VMEM((rows, width), BF16),
            pltpu.VMEM((features // part, part, 2 * width), BF16),
            pltpu.VMEM((features // part, part, 3 * width), BF16),
        ),
    )
    theirs = lax.ppermute(theirs, "tp", [(i, i ^ 1) for i in range(tp)])
    pair = call(add_kernel, piece, 1 << 20, mine, theirs)
    same_core = [[i for i in range(core, tp, 2)] for core in range(2)]
    parts = lax.all_to_all(pair, "tp", 0, 0, tiled=True, axis_index_groups=same_core)
    mixed = jnp.sum(parts.astype(F32), axis=0).astype(BF16)
    return (mixed[None], closing[None])


def solution(mesh):
    return jax.shard_map(
        body,
        mesh=mesh,
        in_specs=(
            P("fs", "sp", None),
            P(),
            P(("sp", "fs"), "tp"),
            P(("sp", "fs"), "tp"),
            P(("sp", "fs"), "tp"),
            P(("sp", "fs"), "tp"),
            P(("sp", "fs"), "tp"),
            P(("sp", "fs"), "tp"),
            P("tp"),
            P("tp", None),
            P("tp", None),
            P("fs", "sp"),
            P("tp", None, None),
            P("tp", None, None),
            P("tp", None, None),
            P("tp", None, None),
            P("tp", None),
            P(None, "tp"),
            P("fs", None, "tp", None),
        ),
        out_specs=(P("fs", ("sp", "tp"), None), P("fs", None, "tp", "sp")),
        check_vma=False,
    )
```
